128 devices in a mesh: kv: 16 (over z, x), tp: 8 (over y, core).
Axes of the slice: x: 4, y: 4, z: 4, core: 2. Of those that a mesh axis runs over, the one named last changes fastest.
Arguments:
- tokens: bfloat16 [64, 2048], P(None, 'kv'), may hold values from -6 to 6
- token_gain: float32 [2048], P('kv'), may hold values from 0.1 to 1.9
- w_query: bfloat16 [2048, 1536], P('kv', 'tp'), may hold values from -0.125 to 0.125
- w_down_kv: bfloat16 [2048, 512], P('kv'), may hold values from -0.125 to 0.125
- w_rope_key: bfloat16 [2048, 64], P('kv'), may hold values from -0.125 to 0.125
- latent_gain: float32 [512], replicated, may hold values from 0.1 to 1.9
- w_key_up: bfloat16 [8, 512, 128], P('tp'), may hold values from -0.25 to 0.25
- w_value_up: bfloat16 [8, 512, 128], P('tp'), may hold values from -0.25 to 0.25
- w_out: bfloat16 [1024, 2048], P('tp', 'kv'), may hold values from -0.1875 to 0.1875
- out_gain: float32 [2048], P('kv'), may hold values from 0.1 to 1.9
- cache_latent: bfloat16 [64, 8192, 512], P('tp', 'kv'), may hold values from -6 to 6
- cache_rope: bfloat16 [64, 8192, 64], P('tp', 'kv'), may hold values from -6 to 6
- lengths: int32 [64], replicated, may hold values from 1 to 8191, as said below
Outputs:
- mixed: bfloat16 [64, 2048], P(None, 'kv')
The draws below stay inside these ranges and needn't reach their ends.
Inputs may be any that keep to these rules, and one draw needn't show every extreme that they name: `lengths`: each of the 64 sequences has 1 to 8191 cached positions; some sequence has exactly 8191 and some exactly 1.
All inputs are finite; a program needn't handle non-finite values.
Results may differ from the reference program's by a relative error of at most 0.015.
Values may be sent and summed in bfloat16 or wider, within the bound.
No kernel may reach another device: no remote copies, remote signals or barrier semaphores. Data moves between devices by JAX's collectives and lax.ppermute only.
A program may use at most 64 MiB of HBM per device.

```python
import jax
import jax.numpy as jnp
from jax import lax

D = 2048
HEADS = 8
LATENT = 512
NOPE = 128
ROPE = 64
VDIM = 128
BATCH = 64
CACHE_LEN = 8192


def draw_lengths(key, part):
    first_key, second_key = jax.random.split(jax.random.fold_in(key, 11))
    first_draw = jax.random.randint(first_key, (BATCH,), 1, CACHE_LEN)
    second_draw = jax.random.randint(second_key, (BATCH,), 1, CACHE_LEN)
    joined = jnp.minimum(first_draw, second_draw)
    joined = joined.at[0].set(CACHE_LEN - 1).at[BATCH - 1].set(1)
    return joined.astype(jnp.int32)


def block_scale(stream_key, extent, shards, least, high):
    def one(axis_at, shards_of):
        heights = jax.random.uniform(jax.random.fold_in(jax.random.fold_in(stream_key, 6), axis_at), (shards_of,), jnp.float32, least / len(shards), high / len(shards))
        return jnp.repeat(jnp.exp(heights), extent[axis_at] // shards_of).reshape((-1,) + (1,) * (len(extent) - axis_at - 1))

    gain = one(*shards[0])
    for cut in shards[1:]:
        gain = gain * one(*cut)
    return gain


def centred(stream_key, shape, spread, limit, pieces=(), kind=jnp.bfloat16):
    values = jax.random.normal(stream_key, shape, jnp.float32) * spread
    if len(pieces) > 0:
        values = block_scale(stream_key, shape, pieces, -0.22, 0.18) * values
    return jnp.clip(values, min=-limit, max=limit).astype(kind)


def setup_inputs(seed: int = 0) -> dict:
    keys = jax.random.split(jax.random.key(seed), 14)
    return {
        "tokens": centred(keys[0], (BATCH, D), 1.0, 6.0, ((1, 16),)),
        "token_gain": jnp.clip(1.0 + 0.18 * jax.random.normal(keys[1], (D,), jnp.float32), 0.1, 1.9),
        "w_query": centred(keys[2], (D, HEADS * (NOPE + ROPE)), D ** -0.5, 0.125, ((0, 16), (1, 8))),
        "w_down_kv": centred(keys[3], (D, LATENT), D ** -0.5, 0.125, ((0, 16),)),
        "w_rope_key": centred(keys[4], (D, ROPE), D ** -0.5, 0.125, ((0, 16),)),
        "latent_gain": jnp.clip(1.0 + 0.18 * jax.random.normal(keys[5], (LATENT,), jnp.float32), 0.1, 1.9),
        "w_key_up": centred(keys[6], (HEADS, LATENT, NOPE), LATENT ** -0.5, 0.25, ((0, 8),)),
        "w_value_up": centred(keys[7], (HEADS, LATENT, VDIM), LATENT ** -0.5, 0.25, ((0, 8),)),
        "w_out": centred(keys[8], (HEADS * VDIM, D), (HEADS * VDIM) ** -0.5, 0.1875, ((0, 8), (1, 16))),
        "out_gain": jnp.clip(1.0 + 0.18 * jax.random.normal(keys[9], (D,), jnp.float32), 0.1, 1.9),
        "cache_latent": centred(keys[10], (BATCH, CACHE_LEN, LATENT), 1.0, 6.0, ((0, 8), (1, 16))),
        "cache_rope": centred(keys[11], (BATCH, CACHE_LEN, ROPE), 1.0, 6.0, ((0, 8), (1, 16))),
        "lengths": draw_lengths(jax.random.fold_in(keys[13], 71), 0),
    }


EPSILON = 1e-06
NEGATIVE = -1e+30

def rotate_half(values, cosine, sine_table):
    half_width = values.shape[-1] // 2
    lower_half = values[..., :half_width]
    upper_half = values[..., half_width:]
    return jnp.concatenate([lower_half * cosine - upper_half * sine_table, upper_half * cosine + lower_half * sine_table], axis=-1)

def angle_tables(lengths, rope_width):
    inverse_freq = 1.0 / 10000.0 ** (jnp.arange(0, rope_width, 2, dtype=jnp.float32) / rope_width)
    angles = lengths.astype(jnp.float32)[:, None] * inverse_freq[None, :]
    return (jnp.cos(angles), jnp.sin(angles))

def attend_one(packed):
    query_lat, query_rot, new_latent, new_key, length, cached_lat, cached_rot = packed
    factor = (NOPE + ROPE) ** (-0.5)
    scores = (jnp.dot(query_lat, cached_lat.T, preferred_element_type=jnp.float32) + jnp.dot(query_rot, cached_rot.T, preferred_element_type=jnp.float32)) * factor
    new_score = (jnp.dot(query_lat, new_latent, preferred_element_type=jnp.float32) + jnp.dot(query_rot, new_key, preferred_element_type=jnp.float32)) * factor
    visible = jnp.arange(CACHE_LEN) < length
    top_score = jnp.maximum(lax.optimization_barrier(jnp.max(jnp.where(visible[None, :], scores, NEGATIVE), axis=1)), new_score)
    weights = jnp.where(visible[None, :], jnp.exp(scores - top_score[:, None]), jnp.float32(0.0))
    new_weight = jnp.exp(new_score - top_score)
    weight_sum = lax.optimization_barrier(jnp.sum(weights, axis=1)) + new_weight
    rounded_new = lax.optimization_barrier(new_weight.astype(jnp.bfloat16)).astype(jnp.float32)
    weighted = jnp.dot(weights.astype(jnp.bfloat16), cached_lat, preferred_element_type=jnp.float32) + rounded_new[:, None] * new_latent.astype(jnp.float32)[None, :]
    return (weighted / weight_sum[:, None]).astype(jnp.bfloat16)

def reference(tokens, token_gain, w_query, w_down_kv, w_rope_key, latent_gain, w_key_up, w_value_up, w_out, out_gain, cache_latent, cache_rope, lengths):
    token_values = tokens.astype(jnp.float32)
    scaled = (token_values * token_gain).astype(jnp.bfloat16)
    query_heads = jnp.dot(scaled, w_query, preferred_element_type=jnp.float32).astype(jnp.bfloat16).reshape(BATCH, HEADS, NOPE + ROPE)
    latent_raw = jnp.dot(scaled, w_down_kv, preferred_element_type=jnp.float32)
    rope_raw = jnp.dot(scaled, w_rope_key, preferred_element_type=jnp.float32)
    latent = (latent_raw * lax.rsqrt(lax.optimization_barrier(jnp.mean(latent_raw * latent_raw, axis=1, keepdims=True)) + EPSILON) * latent_gain).astype(jnp.bfloat16)
    cosine, sine_table = angle_tables(lengths, ROPE)
    new_rope = rotate_half(rope_raw, cosine, sine_table).astype(jnp.bfloat16)
    query_nope = query_heads[..., :NOPE]
    query_rope = rotate_half(query_heads[..., NOPE:].astype(jnp.float32), cosine[:, None, :], sine_table[:, None, :]).astype(jnp.bfloat16)
    query_latent = jnp.einsum('bhn,hcn->bhc', query_nope.astype(jnp.float32), w_key_up.astype(jnp.float32)).astype(jnp.bfloat16)
    head_latent = lax.map(attend_one, (query_latent, query_rope, latent, new_rope, lengths, cache_latent, cache_rope))
    head_out = jnp.einsum('bhc,hcv->bhv', head_latent.astype(jnp.float32), w_value_up.astype(jnp.float32)).astype(jnp.bfloat16).reshape(BATCH, HEADS * VDIM)
    mixed_sum = jnp.dot(head_out, w_out, preferred_element_type=jnp.float32)
    out_inverse = lax.rsqrt(lax.optimization_barrier(jnp.mean(mixed_sum * mixed_sum, axis=1)) + EPSILON)[:, None]
    return (mixed_sum * out_inverse * out_gain).astype(jnp.bfloat16)
```

```python
import jax
import jax.numpy as jnp
from jax import lax
from jax.sharding import Mesh
from jax.sharding import PartitionSpec as P

KV = ("kv_0", "kv_1")
ALL = ("kv_0", "kv_1", "tp")
EPSILON = 1e-06
NEGATIVE = -1e30


def rotate_half(values, cosine, sine_table):
    half_width = values.shape[-1] // 2
    lower_half = values[..., :half_width]
    upper_half = values[..., half_width:]
    return jnp.concatenate(
        [
            lower_half * cosine - upper_half * sine_table,
            upper_half * cosine + lower_half * sine_table,
        ],
        axis=-1,
    )


def angle_tables(lengths, rope_width):
    inverse_freq = 1.0 / 10000.0 ** (jnp.arange(0, rope_width, 2, dtype=jnp.float32) / rope_width)
    angles = lengths.astype(jnp.float32)[:, None] * inverse_freq[None, :]
    return (jnp.cos(angles), jnp.sin(angles))


def exchange(value, axes):
    return lax.all_to_all(value, axes, split_axis=0, concat_axis=0, tiled=True)


def flip_pairs(value, index, bits):
    for bit in range(bits):
        width = 1 << bit
        shape = value.shape
        pairs = value.reshape((shape[0] // (2 * width), 2, width) + shape[1:])
        value = jnp.where((index >> bit) & 1 == 1, pairs[:, ::-1], pairs).reshape(shape)
    return value


def three_parts(value):
    high = lax.reduce_precision(value, 8, 7)
    middle = lax.reduce_precision(value - high, 8, 7)
    low = lax.reduce_precision(value - high - middle, 8, 7)
    return [part.astype(jnp.bfloat16) for part in (high, middle, low)]


def on_device(
    tokens,
    token_gain,
    w_query,
    w_down_kv,
    w_rope_key,
    latent_gain,
    w_key_up,
    w_value_up,
    w_out,
    out_gain,
    cache_latent,
    cache_rope,
    lengths,
):
    kv_size = lax.axis_size(KV)
    tp_size = lax.axis_size("tp")
    kv_index = lax.axis_index(KV)
    tp_index = lax.axis_index("tp")
    model_width = tokens.shape[1] * kv_size
    seqs = tokens.shape[0]
    local_seqs, local_pos, latent_width = cache_latent.shape
    rope_width = cache_rope.shape[2]
    nope = w_key_up.shape[2]
    value_width = w_value_up.shape[2]
    head_width = nope + rope_width
    factor = head_width ** (-0.5)

    weights = jnp.concatenate([w_key_up[0], w_value_up[0], w_out], axis=0)[None]
    for mask in (2, 6, 1):
        other = lax.ppermute(weights, "tp", [(i, i ^ mask) for i in range(tp_size)])
        weights = jnp.concatenate([weights, other], axis=0)
    order = (0, 2, 6, 4, 1, 3, 7, 5)

    scaled = (tokens.astype(jnp.float32) * token_gain).astype(jnp.bfloat16)
    query_part = jnp.dot(scaled, w_query, preferred_element_type=jnp.float32).astype(jnp.bfloat16)
    chunk = latent_width // tp_size
    rope_chunk = rope_width // tp_size
    down = lax.dynamic_slice_in_dim(w_down_kv, tp_index * chunk, chunk, 1)
    down_rope = lax.dynamic_slice_in_dim(w_rope_key, tp_index * rope_chunk, rope_chunk, 1)
    key_part = jnp.dot(
        scaled, jnp.concatenate([down, down_rope], axis=1), preferred_element_type=jnp.float32
    ).astype(jnp.bfloat16)
    key_part = key_part.reshape(tp_size, local_seqs, chunk + rope_chunk).transpose(1, 0, 2)
    key_part = jnp.tile(key_part, (kv_size // local_seqs, 1, 1))
    query_part = jnp.broadcast_to(
        query_part.reshape(1, tp_size, local_seqs * head_width),
        (kv_size, tp_size, local_seqs * head_width),
    )
    used = local_seqs * head_width + chunk + rope_chunk
    filled = -(-used // 128) * 128
    sent = jnp.concatenate(
        [query_part, key_part, jnp.zeros((kv_size, tp_size, filled - used), jnp.bfloat16)], axis=2
    ).reshape(kv_size * tp_size, filled)
    got = exchange(sent, ALL).reshape(kv_size, tp_size, filled).astype(jnp.float32).sum(axis=0)

    query = got[:, : local_seqs * head_width].reshape(tp_size, local_seqs, head_width)
    query = flip_pairs(query, tp_index, 3).astype(jnp.bfloat16)
    query = jnp.stack([query[i] for i in order])
    latent_raw = got[:, used - chunk - rope_chunk : used - rope_chunk].reshape(1, latent_width)
    rope_raw = got[:, used - rope_chunk : used].reshape(1, rope_width)
    latent = (
        latent_raw
        * lax.rsqrt(jnp.mean(latent_raw * latent_raw, axis=1, keepdims=True) + EPSILON)
        * latent_gain
    ).astype(jnp.bfloat16)
    own_length = lax.dynamic_slice_in_dim(lengths, tp_index * local_seqs, local_seqs, 0)
    cosine, sine_table = angle_tables(own_length, rope_width)
    new_seq = kv_index % local_seqs
    is_new = (jnp.arange(local_seqs) == new_seq) & (kv_index < local_seqs)
    new_rope = rotate_half(
        rope_raw,
        lax.dynamic_slice_in_dim(cosine, new_seq, 1, 0),
        lax.dynamic_slice_in_dim(sine_table, new_seq, 1, 0),
    ).astype(jnp.bfloat16)
    query_rope = rotate_half(query[..., nope:].astype(jnp.float32), cosine, sine_table).astype(
        jnp.bfloat16
    )
    query_latent = jnp.einsum(
        "hsn,hcn->shc",
        query[..., :nope],
        weights[:, :latent_width],
        preferred_element_type=jnp.float32,
    ).astype(jnp.bfloat16)
    query_rope = query_rope.transpose(1, 0, 2)

    positions = kv_index * local_pos + jnp.arange(local_pos, dtype=jnp.int32)
    scores = (
        jnp.einsum("bhc,blc->bhl", query_latent, cache_latent, preferred_element_type=jnp.float32)
        + jnp.einsum("bhr,blr->bhl", query_rope, cache_rope, preferred_element_type=jnp.float32)
    ) * factor
    visible = positions[None, None, :] < own_length[:, None, None]
    new_score = (
        jnp.einsum("bhc,c->bh", query_latent, latent[0], preferred_element_type=jnp.float32)
        + jnp.einsum("bhr,r->bh", query_rope, new_rope[0], preferred_element_type=jnp.float32)
    ) * factor
    holder = is_new[:, None]
    local_max = jnp.maximum(
        jnp.max(jnp.where(visible, scores, NEGATIVE), axis=2),
        jnp.where(holder, new_score, NEGATIVE),
    )
    weight = jnp.where(visible, jnp.exp(scores - local_max[..., None]), 0.0)
    new_weight = jnp.where(holder, jnp.exp(new_score - local_max), 0.0)
    weight_sum = jnp.sum(weight, axis=2) + new_weight
    weighted = (
        jnp.einsum(
            "bhl,blc->bhc",
            weight.astype(jnp.bfloat16),
            cache_latent,
            preferred_element_type=jnp.float32,
        )
        + new_weight[..., None] * latent.astype(jnp.float32)[:, None, :]
    )
    some = weight_sum > 0.0
    safe_sum = jnp.where(some, weight_sum, 1.0)
    log_sum = jnp.where(some, local_max + jnp.log(safe_sum), NEGATIVE)
    mean_latent = (weighted / safe_sum[..., None]).astype(jnp.bfloat16)
    part = jnp.einsum(
        "shc,hcv->shv",
        mean_latent,
        weights[:, latent_width : 2 * latent_width],
        preferred_element_type=jnp.float32,
    ).astype(jnp.bfloat16)

    heads = tp_size
    pairs = local_seqs * heads
    block = jnp.concatenate(
        [part.reshape(1, pairs * value_width)]
        + [x.reshape(1, pairs) for x in three_parts(log_sum)]
        + [jnp.zeros((1, pairs), jnp.bfloat16)],
        axis=1,
    )
    got = exchange(jnp.broadcast_to(block, (kv_size, block.shape[1])), KV)
    logs = got[:, pairs * value_width :].astype(jnp.float32).reshape(kv_size, 4, pairs)
    logs = logs[:, 0] + logs[:, 1] + logs[:, 2]
    share = jnp.exp(logs - jnp.max(logs, axis=0, keepdims=True))
    share = share / jnp.sum(share, axis=0, keepdims=True)
    parts = got[:, : pairs * value_width].reshape(kv_size, pairs, value_width)
    head_out = jnp.sum(parts.astype(jnp.float32) * share[..., None], axis=0)
    head_out = head_out.astype(jnp.bfloat16).reshape(local_seqs, heads * value_width)
    mixed = jnp.dot(
        head_out,
        weights[:, 2 * latent_width :].reshape(heads * value_width, -1),
        preferred_element_type=jnp.float32,
    ).astype(jnp.bfloat16)

    everyone = kv_size * tp_size
    got = exchange(jnp.broadcast_to(mixed[None], (everyone,) + mixed.shape), ALL)
    got = got.reshape(kv_size, seqs, mixed.shape[1])
    squares = jnp.sum(jnp.square(got.astype(jnp.float32)), axis=(0, 2))
    own = lax.dynamic_index_in_dim(got, kv_index, 0, keepdims=False).astype(jnp.float32)
    return (own * lax.rsqrt(squares / model_width + EPSILON)[:, None] * out_gain).astype(
        jnp.bfloat16
    )


def solution(mesh):
    finer = Mesh(mesh.devices.reshape(4, 4, mesh.shape["tp"]), ("kv_0", "kv_1", "tp"))
    return jax.shard_map(
        on_device,
        mesh=finer,
        in_specs=(
            P(None, KV),
            P(KV),
            P(KV, "tp"),
            P(KV, None),
            P(KV, None),
            P(),
            P("tp", None, None),
            P("tp", None, None),
            P("tp", KV),
            P(KV),
            P("tp", KV, None),
            P("tp", KV, None),
            P(),
        ),
        out_specs=P(None, KV),
        check_vma=False,
    )
```

```python
import functools

import jax
import jax.numpy as jnp
from jax import lax
from jax.experimental import pallas as pl
from jax.experimental.pallas import tpu as pltpu
from jax.sharding import Mesh
from jax.sharding import PartitionSpec as P


KV = ("kv_0", "kv_1")
ALL = ("kv_0", "kv_1", "tp")
EPSILON = 1e-06
NEGATIVE = -1e30
F32 = jnp.float32
BF16 = jnp.bfloat16

NT = (((1,), (1,)), ((), ()))
NN = (((1,), (0,)), ((), ()))


def dot(a, b, dims):
    return lax.dot_general(a, b, dims, preferred_element_type=F32)


def params(mib):
    return pltpu.CompilerParams(vmem_limit_bytes=mib * 1024 * 1024)


def in_vmem():
    return pl.BlockSpec(memory_space=pltpu.VMEM)


def in_smem():
    return pl.BlockSpec(memory_space=pltpu.SMEM)


def lanes(shape):
    return lax.broadcasted_iota(jnp.int32, shape, 1)


def rows(shape):
    return lax.broadcasted_iota(jnp.int32, shape, 0)


def project_kernel(index, tokens, gain, wq, wd, wr, out, *, groups, local, copies):
    tp = index[1]
    scaled = (tokens[...].astype(F32) * gain[...]).astype(BF16)
    query = dot(scaled, wq[...], NT)
    latent = dot(scaled, wd[...], NN)
    rope = dot(scaled, wr[...], NT)
    seqs = scaled.shape[0]
    chunk = latent.shape[1] // groups
    own = jnp.zeros((seqs, chunk), F32)
    for g in range(groups):
        own = jnp.where(tp == g, latent[:, g * chunk : (g + 1) * chunk], own)
    width = rope.shape[1]
    rope = jnp.where(lanes(rope.shape) // (width // groups) == tp, rope, 0.0)
    blank = jnp.zeros((seqs, 128 - width), F32)
    own = jnp.concatenate([blank, own], axis=1)
    rope = jnp.concatenate([blank, rope], axis=1)
    first = query[:, :128].astype(BF16)
    second = jnp.concatenate([query[:, 128:], blank], axis=1)
    row = rows((local, 128))
    for t in range(groups):
        top = first[t * local : (t + 1) * local]
        low = second[t * local : (t + 1) * local]
        for j in range(local):
            r = t * local + j
            new = jnp.where(row == 0, own[r : r + 1], 0.0) + jnp.where(row == 1, rope[r : r + 1], 0.0)
            tile = (low + new).astype(BF16)
            for c in range(copies // local):
                b = (c * local + j) * groups + t
                out[b, :, :128] = top
                out[b, :, 128:] = tile


def rotate(values, cosine, sine):
    half = values.shape[1] // 2
    swapped = jnp.concatenate([values[:, half:], values[:, :half]], axis=1)
    return values * cosine + swapped * sine


def attend_kernel(
    index, lengths, got, near, far, gain, cosine, sine, latents, ropes,
    out, cache, cache_rope, sums, lifted, turned, means, sems,
    *, kv_size, groups, local, factor, nope,
):
    kv = index[0]
    tp = index[1]
    copies = []
    for s in range(local):
        a = pltpu.make_async_copy(latents.at[s], cache.at[s], sems.at[s])
        b = pltpu.make_async_copy(ropes.at[s], cache_rope.at[s], sems.at[local + s])
        a.start()
        b.start()
        copies.append((a, b))
    width = cache_rope.shape[1]
    latent_width = cache.shape[2]
    positions = cache.shape[1]
    for h in range(groups):
        total = got[h].astype(F32)
        for k in range(1, kv_size):
            total = total + got[k * groups + h].astype(F32)
        sums[h] = total
    raw = jnp.concatenate([sums[h][0:1, nope + width :] for h in range(groups)], axis=1)
    rope_raw = sums[0][1:2, nope + width :]
    for h in range(1, groups):
        rope_raw = rope_raw + sums[h][1:2, nope + width :]
    square = jnp.sum(raw * raw, axis=1, keepdims=True) / latent_width
    new_latent = (raw * lax.rsqrt(square + EPSILON) * gain[...]).astype(BF16).astype(F32)
    new_seq = lax.rem(kv, local)
    new_rope = rotate(rope_raw, cosine[pl.ds(new_seq, 1), :], sine[pl.ds(new_seq, 1), :])
    new_rope = new_rope.astype(BF16).astype(F32)
    half = groups // 2
    y = tp // 2
    core = lax.rem(tp, 2)
    for i in range(groups):
        step = (0, half - 1, 1, 2)[i % half]
        head = 2 * lax.rem(y + step, half) + (core if i < half else 1 - core)
        q = sums[head]
        w = near if i < half else far
        lifted[i] = dot(q[:, :nope].astype(BF16), w[i % half, :latent_width, :], NT)
        turned[i] = rotate(
            q[:, nope : nope + width].astype(BF16).astype(F32), cosine[...], sine[...]
        )
    position = kv * positions + lanes((groups, positions))
    lane = lanes((groups, 128))
    logs = jnp.full((groups, 128), NEGATIVE, F32)
    for s in range(local):
        q = lifted[:, s, :].astype(BF16)
        qr = turned[:, s, :].astype(BF16)
        for copy in copies[s]:
            copy.wait()
        c = cache[s]
        scores = (dot(q, c, NT) + dot(qr, cache_rope[s], NN)) * factor
        new = (
            jnp.sum(q.astype(F32) * new_latent, axis=1, keepdims=True)
            + jnp.sum(qr.astype(F32) * new_rope, axis=1, keepdims=True)
        ) * factor
        is_new = jnp.logical_and(new_seq == s, kv < local)
        new = jnp.where(is_new, new, NEGATIVE)
        visible = position < lengths[tp * local + s]
        top = jnp.max(jnp.where(visible, scores, NEGATIVE), axis=1, keepdims=True)
        top = jnp.maximum(top, new)
        weight = jnp.where(visible, jnp.exp(scores - top), 0.0)
        new_weight = jnp.where(is_new, jnp.exp(new - top), 0.0)
        total = jnp.sum(weight, axis=1, keepdims=True) + new_weight
        mixed = dot(weight.astype(BF16), c, NN)
        mixed = mixed + new_weight.astype(BF16).astype(F32) * new_latent
        some = total > 0.0
        safe = jnp.where(some, total, 1.0)
        means[s] = mixed / safe
        logs = jnp.where(lane == s, jnp.where(some, top + jnp.log(safe), NEGATIVE), logs)
    for i in range(groups):
        w = near if i < half else far
        x = means[:, i, :].astype(BF16)
        up = dot(x, w[i % half, latent_width : 2 * latent_width, :], NN).astype(BF16)
        for k in range(kv_size):
            out[k, i * local : (i + 1) * local, :] = up
    square = jnp.concatenate([logs, jnp.zeros((128 - groups, 128), F32)], axis=0)
    turned_logs = jnp.transpose(square)[:local]
    high = turned_logs.astype(BF16).astype(F32)
    rest = turned_logs - high
    middle = rest.astype(BF16).astype(F32)
    low = (rest - middle).astype(BF16).astype(F32)
    packed = jnp.where(
        lane < groups,
        high,
        jnp.where(
            lane < 2 * groups,
            pltpu.roll(middle, groups, 1),
            jnp.where(lane < 3 * groups, pltpu.roll(low, 2 * groups, 1), 0.0),
        ),
    ).astype(BF16)
    for k in range(kv_size):
        out[k, groups * local :, :] = packed


def combine_kernel(got, near, far, out, *, kv_size, groups, local, first):
    logs = []
    for k in range(kv_size):
        x = got[k, groups * local :, :].astype(F32)
        logs.append(x + pltpu.roll(x, 128 - groups, 1) + pltpu.roll(x, 128 - 2 * groups, 1))
    top = functools.reduce(jnp.maximum, logs)
    shares = [jnp.exp(x - top) for x in logs]
    total = functools.reduce(jnp.add, shares)
    inverse = 1.0 / total
    shares = [x * inverse for x in shares]
    half = groups // 2
    mixed = jnp.zeros((local, out.shape[2]), F32)
    for i in range(groups):
        head = jnp.zeros((local, 128), F32)
        for k in range(kv_size):
            part = got[k, i * local : (i + 1) * local, :].astype(F32)
            head = head + part * shares[k][:, i : i + 1]
        w = near if i < half else far
        mixed = mixed + dot(head.astype(BF16), w[i % half, first:, :], NN)
    mixed = mixed.astype(BF16)
    for d in range(out.shape[0]):
        out[d] = mixed


def finish_kernel(index, got, gain, out, *, kv_size, groups, local):
    kv = index[0]
    width = got.shape[2]
    for t in range(groups):
        squares = jnp.zeros((local, width), F32)
        for k in range(kv_size):
            x = got[k * groups + t].astype(F32)
            squares = squares + x * x
        mean = jnp.sum(squares, axis=1, keepdims=True) / (width * kv_size)
        own = got[kv * groups + t].astype(F32)
        out[t * local : (t + 1) * local, :] = (
            own * lax.rsqrt(mean + EPSILON) * gain[...]
        ).astype(BF16)


def exchange(value, axes):
    return lax.all_to_all(value, axes, split_axis=0, concat_axis=0, tiled=True)


def on_device(
    tokens,
    token_gain,
    w_query,
    w_down_kv,
    w_rope_key,
    latent_gain,
    w_key_up,
    w_value_up,
    w_out,
    out_gain,
    cache_latent,
    cache_rope,
    lengths,
):
    kv_size = lax.axis_size(KV)
    groups = lax.axis_size("tp")
    everyone = kv_size * groups
    index = jnp.stack([lax.axis_index(KV), lax.axis_index("tp")]).astype(jnp.int32)
    seqs = tokens.shape[0]
    local, positions, latent_width = cache_latent.shape
    rope = cache_rope.shape[2]
    nope = w_key_up.shape[2]
    value = w_value_up.shape[2]
    factor = (nope + rope) ** (-0.5)

    own = jnp.concatenate([w_key_up[0], w_value_up[0], w_out], axis=0)
    cut = own.shape[0] // 2
    up = [(i, (i + 2) % groups) for i in range(groups)]
    down = [(i, (i - 2) % groups) for i in range(groups)]
    before = lax.ppermute(own, "tp", up)
    after = lax.ppermute(own, "tp", down)
    far_low = lax.ppermute(before[:cut], "tp", up)
    far_high = lax.ppermute(after[cut:], "tp", down)
    near = jnp.concatenate([own, before, after, far_low, far_high], axis=0)
    near = near.reshape(4, own.shape[0], own.shape[1])
    far = lax.ppermute(near, "tp", [(i, i ^ 1) for i in range(groups)])

    sent = pl.pallas_call(
        functools.partial(project_kernel, groups=groups, local=local, copies=kv_size),
        out_shape=jax.ShapeDtypeStruct((everyone, local, 256), BF16),
        in_specs=[in_smem()] + [in_vmem()] * 5,
        out_specs=in_vmem(),
        compiler_params=params(8),
        name="project",
    )(index, tokens, token_gain[None], w_query.T, w_down_kv, w_rope_key.T)
    got = exchange(sent, ALL)

    own_length = lax.dynamic_slice_in_dim(
        lengths, lax.axis_index("tp") * local, local, 0
    ).astype(F32)
    inverse_freq = 1.0 / 10000.0 ** (jnp.arange(0, rope, 2, dtype=F32) / rope)
    angles = own_length[:, None] * jnp.concatenate([inverse_freq, inverse_freq])[None, :]
    cosine = jnp.cos(angles)
    sine = jnp.sin(angles) * jnp.where(jnp.arange(rope) < rope // 2, -1.0, 1.0)[None, :]

    sent = pl.pallas_call(
        functools.partial(
            attend_kernel,
            kv_size=kv_size,
            groups=groups,
            local=local,
            factor=factor,
            nope=nope,
        ),
        out_shape=jax.ShapeDtypeStruct((kv_size, groups * local + local, value), BF16),
        in_specs=[in_smem(), in_smem()]
        + [in_vmem()] * 6
        + [pl.BlockSpec(memory_space=pl.ANY)] * 2,
        out_specs=in_vmem(),
        scratch_shapes=[
            pltpu.VMEM((local, positions, latent_width), BF16),
            pltpu.VMEM((local, rope, positions), BF16),
            pltpu.VMEM((groups, local, 256), F32),
            pltpu.VMEM((groups, local, latent_width), F32),
            pltpu.VMEM((groups, local, rope), F32),
            pltpu.VMEM((local, groups, latent_width), F32),
            pltpu.SemaphoreType.DMA((2 * local,)),
        ],
        compiler_params=params(24),
        name="attend",
    )(
        index,
        lengths,
        got,
        near,
        far,
        latent_gain[None],
        cosine,
        sine,
        cache_latent,
        cache_rope.transpose(0, 2, 1),
    )
    got = exchange(sent, KV)

    sent = pl.pallas_call(
        functools.partial(
            combine_kernel,
            kv_size=kv_size,
            groups=groups,
            local=local,
            first=2 * latent_width,
        ),
        out_shape=jax.ShapeDtypeStruct((everyone, local, w_out.shape[1]), BF16),
        in_specs=[in_vmem()] * 3,
        out_specs=in_vmem(),
        compiler_params=params(8),
        name="combine",
    )(got, near, far)
    got = exchange(sent, ALL)
    return pl.pallas_call(
        functools.partial(finish_kernel, kv_size=kv_size, groups=groups, local=local),
        out_shape=jax.ShapeDtypeStruct((seqs, w_out.shape[1]), BF16),
        in_specs=[in_smem(), in_vmem(), in_vmem()],
        out_specs=in_vmem(),
        compiler_params=params(8),
        name="finish",
    )(index, got, out_gain[None])


def solution(mesh):
    finer = Mesh(mesh.devices.reshape(4, 4, mesh.shape["tp"]), ("kv_0", "kv_1", "tp"))

    return jax.shard_map(
        on_device,
        mesh=finer,
        in_specs=(
            P(None, KV),
            P(KV),
            P(KV, "tp"),
            P(KV, None),
            P(KV, None),
            P(),
            P("tp", None, None),
            P("tp", None, None),
            P("tp", KV),
            P(KV),
            P("tp", KV, None),
            P("tp", KV, None),
            P(),
        ),
        out_specs=P(None, KV),
        check_vma=False,
    )
```

```python
import functools

import jax
import jax.numpy as jnp
from jax import lax
from jax.experimental import pallas as pl
from jax.experimental.pallas import tpu as pltpu
from jax.sharding import Mesh
from jax.sharding import PartitionSpec as P


KV = ("kv_0", "kv_1")
ALL = ("kv_0", "kv_1", "tp")
EPSILON = 1e-06
NEGATIVE = -1e30
F32 = jnp.float32
BF16 = jnp.bfloat16

NT = (((1,), (1,)), ((), ()))
NN = (((1,), (0,)), ((), ()))


def dot(a, b, dims):
    return lax.dot_general(a, b, dims, preferred_element_type=F32)


def params(mib):
    return pltpu.CompilerParams(vmem_limit_bytes=mib * 1024 * 1024)


def in_vmem():
    return pl.BlockSpec(memory_space=pltpu.VMEM)


def in_hbm():
    return pl.BlockSpec(memory_space=pltpu.HBM)


def lanes(shape):
    return lax.broadcasted_iota(jnp.int32, shape, 1)


def project_kernel(
    tokens, gain, wq, wd, wr, wk, wv, wo, out, key, own, tokens_, gain_, wq_, wd_, wr_, mixed, sems
):
    kv = lax.axis_index(KV)
    tp = lax.axis_index("tp")
    groups = lax.axis_size("tp")
    half_rows = key.shape[0]
    values = wv.shape[1]
    pairs = (
        (tokens, tokens_),
        (gain, gain_),
        (wq, wq_),
        (wd, wd_),
        (wr, wr_),
        (wk.at[0, pl.ds(lax.rem(kv, 2) * half_rows, half_rows)], key),
        (wv.at[0], own.at[pl.ds(0, values)]),
        (wo, own.at[pl.ds(values, wo.shape[0])]),
    )
    copies = [pltpu.make_async_copy(x, y, sems.at[n]) for n, (x, y) in enumerate(pairs)]
    for copy in copies:
        copy.start()
    for copy in copies[:5]:
        copy.wait()
    scaled = (tokens_[...].astype(F32) * gain_[...]).astype(BF16)
    query = dot(scaled, wq_[...], NT)
    latent = dot(scaled, wd_[...], NN)
    rope = dot(scaled, wr_[...], NT)
    chunk = latent.shape[1] // groups
    part = latent[:, :chunk]
    for g in range(1, groups):
        part = jnp.where(tp == g, latent[:, g * chunk : (g + 1) * chunk], part)
    width = rope.shape[1]
    rope = jnp.where(lanes(rope.shape) // (width // groups) == tp, rope, 0.0)
    local = mixed.shape[1]
    tiles = (
        query[:, :128],
        jnp.concatenate([query[:, 128:], part], axis=1),
        jnp.concatenate([rope, jnp.zeros_like(rope)], axis=1),
    )
    for n, tile in enumerate(tiles):
        mixed[:, :, n * 128 : (n + 1) * 128] = tile.reshape(groups, local, 128)
    for s in range(local):
        tile = mixed[:, s, :].astype(BF16)
        out[2 * s] = tile
        out[2 * s + 1] = tile
    for copy in copies[5:]:
        copy.wait()


def lift_kernel(got, key, out, *, nope, rope):
    kv = lax.axis_index(KV)
    kv_size, groups, _ = got.shape
    total = got[0].astype(F32)
    for k in range(1, kv_size):
        total = total + got[k].astype(F32)
    lifted = dot(total[:, :nope].astype(BF16), key[...], NT)
    query_rope = total[:, nope : nope + rope].astype(BF16).astype(F32)
    latent = total[:, nope + rope : 256]
    new_rope = total[:, 256 : 256 + rope]
    last = jnp.concatenate(
        [jnp.where(lax.rem(kv, 2) == 0, query_rope, new_rope), latent], axis=1
    )
    row = jnp.concatenate([lifted, last], axis=1)
    for t in range(groups):
        for k in range(kv_size):
            out[k * groups + t] = row[t : t + 1]


def rotate(values, cosine, sine):
    half = values.shape[1] // 2
    swapped = jnp.concatenate([values[:, half:], values[:, :half]], axis=1)
    return values * cosine + swapped * sine


def slot_head(i):
    tp = lax.axis_index("tp")
    groups = lax.axis_size("tp")
    half = groups // 2
    core = lax.rem(tp, 2)
    step = (0, half - 1, 1, 2)[i % half]
    return 2 * lax.rem(tp // 2 + step, half) + (core if i < half else 1 - core)


def attend_kernel(
    got, lengths, gain, cosine, sine, latents, ropes, means, packed, cache, cache_rope, slots, sems,
    *, factor,
):
    kv = lax.axis_index(KV)
    local, positions, latent_width = cache.shape
    rope = cache_rope.shape[1]
    groups = slots.shape[1]
    copies = []
    for s in range(local):
        a = pltpu.make_async_copy(latents.at[s], cache.at[s], sems.at[s])
        b = pltpu.make_async_copy(ropes.at[s], cache_rope.at[s], sems.at[local + s])
        a.start()
        b.start()
        copies.append((a, b))
    heads = [slot_head(i) for i in range(groups)]
    for i in range(groups):
        for n in range(2 * local):
            slots[n, i : i + 1, :] = got[n * groups + heads[i]]
    new_seq = lax.rem(kv, local)
    first = [got[2 * new_seq * groups + h] for h in range(groups)]
    second = [got[(2 * new_seq + 1) * groups + h] for h in range(groups)]
    raw = jnp.concatenate([x[:, 256 + rope :] for x in first], axis=1)
    rope_raw = functools.reduce(jnp.add, [x[:, 256 : 256 + rope] for x in second])
    square = jnp.sum(raw * raw, axis=1, keepdims=True) / latent_width
    new_latent = (raw * lax.rsqrt(square + EPSILON) * gain[...]).astype(BF16).astype(F32)
    new_rope = rotate(rope_raw, cosine[pl.ds(new_seq, 1), :], sine[pl.ds(new_seq, 1), :])
    new_rope = new_rope.astype(BF16).astype(F32)
    position = kv * positions + lanes((groups, positions))
    lane = lanes((groups, 128))
    logs = jnp.full((groups, 128), NEGATIVE, F32)
    for s in range(local):
        even = slots[2 * s]
        q = jnp.concatenate([even[:, :256], slots[2 * s + 1][:, :256]], axis=1).astype(BF16)
        qr = rotate(even[:, 256 : 256 + rope], cosine[s : s + 1, :], sine[s : s + 1, :])
        qr = qr.astype(BF16)
        for copy in copies[s]:
            copy.wait()
        c = cache[s]
        scores = (dot(q, c, NT) + dot(qr, cache_rope[s], NN)) * factor
        new = (
            jnp.sum(q.astype(F32) * new_latent, axis=1, keepdims=True)
            + jnp.sum(qr.astype(F32) * new_rope, axis=1, keepdims=True)
        ) * factor
        is_new = jnp.logical_and(new_seq == s, kv < local)
        new = jnp.where(is_new, new, NEGATIVE)
        visible = position < lengths[s : s + 1, :1]
        top = jnp.max(jnp.where(visible, scores, NEGATIVE), axis=1, keepdims=True)
        top = jnp.maximum(top, new)
        weight = jnp.where(visible, jnp.exp(scores - top), 0.0)
        new_weight = jnp.where(is_new, jnp.exp(new - top), 0.0)
        total = jnp.sum(weight, axis=1, keepdims=True) + new_weight
        mixed = dot(weight.astype(BF16), c, NN)
        mixed = mixed + new_weight.astype(BF16).astype(F32) * new_latent
        some = total > 0.0
        safe = jnp.where(some, total, 1.0)
        means[s] = mixed / safe
        logs = jnp.where(lane == s, jnp.where(some, top + jnp.log(safe), NEGATIVE), logs)
    square = jnp.concatenate([logs, jnp.zeros((128 - groups, 128), F32)], axis=0)
    turned = jnp.transpose(square)[:local]
    high = turned.astype(BF16).astype(F32)
    rest = turned - high
    middle = rest.astype(BF16).astype(F32)
    low = (rest - middle).astype(BF16).astype(F32)
    packed[...] = jnp.where(
        lane < groups,
        high,
        jnp.where(
            lane < 2 * groups,
            pltpu.roll(middle, groups, 1),
            jnp.where(lane < 3 * groups, pltpu.roll(low, 2 * groups, 1), 0.0),
        ),
    ).astype(BF16)


def up_kernel(means, packed, near, far, out):
    local, groups, latent_width = means.shape
    half = groups // 2
    kv_size = out.shape[0]
    for i in range(groups):
        w = near if i < half else far
        x = means[:, i, :].astype(BF16)
        up = dot(x, w[i % half, :latent_width, :], NN).astype(BF16)
        for k in range(kv_size):
            out[k, i * local : (i + 1) * local, :] = up
    logs = packed[...]
    for k in range(kv_size):
        out[k, groups * local :, :] = logs


def combine_kernel(got, near, far, out, *, kv_size, groups, local, first):
    logs = []
    for k in range(kv_size):
        x = got[k, groups * local :, :].astype(F32)
        logs.append(x + pltpu.roll(x, 128 - groups, 1) + pltpu.roll(x, 128 - 2 * groups, 1))
    top = functools.reduce(jnp.maximum, logs)
    shares = [jnp.exp(x - top) for x in logs]
    total = functools.reduce(jnp.add, shares)
    inverse = 1.0 / total
    shares = [x * inverse for x in shares]
    half = groups // 2
    mixed = jnp.zeros((local, out.shape[2]), F32)
    for i in range(groups):
        head = jnp.zeros((local, 128), F32)
        for k in range(kv_size):
            part = got[k, i * local : (i + 1) * local, :].astype(F32)
            head = head + part * shares[k][:, i : i + 1]
        w = near if i < half else far
        mixed = mixed + dot(head.astype(BF16), w[i % half, first:, :], NN)
    mixed = mixed.astype(BF16)
    for d in range(out.shape[0]):
        out[d] = mixed


def finish_kernel(got, gain, out, *, kv_size, groups, local):
    kv = lax.axis_index(KV)
    width = got.shape[2]
    for t in range(groups):
        squares = jnp.zeros((local, width), F32)
        for k in range(kv_size):
            x = got[k * groups + t].astype(F32)
            squares = squares + x * x
        mean = jnp.sum(squares, axis=1, keepdims=True) / (width * kv_size)
        own = got[kv * groups + t].astype(F32)
        out[t * local : (t + 1) * local, :] = (
            own * lax.rsqrt(mean + EPSILON) * gain[...]
        ).astype(BF16)


def exchange(value, axes):
    return lax.all_to_all(value, axes, split_axis=0, concat_axis=0, tiled=True)


def on_device(
    tokens,
    token_gain,
    w_query,
    w_down_kv,
    w_rope_key,
    latent_gain,
    w_key_up,
    w_value_up,
    w_out,
    out_gain,
    cache_latent,
    cache_rope,
    lengths,
):
    kv_size = lax.axis_size(KV)
    groups = lax.axis_size("tp")
    everyone = kv_size * groups
    seqs, width = tokens.shape
    local, positions, latent_width = cache_latent.shape
    rope = cache_rope.shape[2]
    nope = w_key_up.shape[2]
    value = w_value_up.shape[2]
    factor = (nope + rope) ** (-0.5)

    own_length = lax.dynamic_slice_in_dim(lengths, lax.axis_index("tp") * local, local, 0)
    inverse_freq = 1.0 / 10000.0 ** (jnp.arange(0, rope, 2, dtype=F32) / rope)
    angles = own_length.astype(F32)[:, None] * jnp.concatenate([inverse_freq, inverse_freq])[None]
    cosine = jnp.cos(angles)
    sine = jnp.sin(angles) * jnp.where(jnp.arange(rope) < rope // 2, -1.0, 1.0)[None, :]
    own_length = jnp.broadcast_to(own_length[:, None], (local, 128))

    sent, key, own = pl.pallas_call(
        project_kernel,
        out_shape=(
            jax.ShapeDtypeStruct((kv_size, groups, 384), BF16),
            jax.ShapeDtypeStruct((latent_width // 2, nope), BF16),
            jax.ShapeDtypeStruct((latent_width + value, value), BF16),
        ),
        in_specs=[in_hbm()] * 8,
        out_specs=(in_vmem(),) * 3,
        scratch_shapes=[
            pltpu.VMEM((seqs, width), BF16),
            pltpu.VMEM((1, width), F32),
            pltpu.VMEM((nope + rope, width), BF16),
            pltpu.VMEM((width, latent_width), BF16),
            pltpu.VMEM((rope, width), BF16),
            pltpu.VMEM((groups, local, 384), F32),
            pltpu.SemaphoreType.DMA((8,)),
        ],
        compiler_params=params(8),
        name="project",
    )(
        tokens,
        token_gain[None],
        w_query.T,
        w_down_kv,
        w_rope_key.T,
        w_key_up,
        w_value_up,
        w_out,
    )
    got = exchange(sent, KV)

    cut = own.shape[0] // 2
    up = [(i, (i + 2) % groups) for i in range(groups)]
    down = [(i, (i - 2) % groups) for i in range(groups)]
    before = lax.ppermute(own, "tp", up)
    after = lax.ppermute(own, "tp", down)
    far_low = lax.ppermute(before[:cut], "tp", up)
    far_high = lax.ppermute(after[cut:], "tp", down)
    near = jnp.concatenate([own, before, after, far_low, far_high], axis=0)
    near = near.reshape(4, own.shape[0], own.shape[1])
    far = lax.ppermute(near, "tp", [(i, i ^ 1) for i in range(groups)])

    sent = pl.pallas_call(
        functools.partial(lift_kernel, nope=nope, rope=rope),
        out_shape=jax.ShapeDtypeStruct((everyone, 1, 384), F32),
        in_specs=[in_vmem()] * 2,
        out_specs=in_vmem(),
        compiler_params=params(8),
        name="lift",
    )(got, key)
    got = exchange(sent, ALL)

    means, packed = pl.pallas_call(
        functools.partial(attend_kernel, factor=factor),
        out_shape=(
            jax.ShapeDtypeStruct((local, groups, latent_width), F32),
            jax.ShapeDtypeStruct((local, 128), BF16),
        ),
        in_specs=[in_vmem()] * 5 + [in_hbm()] * 2,
        out_specs=(in_vmem(),) * 2,
        scratch_shapes=[
            pltpu.VMEM((local, positions, latent_width), BF16),
            pltpu.VMEM((local, rope, positions), BF16),
            pltpu.VMEM((2 * local, groups, 384), F32),
            pltpu.SemaphoreType.DMA((2 * local,)),
        ],
        compiler_params=params(24),
        name="attend",
    )(got, own_length, latent_gain[None], cosine, sine, cache_latent, cache_rope.transpose(0, 2, 1))
    sent = pl.pallas_call(
        up_kernel,
        out_shape=jax.ShapeDtypeStruct((kv_size, groups * local + local, value), BF16),
        in_specs=[in_vmem()] * 4,
        out_specs=in_vmem(),
        compiler_params=params(8),
        name="value_up",
    )(means, packed, near, far)
    got = exchange(sent, KV)

    sent = pl.pallas_call(
        functools.partial(
            combine_kernel,
            kv_size=kv_size,
            groups=groups,
            local=local,
            first=latent_width,
        ),
        out_shape=jax.ShapeDtypeStruct((everyone, local, w_out.shape[1]), BF16),
        in_specs=[in_vmem()] * 3,
        out_specs=in_vmem(),
        compiler_params=params(8),
        name="combine",
    )(got, near, far)
    got = exchange(sent, ALL)
    return pl.pallas_call(
        functools.partial(finish_kernel, kv_size=kv_size, groups=groups, local=local),
        out_shape=jax.ShapeDtypeStruct((seqs, w_out.shape[1]), BF16),
        in_specs=[in_vmem(), in_vmem()],
        out_specs=in_vmem(),
        compiler_params=params(8),
        name="finish",
    )(got, out_gain[None])


def solution(mesh):
    finer = Mesh(mesh.devices.reshape(4, 4, mesh.shape["tp"]), ("kv_0", "kv_1", "tp"))

    return jax.shard_map(
        on_device,
        mesh=finer,
        in_specs=(
            P(None, KV),
            P(KV),
            P(KV, "tp"),
            P(KV, None),
            P(KV, None),
            P(),
            P("tp", None, None),
            P("tp", None, None),
            P("tp", KV),
            P(KV),
            P("tp", KV, None),
            P("tp", KV, None),
            P(),
        ),
        out_specs=P(None, KV),
        check_vma=False,
    )
```

```python
import functools

import jax
import jax.numpy as jnp
from jax import lax
from jax.experimental import pallas as pl
from jax.experimental.pallas import tpu as pltpu
from jax.sharding import Mesh
from jax.sharding import PartitionSpec as P


KV = ("kv_0", "kv_1")
ALL = ("kv_0", "kv_1", "tp")
EPSILON = 1e-06
NEGATIVE = -1e30
F32 = jnp.float32
BF16 = jnp.bfloat16

NT = (((1,), (1,)), ((), ()))
NN = (((1,), (0,)), ((), ()))


def dot(a, b, dims):
    return lax.dot_general(a, b, dims, preferred_element_type=F32)


def params(mib):
    return pltpu.CompilerParams(vmem_limit_bytes=mib * 1024 * 1024)


def in_vmem():
    return pl.BlockSpec(memory_space=pltpu.VMEM)


def in_hbm():
    return pl.BlockSpec(memory_space=pltpu.HBM)


def keep_in_hbm(*arrays):
    return [pltpu.with_memory_space_constraint(x, pltpu.HBM) for x in arrays]


def lanes(shape):
    return lax.broadcasted_iota(jnp.int32, shape, 1)


def rows(shape):
    return lax.broadcasted_iota(jnp.int32, shape, 0)


def project_kernel(
    tokens, gain, wq, wd, wr, wk, wv, wo, out, own, tokens_, gain_, wq_, wd_, wr_, sems
):
    tp = lax.axis_index("tp")
    groups = lax.axis_size("tp")
    kv_size = lax.axis_size(KV)
    deep = wk.shape[1]
    pairs = (
        (tokens, tokens_),
        (gain, gain_),
        (wq, wq_),
        (wd, wd_),
        (wr, wr_),
        (wk.at[0], own.at[pl.ds(0, deep)]),
        (wv.at[0], own.at[pl.ds(deep, deep)]),
        (wo, own.at[pl.ds(2 * deep, wo.shape[0])]),
    )
    copies = [pltpu.make_async_copy(x, y, sems.at[n]) for n, (x, y) in enumerate(pairs)]
    for copy in copies:
        copy.start()
    for copy in copies[:5]:
        copy.wait()
    scaled = (tokens_[...].astype(F32) * gain_[...]).astype(BF16)
    query = dot(scaled, wq_[...], NT)
    latent = dot(scaled, wd_[...], NN)
    rope = dot(scaled, wr_[...], NT)
    seqs = scaled.shape[0]
    local = seqs // groups
    chunk = latent.shape[1] // groups
    part = latent[:, :chunk]
    for g in range(1, groups):
        part = jnp.where(tp == g, latent[:, g * chunk : (g + 1) * chunk], part)
    width = rope.shape[1]
    rope = jnp.where(lanes(rope.shape) // (width // groups) == tp, rope, 0.0)
    blank = jnp.zeros((seqs, 128 - width), F32)
    part = jnp.concatenate([blank, part], axis=1)
    rope = jnp.concatenate([blank, rope], axis=1)
    first = query[:, :128].astype(BF16)
    second = jnp.concatenate([query[:, 128:], blank], axis=1)
    row = rows((local, 128))
    for t in range(groups):
        top = first[t * local : (t + 1) * local]
        low = second[t * local : (t + 1) * local]
        for j in range(local):
            r = t * local + j
            new = jnp.where(row == 0, part[r : r + 1], 0.0) + jnp.where(row == 1, rope[r : r + 1], 0.0)
            tile = (low + new).astype(BF16)
            for c in range(kv_size // local):
                b = (c * local + j) * groups + t
                out[b, :, :128] = top
                out[b, :, 128:] = tile
    for copy in copies[5:]:
        copy.wait()


def rotate(values, cosine, sine):
    half = values.shape[1] // 2
    swapped = jnp.concatenate([values[:, half:], values[:, :half]], axis=1)
    return values * cosine + swapped * sine


def attend_kernel(
    got, lengths, near, far, gain, cosine, sine, latents, ropes,
    out, cache, cache_rope, sums, lifted, turned, means, sems,
    *, factor, nope,
):
    kv = lax.axis_index(KV)
    tp = lax.axis_index("tp")
    kv_size = lax.axis_size(KV)
    groups = lax.axis_size("tp")
    local = cache.shape[0]
    copies = []
    for s in range(local):
        a = pltpu.make_async_copy(latents.at[s], cache.at[s], sems.at[s])
        b = pltpu.make_async_copy(ropes.at[s], cache_rope.at[s], sems.at[local + s])
        a.start()
        b.start()
        copies.append((a, b))
    width = cache_rope.shape[1]
    latent_width = cache.shape[2]
    positions = cache.shape[1]
    for h in range(groups):
        total = got[h].astype(F32)
        for k in range(1, kv_size):
            total = total + got[k * groups + h].astype(F32)
        sums[h] = total
    raw = jnp.concatenate([sums[h][0:1, nope + width :] for h in range(groups)], axis=1)
    rope_raw = sums[0][1:2, nope + width :]
    for h in range(1, groups):
        rope_raw = rope_raw + sums[h][1:2, nope + width :]
    square = jnp.sum(raw * raw, axis=1, keepdims=True) / latent_width
    new_latent = (raw * lax.rsqrt(square + EPSILON) * gain[...]).astype(BF16).astype(F32)
    new_seq = lax.rem(kv, local)
    new_rope = rotate(rope_raw, cosine[pl.ds(new_seq, 1), :], sine[pl.ds(new_seq, 1), :])
    new_rope = new_rope.astype(BF16).astype(F32)
    half = groups // 2
    y = tp // 2
    core = lax.rem(tp, 2)
    for i in range(groups):
        step = (0, half - 1, 1, 2)[i % half]
        head = 2 * lax.rem(y + step, half) + (core if i < half else 1 - core)
        q = sums[head]
        w = near if i < half else far
        lifted[i] = dot(q[:, :nope].astype(BF16), w[i % half, :latent_width, :], NT)
        turned[i] = rotate(
            q[:, nope : nope + width].astype(BF16).astype(F32), cosine[...], sine[...]
        )
    position = kv * positions + lanes((groups, positions))
    lane = lanes((groups, 128))
    logs = jnp.full((groups, 128), NEGATIVE, F32)
    for s in range(local):
        q = lifted[:, s, :].astype(BF16)
        qr = turned[:, s, :].astype(BF16)
        for copy in copies[s]:
            copy.wait()
        c = cache[s]
        scores = (dot(q, c, NT) + dot(qr, cache_rope[s], NN)) * factor
        new = (
            jnp.sum(q.astype(F32) * new_latent, axis=1, keepdims=True)
            + jnp.sum(qr.astype(F32) * new_rope, axis=1, keepdims=True)
        ) * factor
        is_new = jnp.logical_and(new_seq == s, kv < local)
        new = jnp.where(is_new, new, NEGATIVE)
        visible = position < lengths[s : s + 1, :1]
        top = jnp.max(jnp.where(visible, scores, NEGATIVE), axis=1, keepdims=True)
        top = jnp.maximum(top, new)
        weight = jnp.where(visible, jnp.exp(scores - top), 0.0)
        new_weight = jnp.where(is_new, jnp.exp(new - top), 0.0)
        total = jnp.sum(weight, axis=1, keepdims=True) + new_weight
        mixed = dot(weight.astype(BF16), c, NN)
        mixed = mixed + new_weight.astype(BF16).astype(F32) * new_latent
        some = total > 0.0
        safe = jnp.where(some, total, 1.0)
        means[s] = mixed / safe
        logs = jnp.where(lane == s, jnp.where(some, top + jnp.log(safe), NEGATIVE), logs)
    for i in range(groups):
        w = near if i < half else far
        x = means[:, i, :].astype(BF16)
        up = dot(x, w[i % half, latent_width : 2 * latent_width, :], NN).astype(BF16)
        for k in range(kv_size):
            out[k, i * local : (i + 1) * local, :] = up
    square = jnp.concatenate([logs, jnp.zeros((128 - groups, 128), F32)], axis=0)
    turned_logs = jnp.transpose(square)[:local]
    high = turned_logs.astype(BF16).astype(F32)
    rest = turned_logs - high
    middle = rest.astype(BF16).astype(F32)
    low = (rest - middle).astype(BF16).astype(F32)
    packed = jnp.where(
        lane < groups,
        high,
        jnp.where(
            lane < 2 * groups,
            pltpu.roll(middle, groups, 1),
            jnp.where(lane < 3 * groups, pltpu.roll(low, 2 * groups, 1), 0.0),
        ),
    ).astype(BF16)
    for k in range(kv_size):
        out[k, groups * local :, :] = packed


def combine_kernel(got, near, far, out, *, kv_size, groups, local, first):
    logs = []
    for k in range(kv_size):
        x = got[k, groups * local :, :].astype(F32)
        logs.append(x + pltpu.roll(x, 128 - groups, 1) + pltpu.roll(x, 128 - 2 * groups, 1))
    top = functools.reduce(jnp.maximum, logs)
    shares = [jnp.exp(x - top) for x in logs]
    total = functools.reduce(jnp.add, shares)
    inverse = 1.0 / total
    shares = [x * inverse for x in shares]
    half = groups // 2
    mixed = jnp.zeros((local, out.shape[2]), F32)
    for i in range(groups):
        head = jnp.zeros((local, 128), F32)
        for k in range(kv_size):
            part = got[k, i * local : (i + 1) * local, :].astype(F32)
            head = head + part * shares[k][:, i : i + 1]
        w = near if i < half else far
        mixed = mixed + dot(head.astype(BF16), w[i % half, first:, :], NN)
    mixed = mixed.astype(BF16)
    for d in range(out.shape[0]):
        out[d] = mixed


def finish_kernel(got, gain, out, *, kv_size, groups, local):
    kv = lax.axis_index(KV)
    width = got.shape[2]
    for t in range(groups):
        squares = jnp.zeros((local, width), F32)
        for k in range(kv_size):
            x = got[k * groups + t].astype(F32)
            squares = squares + x * x
        mean = jnp.sum(squares, axis=1, keepdims=True) / (width * kv_size)
        own = got[kv * groups + t].astype(F32)
        out[t * local : (t + 1) * local, :] = (
            own * lax.rsqrt(mean + EPSILON) * gain[...]
        ).astype(BF16)


def exchange(value, axes):
    return lax.all_to_all(value, axes, split_axis=0, concat_axis=0, tiled=True)


def on_device(
    tokens,
    token_gain,
    w_query,
    w_down_kv,
    w_rope_key,
    latent_gain,
    w_key_up,
    w_value_up,
    w_out,
    out_gain,
    cache_latent,
    cache_rope,
    lengths,
):
    kv_size = lax.axis_size(KV)
    groups = lax.axis_size("tp")
    everyone = kv_size * groups
    seqs, width = tokens.shape
    local, positions, latent_width = cache_latent.shape
    rope = cache_rope.shape[2]
    nope = w_key_up.shape[2]
    value = w_value_up.shape[2]
    factor = (nope + rope) ** (-0.5)

    own_length = lax.dynamic_slice_in_dim(lengths, lax.axis_index("tp") * local, local, 0)
    inverse_freq = 1.0 / 10000.0 ** (jnp.arange(0, rope, 2, dtype=F32) / rope)
    angles = own_length.astype(F32)[:, None] * jnp.concatenate([inverse_freq, inverse_freq])[None]
    cosine = jnp.cos(angles)
    sine = jnp.sin(angles) * jnp.where(jnp.arange(rope) < rope // 2, -1.0, 1.0)[None, :]
    own_length = jnp.broadcast_to(own_length[:, None], (local, 128))

    sent, own = pl.pallas_call(
        project_kernel,
        out_shape=(
            jax.ShapeDtypeStruct((everyone, local, 256), BF16),
            jax.ShapeDtypeStruct((2 * latent_width + value, nope), BF16),
        ),
        in_specs=[in_hbm()] * 8,
        out_specs=(in_vmem(),) * 2,
        scratch_shapes=[
            pltpu.VMEM((seqs, width), BF16),
            pltpu.VMEM((1, width), F32),
            pltpu.VMEM((nope + rope, width), BF16),
            pltpu.VMEM((width, latent_width), BF16),
            pltpu.VMEM((rope, width), BF16),
            pltpu.SemaphoreType.DMA((8,)),
        ],
        compiler_params=params(8),
        name="project",
    )(
        *keep_in_hbm(
            tokens,
            token_gain[None],
            w_query.T,
            w_down_kv,
            w_rope_key.T,
            w_key_up,
            w_value_up,
            w_out,
        )
    )

    collected = [own]
    for step in (1, 3, 2):
        collected.append(
            lax.ppermute(own, "tp", [(i, (i + 2 * step) % groups) for i in range(groups)])
        )
    near = jnp.stack(collected)
    far = lax.ppermute(near, "tp", [(i, i ^ 1) for i in range(groups)])

    got = exchange(sent, ALL)
    sent = pl.pallas_call(
        functools.partial(attend_kernel, factor=factor, nope=nope),
        out_shape=jax.ShapeDtypeStruct((kv_size, groups * local + local, value), BF16),
        in_specs=[in_vmem()] * 7 + [in_hbm()] * 2,
        out_specs=in_vmem(),
        scratch_shapes=[
            pltpu.VMEM((local, positions, latent_width), BF16),
            pltpu.VMEM((local, rope, positions), BF16),
            pltpu.VMEM((groups, local, 256), F32),
            pltpu.VMEM((groups, local, latent_width), F32),
            pltpu.VMEM((groups, local, rope), F32),
            pltpu.VMEM((local, groups, latent_width), F32),
            pltpu.SemaphoreType.DMA((2 * local,)),
        ],
        compiler_params=params(24),
        name="attend",
    )(
        got,
        own_length,
        near,
        far,
        latent_gain[None],
        cosine,
        sine,
        *keep_in_hbm(cache_latent, cache_rope.transpose(0, 2, 1)),
    )
    got = exchange(sent, KV)

    sent = pl.pallas_call(
        functools.partial(
            combine_kernel,
            kv_size=kv_size,
            groups=groups,
            local=local,
            first=2 * latent_width,
        ),
        out_shape=jax.ShapeDtypeStruct((everyone, local, w_out.shape[1]), BF16),
        in_specs=[in_vmem()] * 3,
        out_specs=in_vmem(),
        compiler_params=params(8),
        name="combine",
    )(got, near, far)
    got = exchange(sent, ALL)
    return pl.pallas_call(
        functools.partial(finish_kernel, kv_size=kv_size, groups=groups, local=local),
        out_shape=jax.ShapeDtypeStruct((seqs, w_out.shape[1]), BF16),
        in_specs=[in_vmem(), in_vmem()],
        out_specs=in_vmem(),
        compiler_params=params(8),
        name="finish",
    )(got, out_gain[None])


def solution(mesh):
    finer = Mesh(mesh.devices.reshape(4, 4, mesh.shape["tp"]), ("kv_0", "kv_1", "tp"))

    return jax.shard_map(
        on_device,
        mesh=finer,
        in_specs=(
            P(None, KV),
            P(KV),
            P(KV, "tp"),
            P(KV, None),
            P(KV, None),
            P(),
            P("tp", None, None),
            P("tp", None, None),
            P("tp", KV),
            P(KV),
            P("tp", KV, None),
            P("tp", KV, None),
            P(),
        ),
        out_specs=P(None, KV),
        check_vma=False,
    )
```

```python
import functools

import jax
import jax.numpy as jnp
from jax import lax
from jax.experimental import pallas as pl
from jax.experimental.pallas import tpu as pltpu
from jax.sharding import Mesh
from jax.sharding import PartitionSpec as P


KV = ("kv_0", "kv_1")
ALL = ("kv_0", "kv_1", "tp")
EPSILON = 1e-06
NEGATIVE = -1e30
F32 = jnp.float32
BF16 = jnp.bfloat16

NT = (((1,), (1,)), ((), ()))
NN = (((1,), (0,)), ((), ()))


def dot(a, b, dims):
    return lax.dot_general(a, b, dims, preferred_element_type=F32)


def params(mib):
    return pltpu.CompilerParams(vmem_limit_bytes=mib * 1024 * 1024)


def in_vmem():
    return pl.BlockSpec(memory_space=pltpu.VMEM)


def in_hbm():
    return pl.BlockSpec(memory_space=pltpu.HBM)


def keep_in_hbm(*arrays):
    return [pltpu.with_memory_space_constraint(x, pltpu.HBM) for x in arrays]


def lanes(shape):
    return lax.broadcasted_iota(jnp.int32, shape, 1)


def rows(shape):
    return lax.broadcasted_iota(jnp.int32, shape, 0)


def project_kernel(
    tokens, gain, wq, wd, wr, wv, wo, out, own, tokens_, gain_, wq_, wd_, wr_, sems
):
    tp = lax.axis_index("tp")
    groups = lax.axis_size("tp")
    kv_size = lax.axis_size(KV)
    deep = wv.shape[1]
    pairs = (
        (tokens, tokens_),
        (gain, gain_),
        (wq, wq_),
        (wd, wd_),
        (wr, wr_),
        (wv.at[0], own.at[pl.ds(0, deep)]),
        (wo, own.at[pl.ds(deep, wo.shape[0])]),
    )
    copies = [pltpu.make_async_copy(x, y, sems.at[n]) for n, (x, y) in enumerate(pairs)]
    for copy in copies:
        copy.start()
    for copy in copies[:5]:
        copy.wait()
    scaled = (tokens_[...].astype(F32) * gain_[...]).astype(BF16)
    query = dot(scaled, wq_[...], NT)
    latent = dot(scaled, wd_[...], NN)
    rope = dot(scaled, wr_[...], NT)
    seqs = scaled.shape[0]
    local = seqs // groups
    chunk = latent.shape[1] // groups
    part = latent[:, :chunk]
    for g in range(1, groups):
        part = jnp.where(tp == g, latent[:, g * chunk : (g + 1) * chunk], part)
    width = rope.shape[1]
    rope = jnp.where(lanes(rope.shape) // (width // groups) == tp, rope, 0.0)
    blank = jnp.zeros((seqs, 128 - width), F32)
    part = jnp.concatenate([blank, part], axis=1)
    rope = jnp.concatenate([blank, rope], axis=1)
    first = query[:, :128].astype(BF16)
    second = jnp.concatenate([query[:, 128:], blank], axis=1)
    row = rows((local, 128))
    for t in range(groups):
        top = first[t * local : (t + 1) * local]
        low = second[t * local : (t + 1) * local]
        for j in range(local):
            r = t * local + j
            new = jnp.where(row == 0, part[r : r + 1], 0.0) + jnp.where(row == 1, rope[r : r + 1], 0.0)
            tile = (low + new).astype(BF16)
            for c in range(kv_size // local):
                b = (c * local + j) * groups + t
                out[b, :, :128] = top
                out[b, :, 128:] = tile
    for copy in copies[5:]:
        copy.wait()


def rotate(values, cosine, sine):
    half = values.shape[1] // 2
    swapped = jnp.concatenate([values[:, half:], values[:, :half]], axis=1)
    return values * cosine + swapped * sine


def attend_kernel(
    got, lengths, near, far, gain, cosine, sine, latents, ropes,
    means, packed, cache, cache_rope, sums, lifted, turned, sems,
    *, factor, nope,
):
    kv = lax.axis_index(KV)
    tp = lax.axis_index("tp")
    kv_size = lax.axis_size(KV)
    groups = lax.axis_size("tp")
    local = cache.shape[0]
    copies = []
    for s in range(local):
        a = pltpu.make_async_copy(latents.at[s], cache.at[s], sems.at[s])
        b = pltpu.make_async_copy(ropes.at[s], cache_rope.at[s], sems.at[local + s])
        a.start()
        b.start()
        copies.append((a, b))
    width = cache_rope.shape[1]
    latent_width = cache.shape[2]
    positions = cache.shape[1]
    for h in range(groups):
        total = got[h].astype(F32)
        for k in range(1, kv_size):
            total = total + got[k * groups + h].astype(F32)
        sums[h] = total
    raw = jnp.concatenate([sums[h][0:1, nope + width :] for h in range(groups)], axis=1)
    rope_raw = sums[0][1:2, nope + width :]
    for h in range(1, groups):
        rope_raw = rope_raw + sums[h][1:2, nope + width :]
    square = jnp.sum(raw * raw, axis=1, keepdims=True) / latent_width
    new_latent = (raw * lax.rsqrt(square + EPSILON) * gain[...]).astype(BF16).astype(F32)
    new_seq = lax.rem(kv, local)
    new_rope = rotate(rope_raw, cosine[pl.ds(new_seq, 1), :], sine[pl.ds(new_seq, 1), :])
    new_rope = new_rope.astype(BF16).astype(F32)
    half = groups // 2
    y = tp // 2
    core = lax.rem(tp, 2)
    for i in range(groups):
        step = (0, half - 1, 1, 2)[i % half]
        head = 2 * lax.rem(y + step, half) + (core if i < half else 1 - core)
        q = sums[head]
        w = near if i < half else far
        lifted[i] = dot(q[:, :nope].astype(BF16), w[i % half], NT)
        turned[i] = rotate(
            q[:, nope : nope + width].astype(BF16).astype(F32), cosine[...], sine[...]
        )
    position = kv * positions + lanes((groups, positions))
    lane = lanes((groups, 128))
    logs = jnp.full((groups, 128), NEGATIVE, F32)
    for s in range(local):
        q = lifted[:, s, :].astype(BF16)
        qr = turned[:, s, :].astype(BF16)
        for copy in copies[s]:
            copy.wait()
        c = cache[s]
        scores = (dot(q, c, NT) + dot(qr, cache_rope[s], NN)) * factor
        new = (
            jnp.sum(q.astype(F32) * new_latent, axis=1, keepdims=True)
            + jnp.sum(qr.astype(F32) * new_rope, axis=1, keepdims=True)
        ) * factor
        is_new = jnp.logical_and(new_seq == s, kv < local)
        new = jnp.where(is_new, new, NEGATIVE)
        visible = position < lengths[s : s + 1, :1]
        top = jnp.max(jnp.where(visible, scores, NEGATIVE), axis=1, keepdims=True)
        top = jnp.maximum(top, new)
        weight = jnp.where(visible, jnp.exp(scores - top), 0.0)
        new_weight = jnp.where(is_new, jnp.exp(new - top), 0.0)
        total = jnp.sum(weight, axis=1, keepdims=True) + new_weight
        mixed = dot(weight.astype(BF16), c, NN)
        mixed = mixed + new_weight.astype(BF16).astype(F32) * new_latent
        some = total > 0.0
        safe = jnp.where(some, total, 1.0)
        means[s] = mixed / safe
        logs = jnp.where(lane == s, jnp.where(some, top + jnp.log(safe), NEGATIVE), logs)
    square = jnp.concatenate([logs, jnp.zeros((128 - groups, 128), F32)], axis=0)
    turned_logs = jnp.transpose(square)[:local]
    high = turned_logs.astype(BF16).astype(F32)
    rest = turned_logs - high
    middle = rest.astype(BF16).astype(F32)
    low = (rest - middle).astype(BF16).astype(F32)
    packed[...] = jnp.where(
        lane < groups,
        high,
        jnp.where(
            lane < 2 * groups,
            pltpu.roll(middle, groups, 1),
            jnp.where(lane < 3 * groups, pltpu.roll(low, 2 * groups, 1), 0.0),
        ),
    ).astype(BF16)


def up_kernel(means, packed, near, far, out):
    local, groups, latent_width = means.shape
    half = groups // 2
    kv_size = out.shape[0]
    for i in range(groups):
        w = near if i < half else far
        x = means[:, i, :].astype(BF16)
        up = dot(x, w[i % half, :latent_width, :], NN).astype(BF16)
        for k in range(kv_size):
            out[k, i * local : (i + 1) * local, :] = up
    logs = packed[...]
    for k in range(kv_size):
        out[k, groups * local :, :] = logs


def combine_kernel(got, near, far, out, *, kv_size, groups, local, first):
    logs = []
    for k in range(kv_size):
        x = got[k, groups * local :, :].astype(F32)
        logs.append(x + pltpu.roll(x, 128 - groups, 1) + pltpu.roll(x, 128 - 2 * groups, 1))
    top = functools.reduce(jnp.maximum, logs)
    shares = [jnp.exp(x - top) for x in logs]
    total = functools.reduce(jnp.add, shares)
    inverse = 1.0 / total
    shares = [x * inverse for x in shares]
    half = groups // 2
    mixed = jnp.zeros((local, out.shape[2]), F32)
    for i in range(groups):
        head = jnp.zeros((local, 128), F32)
        for k in range(kv_size):
            part = got[k, i * local : (i + 1) * local, :].astype(F32)
            head = head + part * shares[k][:, i : i + 1]
        w = near if i < half else far
        mixed = mixed + dot(head.astype(BF16), w[i % half, first:, :], NN)
    mixed = mixed.astype(BF16)
    for d in range(out.shape[0]):
        out[d] = mixed


def finish_kernel(got, gain, out, *, kv_size, groups, local):
    kv = lax.axis_index(KV)
    width = got.shape[2]
    for t in range(groups):
        squares = jnp.zeros((local, width), F32)
        for k in range(kv_size):
            x = got[k * groups + t].astype(F32)
            squares = squares + x * x
        mean = jnp.sum(squares, axis=1, keepdims=True) / (width * kv_size)
        own = got[kv * groups + t].astype(F32)
        out[t * local : (t + 1) * local, :] = (
            own * lax.rsqrt(mean + EPSILON) * gain[...]
        ).astype(BF16)


def exchange(value, axes):
    return lax.all_to_all(value, axes, split_axis=0, concat_axis=0, tiled=True)


def swap(value):
    return lax.ppermute(value, "tp", [(i, i ^ 1) for i in range(lax.axis_size("tp"))])


def along(own):
    groups = lax.axis_size("tp")
    up = [(i, (i + 2) % groups) for i in range(groups)]
    down = [(i, (i - 2) % groups) for i in range(groups)]
    cut = own.shape[0] // 2
    before = lax.ppermute(own, "tp", up)
    after = lax.ppermute(own, "tp", down)
    low = lax.ppermute(before[:cut], "tp", up)
    high = lax.ppermute(after[cut:], "tp", down)
    return jnp.concatenate([own, before, after, low, high], axis=0).reshape((4,) + own.shape)


def on_device(
    tokens,
    token_gain,
    w_query,
    w_down_kv,
    w_rope_key,
    latent_gain,
    w_key_up,
    w_value_up,
    w_out,
    out_gain,
    cache_latent,
    cache_rope,
    lengths,
):
    kv_size = lax.axis_size(KV)
    groups = lax.axis_size("tp")
    everyone = kv_size * groups
    seqs, width = tokens.shape
    local, positions, latent_width = cache_latent.shape
    rope = cache_rope.shape[2]
    nope = w_key_up.shape[2]
    value = w_value_up.shape[2]
    factor = (nope + rope) ** (-0.5)

    own_length = lax.dynamic_slice_in_dim(lengths, lax.axis_index("tp") * local, local, 0)
    inverse_freq = 1.0 / 10000.0 ** (jnp.arange(0, rope, 2, dtype=F32) / rope)
    angles = own_length.astype(F32)[:, None] * jnp.concatenate([inverse_freq, inverse_freq])[None]
    cosine = jnp.cos(angles)
    sine = jnp.sin(angles) * jnp.where(jnp.arange(rope) < rope // 2, -1.0, 1.0)[None, :]
    own_length = jnp.broadcast_to(own_length[:, None], (local, 128))

    sent, own = pl.pallas_call(
        project_kernel,
        out_shape=(
            jax.ShapeDtypeStruct((everyone, local, 256), BF16),
            jax.ShapeDtypeStruct((latent_width + value, value), BF16),
        ),
        in_specs=[in_hbm()] * 7,
        out_specs=(in_vmem(),) * 2,
        scratch_shapes=[
            pltpu.VMEM((seqs, width), BF16),
            pltpu.VMEM((1, width), F32),
            pltpu.VMEM((nope + rope, width), BF16),
            pltpu.VMEM((width, latent_width), BF16),
            pltpu.VMEM((rope, width), BF16),
            pltpu.SemaphoreType.DMA((7,)),
        ],
        compiler_params=params(8),
        name="project",
    )(
        *keep_in_hbm(
            tokens,
            token_gain[None],
            w_query.T,
            w_down_kv,
            w_rope_key.T,
            w_value_up,
            w_out,
        )
    )

    near_key = along(w_key_up[0])
    far_key = swap(near_key)
    near = along(own)
    far = swap(near)

    got = exchange(sent, ALL)
    means, packed = pl.pallas_call(
        functools.partial(attend_kernel, factor=factor, nope=nope),
        out_shape=(
            jax.ShapeDtypeStruct((local, groups, latent_width), F32),
            jax.ShapeDtypeStruct((local, 128), BF16),
        ),
        in_specs=[in_vmem()] * 7 + [in_hbm()] * 2,
        out_specs=(in_vmem(),) * 2,
        scratch_shapes=[
            pltpu.VMEM((local, positions, latent_width), BF16),
            pltpu.VMEM((local, rope, positions), BF16),
            pltpu.VMEM((groups, local, 256), F32),
            pltpu.VMEM((groups, local, latent_width), F32),
            pltpu.VMEM((groups, local, rope), F32),
            pltpu.SemaphoreType.DMA((2 * local,)),
        ],
        compiler_params=params(24),
        name="attend",
    )(
        got,
        own_length,
        near_key,
        far_key,
        latent_gain[None],
        cosine,
        sine,
        *keep_in_hbm(cache_latent, cache_rope.transpose(0, 2, 1)),
    )
    sent = pl.pallas_call(
        up_kernel,
        out_shape=jax.ShapeDtypeStruct((kv_size, groups * local + local, value), BF16),
        in_specs=[in_vmem()] * 4,
        out_specs=in_vmem(),
        compiler_params=params(8),
        name="value_up",
    )(means, packed, near, far)
    got = exchange(sent, KV)

    sent = pl.pallas_call(
        functools.partial(
            combine_kernel,
            kv_size=kv_size,
            groups=groups,
            local=local,
            first=latent_width,
        ),
        out_shape=jax.ShapeDtypeStruct((everyone, local, w_out.shape[1]), BF16),
        in_specs=[in_vmem()] * 3,
        out_specs=in_vmem(),
        compiler_params=params(8),
        name="combine",
    )(got, near, far)
    got = exchange(sent, ALL)
    return pl.pallas_call(
        functools.partial(finish_kernel, kv_size=kv_size, groups=groups, local=local),
        out_shape=jax.ShapeDtypeStruct((seqs, w_out.shape[1]), BF16),
        in_specs=[in_vmem(), in_vmem()],
        out_specs=in_vmem(),
        compiler_params=params(8),
        name="finish",
    )(got, out_gain[None])


def solution(mesh):
    finer = Mesh(mesh.devices.reshape(4, 4, mesh.shape["tp"]), ("kv_0", "kv_1", "tp"))

    return jax.shard_map(
        on_device,
        mesh=finer,
        in_specs=(
            P(None, KV),
            P(KV),
            P(KV, "tp"),
            P(KV, None),
            P(KV, None),
            P(),
            P("tp", None, None),
            P("tp", None, None),
            P("tp", KV),
            P(KV),
            P("tp", KV, None),
            P("tp", KV, None),
            P(),
        ),
        out_specs=P(None, KV),
        check_vma=False,
    )
```

```python
import functools

import jax
import jax.numpy as jnp
import numpy as np
from jax import lax
from jax.experimental import pallas as pl
from jax.experimental.pallas import tpu as pltpu
from jax.sharding import Mesh
from jax.sharding import PartitionSpec as P


KV = ("kv_0", "kv_1")
ALL = ("kv_0", "kv_1", "tp")
EPSILON = 1e-06
NEGATIVE = -1e30
F32 = jnp.float32
BF16 = jnp.bfloat16

NT = (((1,), (1,)), ((), ()))
NN = (((1,), (0,)), ((), ()))


def dot(a, b, dims):
    return lax.dot_general(a, b, dims, preferred_element_type=F32)


def params(mib):
    return pltpu.CompilerParams(vmem_limit_bytes=mib * 1024 * 1024)


def in_vmem():
    return pl.BlockSpec(memory_space=pltpu.VMEM)


def in_hbm():
    return pl.BlockSpec(memory_space=pltpu.HBM)


def keep_in_hbm(*arrays):
    return [pltpu.with_memory_space_constraint(x, pltpu.HBM) for x in arrays]


def lanes(shape):
    return lax.broadcasted_iota(jnp.int32, shape, 1)


def rows(shape):
    return lax.broadcasted_iota(jnp.int32, shape, 0)


def project_kernel(
    tokens, gain, wq, wd, wr, wk, wv, wo, out, own, tokens_, gain_, wq_, wd_, wr_, sems
):
    tp = lax.axis_index("tp")
    groups = lax.axis_size("tp")
    kv_size = lax.axis_size(KV)
    deep = wk.shape[1]
    pairs = (
        (tokens, tokens_),
        (gain, gain_),
        (wq, wq_),
        (wd, wd_),
        (wr, wr_),
        (wk.at[0], own.at[pl.ds(0, deep)]),
        (wv.at[0], own.at[pl.ds(deep, deep)]),
        (wo, own.at[pl.ds(2 * deep, wo.shape[0])]),
    )
    copies = [pltpu.make_async_copy(x, y, sems.at[n]) for n, (x, y) in enumerate(pairs)]
    for copy in copies:
        copy.start()
    for copy in copies[:5]:
        copy.wait()
    scaled = (tokens_[...].astype(F32) * gain_[...]).astype(BF16)
    query = dot(scaled, wq_[...], NT)
    latent = dot(scaled, wd_[...], NN)
    rope = dot(scaled, wr_[...], NT)
    seqs = scaled.shape[0]
    local = seqs // groups
    chunk = latent.shape[1] // groups
    part = latent[:, :chunk]
    for g in range(1, groups):
        part = jnp.where(tp == g, latent[:, g * chunk : (g + 1) * chunk], part)
    width = rope.shape[1]
    rope = jnp.where(lanes(rope.shape) // (width // groups) == tp, rope, 0.0)
    blank = jnp.zeros((seqs, 128 - width), F32)
    part = jnp.concatenate([blank, part], axis=1)
    rope = jnp.concatenate([blank, rope], axis=1)
    first = query[:, :128].astype(BF16)
    second = jnp.concatenate([query[:, 128:], blank], axis=1)
    row = rows((local, 128))
    for t in range(groups):
        top = first[t * local : (t + 1) * local]
        low = second[t * local : (t + 1) * local]
        for j in range(local):
            r = t * local + j
            new = jnp.where(row == 0, part[r : r + 1], 0.0) + jnp.where(row == 1, rope[r : r + 1], 0.0)
            tile = (low + new).astype(BF16)
            for c in range(kv_size // local):
                b = (c * local + j) * groups + t
                out[b, :, :128] = top
                out[b, :, 128:] = tile
    for copy in copies[5:]:
        copy.wait()


def rotate(values, cosine, sine):
    half = values.shape[1] // 2
    swapped = jnp.concatenate([values[:, half:], values[:, :half]], axis=1)
    return values * cosine + swapped * sine


def attend_kernel(
    got, lengths, frequencies, near, far, gain, latents, ropes,
    out, cache, cache_rope, sums, lifted, turned, scored, weights, means, sems,
    *, factor, nope,
):
    kv = lax.axis_index(KV)
    tp = lax.axis_index("tp")
    kv_size = lax.axis_size(KV)
    groups = lax.axis_size("tp")
    local, positions, latent_width = cache.shape
    width = cache_rope.shape[1]
    copies = []
    for s in range(local):
        a = pltpu.make_async_copy(latents.at[s], cache.at[s], sems.at[s])
        b = pltpu.make_async_copy(ropes.at[s], cache_rope.at[s], sems.at[local + s])
        a.start()
        b.start()
        copies.append((a, b))
    for h in range(groups):
        total = got[h].astype(F32)
        for k in range(1, kv_size):
            total = total + got[k * groups + h].astype(F32)
        sums[h] = total
    shape = (local, lengths.shape[1])
    length = jnp.sum(
        jnp.where(lanes(shape) == rows(shape) + tp * local, lengths[...], 0), axis=1, keepdims=True
    )
    lane = lanes((local, width))
    angles = length.astype(F32) * frequencies[...]
    cosine = jnp.cos(angles)
    sine = jnp.sin(angles)
    sine = jnp.where(lane < width // 2, -sine, sine)
    half = groups // 2
    y = tp // 2
    core = lax.rem(tp, 2)
    for i in range(groups):
        step = (0, half - 1, 1, 2)[i % half]
        head = 2 * lax.rem(y + step, half) + (core if i < half else 1 - core)
        q = sums[head]
        w = near if i < half else far
        lifted[i] = dot(q[:, :nope].astype(BF16), w[i % half, :latent_width, :], NT)
        turned[i] = rotate(q[:, nope : nope + width].astype(BF16).astype(F32), cosine, sine)
    raw = jnp.concatenate([sums[h][0:1, nope + width :] for h in range(groups)], axis=1)
    rope_raw = sums[0][1:2, nope + width :]
    for h in range(1, groups):
        rope_raw = rope_raw + sums[h][1:2, nope + width :]
    square = jnp.sum(raw * raw, axis=1, keepdims=True) / latent_width
    new_latent = (raw * lax.rsqrt(square + EPSILON) * gain[...]).astype(BF16).astype(F32)
    new_seq = lax.rem(kv, local)
    mine = rows((local, width)) == new_seq
    new_rope = rotate(
        rope_raw,
        jnp.sum(jnp.where(mine, cosine, 0.0), axis=0, keepdims=True),
        jnp.sum(jnp.where(mine, sine, 0.0), axis=0, keepdims=True),
    )
    new_rope = new_rope.astype(BF16).astype(F32)
    pairs = local * groups
    for s in range(local):
        q = lifted[:, s, :].astype(BF16)
        qr = turned[:, s, :].astype(BF16)
        fresh = jnp.sum(q.astype(F32) * new_latent, axis=1, keepdims=True) + jnp.sum(
            qr.astype(F32) * new_rope, axis=1, keepdims=True
        )
        for copy in copies[s]:
            copy.wait()
        r = s * groups
        scored[r : r + groups, :positions] = dot(q, cache[s], NT) + dot(qr, cache_rope[s], NN)
        scored[r : r + groups, positions:] = jnp.broadcast_to(fresh, (groups, 128))
    scores = scored[:, :positions] * factor
    row = rows((pairs, 1))
    sequence = row // groups
    limit = jnp.zeros((pairs, 1), jnp.int32)
    for s in range(local):
        limit = jnp.where(sequence == s, length[s : s + 1, :], limit)
    is_new = jnp.logical_and(sequence == new_seq, kv < local)
    new = jnp.where(is_new, scored[:, positions : positions + 1] * factor, NEGATIVE)
    visible = kv * positions + lanes((pairs, positions)) < limit
    top = jnp.max(jnp.where(visible, scores, NEGATIVE), axis=1, keepdims=True)
    top = jnp.maximum(top, new)
    weight = jnp.where(visible, jnp.exp(scores - top), 0.0)
    new_weight = jnp.where(is_new, jnp.exp(new - top), 0.0)
    total = jnp.sum(weight, axis=1, keepdims=True) + new_weight
    weights[...] = weight.astype(BF16)
    some = total > 0.0
    safe = jnp.where(some, total, 1.0)
    inverse = 1.0 / safe
    logs = jnp.where(some, top + jnp.log(safe), NEGATIVE)
    rounded = new_weight.astype(BF16).astype(F32)
    for s in range(local):
        r = slice(s * groups, (s + 1) * groups)
        mixed = dot(weights[r, :], cache[s], NN) + rounded[r] * new_latent
        means[s] = mixed * inverse[r]
    for i in range(groups):
        w = near if i < half else far
        x = means[:, i, :].astype(BF16)
        up = dot(x, w[i % half, latent_width : 2 * latent_width, :], NN).astype(BF16)
        for k in range(kv_size):
            out[k, i * local : (i + 1) * local, :] = up
    lane = lanes((local, 128))
    table = jnp.zeros((groups, 128), F32)
    for s in range(local):
        table = jnp.where(lanes((groups, 128)) == s, logs[s * groups : (s + 1) * groups], table)
    table = jnp.concatenate([table, jnp.zeros((128 - groups, 128), F32)], axis=0)
    table = jnp.transpose(table)[:local]
    high = table.astype(BF16).astype(F32)
    rest = table - high
    middle = rest.astype(BF16).astype(F32)
    low = (rest - middle).astype(BF16).astype(F32)
    packed = jnp.where(
        lane < groups,
        high,
        jnp.where(
            lane < 2 * groups,
            pltpu.roll(middle, groups, 1),
            jnp.where(lane < 3 * groups, pltpu.roll(low, 2 * groups, 1), 0.0),
        ),
    ).astype(BF16)
    for k in range(kv_size):
        out[k, groups * local :, :] = packed


def combine_kernel(got, near, far, out, *, kv_size, groups, local, first):
    logs = []
    for k in range(kv_size):
        x = got[k, groups * local :, :].astype(F32)
        logs.append(x + pltpu.roll(x, 128 - groups, 1) + pltpu.roll(x, 128 - 2 * groups, 1))
    top = functools.reduce(jnp.maximum, logs)
    shares = [jnp.exp(x - top) for x in logs]
    total = functools.reduce(jnp.add, shares)
    inverse = 1.0 / total
    shares = [x * inverse for x in shares]
    half = groups // 2
    mixed = jnp.zeros((local, out.shape[2]), F32)
    for i in range(groups):
        head = jnp.zeros((local, 128), F32)
        for k in range(kv_size):
            part = got[k, i * local : (i + 1) * local, :].astype(F32)
            head = head + part * shares[k][:, i : i + 1]
        w = near if i < half else far
        mixed = mixed + dot(head.astype(BF16), w[i % half, first:, :], NN)
    mixed = mixed.astype(BF16)
    for d in range(out.shape[0]):
        out[d] = mixed


def finish_kernel(got, gain, out, *, kv_size, groups, local):
    kv = lax.axis_index(KV)
    width = got.shape[2]
    for t in range(groups):
        squares = jnp.zeros((local, width), F32)
        for k in range(kv_size):
            x = got[k * groups + t].astype(F32)
            squares = squares + x * x
        mean = jnp.sum(squares, axis=1, keepdims=True) / (width * kv_size)
        own = got[kv * groups + t].astype(F32)
        out[t * local : (t + 1) * local, :] = (
            own * lax.rsqrt(mean + EPSILON) * gain[...]
        ).astype(BF16)


def exchange(value, axes):
    return lax.all_to_all(value, axes, split_axis=0, concat_axis=0, tiled=True)


def on_device(
    tokens,
    token_gain,
    w_query,
    w_down_kv,
    w_rope_key,
    latent_gain,
    w_key_up,
    w_value_up,
    w_out,
    out_gain,
    cache_latent,
    cache_rope,
    lengths,
):
    kv_size = lax.axis_size(KV)
    groups = lax.axis_size("tp")
    everyone = kv_size * groups
    seqs, width = tokens.shape
    local, positions, latent_width = cache_latent.shape
    rope = cache_rope.shape[2]
    nope = w_key_up.shape[2]
    value = w_value_up.shape[2]
    factor = (nope + rope) ** (-0.5)

    sent, own = pl.pallas_call(
        project_kernel,
        out_shape=(
            jax.ShapeDtypeStruct((everyone, local, 256), BF16),
            jax.ShapeDtypeStruct((2 * latent_width + value, nope), BF16),
        ),
        in_specs=[in_hbm()] * 8,
        out_specs=(in_vmem(),) * 2,
        scratch_shapes=[
            pltpu.VMEM((seqs, width), BF16),
            pltpu.VMEM((1, width), F32),
            pltpu.VMEM((nope + rope, width), BF16),
            pltpu.VMEM((width, latent_width), BF16),
            pltpu.VMEM((rope, width), BF16),
            pltpu.SemaphoreType.DMA((8,)),
        ],
        compiler_params=params(8),
        name="project",
    )(
        *keep_in_hbm(
            tokens,
            token_gain[None],
            w_query.T,
            w_down_kv,
            w_rope_key.T,
            w_key_up,
            w_value_up,
            w_out,
        )
    )

    collected = [own]
    for step in (1, 3, 2):
        collected.append(
            lax.ppermute(own, "tp", [(i, (i + 2 * step) % groups) for i in range(groups)])
        )
    near = jnp.stack(collected)
    far = lax.ppermute(near, "tp", [(i, i ^ 1) for i in range(groups)])

    got = exchange(sent, ALL)
    powers = np.arange(0, rope, 2, dtype=np.float64) / rope
    frequencies = np.tile(1.0 / 10000.0**powers, 2)[None].astype(np.float32)
    sent = pl.pallas_call(
        functools.partial(attend_kernel, factor=factor, nope=nope),
        out_shape=jax.ShapeDtypeStruct((kv_size, groups * local + local, value), BF16),
        in_specs=[in_vmem()] * 6 + [in_hbm()] * 2,
        out_specs=in_vmem(),
        scratch_shapes=[
            pltpu.VMEM((local, positions, latent_width), BF16),
            pltpu.VMEM((local, rope, positions), BF16),
            pltpu.VMEM((groups, local, 256), F32),
            pltpu.VMEM((groups, local, latent_width), F32),
            pltpu.VMEM((groups, local, rope), F32),
            pltpu.VMEM((local * groups, positions + 128), F32),
            pltpu.VMEM((local * groups, positions), BF16),
            pltpu.VMEM((local, groups, latent_width), F32),
            pltpu.SemaphoreType.DMA((2 * local,)),
        ],
        compiler_params=params(24),
        name="attend",
    )(
        got,
        lengths[None],
        frequencies,
        near,
        far,
        latent_gain[None],
        *keep_in_hbm(cache_latent, cache_rope.transpose(0, 2, 1)),
    )
    got = exchange(sent, KV)

    sent = pl.pallas_call(
        functools.partial(
            combine_kernel,
            kv_size=kv_size,
            groups=groups,
            local=local,
            first=2 * latent_width,
        ),
        out_shape=jax.ShapeDtypeStruct((everyone, local, w_out.shape[1]), BF16),
        in_specs=[in_vmem()] * 3,
        out_specs=in_vmem(),
        compiler_params=params(8),
        name="combine",
    )(got, near, far)
    got = exchange(sent, ALL)
    return pl.pallas_call(
        functools.partial(finish_kernel, kv_size=kv_size, groups=groups, local=local),
        out_shape=jax.ShapeDtypeStruct((seqs, w_out.shape[1]), BF16),
        in_specs=[in_vmem(), in_vmem()],
        out_specs=in_vmem(),
        compiler_params=params(8),
        name="finish",
    )(got, out_gain[None])


def solution(mesh):
    finer = Mesh(mesh.devices.reshape(4, 4, mesh.shape["tp"]), ("kv_0", "kv_1", "tp"))

    return jax.shard_map(
        on_device,
        mesh=finer,
        in_specs=(
            P(None, KV),
            P(KV),
            P(KV, "tp"),
            P(KV, None),
            P(KV, None),
            P(),
            P("tp", None, None),
            P("tp", None, None),
            P("tp", KV),
            P(KV),
            P("tp", KV, None),
            P("tp", KV, None),
            P(),
        ),
        out_specs=P(None, KV),
        check_vma=False,
    )
```

```python
import functools

import jax
import jax.numpy as jnp
import numpy as np
from jax import lax
from jax.experimental import pallas as pl
from jax.experimental.pallas import tpu as pltpu
from jax.sharding import Mesh
from jax.sharding import PartitionSpec as P


KV = ("kv_0", "kv_1")
ALL = ("kv_0", "kv_1", "tp")
LAST = ("kv_1", "tp")
EPSILON = 1e-06
NEGATIVE = -1e30
F32 = jnp.float32
BF16 = jnp.bfloat16

NT = (((1,), (1,)), ((), ()))
NN = (((1,), (0,)), ((), ()))


def dot(a, b, dims):
    return lax.dot_general(a, b, dims, preferred_element_type=F32)


def params(mib):
    return pltpu.CompilerParams(vmem_limit_bytes=mib * 1024 * 1024)


def in_vmem():
    return pl.BlockSpec(memory_space=pltpu.VMEM)


def in_hbm():
    return pl.BlockSpec(memory_space=pltpu.HBM)


def keep_in_hbm(*arrays):
    return [pltpu.with_memory_space_constraint(x, pltpu.HBM) for x in arrays]


def lanes(shape):
    return lax.broadcasted_iota(jnp.int32, shape, 1)


def rows(shape):
    return lax.broadcasted_iota(jnp.int32, shape, 0)


def project_kernel(
    tokens, gain, wq, wd, wr, wk, wv, out, own, tokens_, gain_, wq_, wd_, wr_, sems
):
    tp = lax.axis_index("tp")
    groups = lax.axis_size("tp")
    kv_size = lax.axis_size(KV)
    deep = wk.shape[1]
    pairs = (
        (tokens, tokens_),
        (gain, gain_),
        (wq, wq_),
        (wd, wd_),
        (wr, wr_),
        (wk.at[0], own.at[pl.ds(0, deep)]),
        (wv.at[0], own.at[pl.ds(deep, deep)]),
    )
    copies = [pltpu.make_async_copy(x, y, sems.at[n]) for n, (x, y) in enumerate(pairs)]
    for copy in copies:
        copy.start()
    for copy in copies[:5]:
        copy.wait()
    scaled = (tokens_[...].astype(F32) * gain_[...]).astype(BF16)
    query = dot(scaled, wq_[...], NT)
    latent = dot(scaled, wd_[...], NN)
    rope = dot(scaled, wr_[...], NT)
    seqs = scaled.shape[0]
    local = seqs // groups
    chunk = latent.shape[1] // groups
    part = latent[:, :chunk]
    for g in range(1, groups):
        part = jnp.where(tp == g, latent[:, g * chunk : (g + 1) * chunk], part)
    width = rope.shape[1]
    rope = jnp.where(lanes(rope.shape) // (width // groups) == tp, rope, 0.0)
    blank = jnp.zeros((seqs, 128 - width), F32)
    part = jnp.concatenate([blank, part], axis=1)
    rope = jnp.concatenate([blank, rope], axis=1)
    first = query[:, :128].astype(BF16)
    second = jnp.concatenate([query[:, 128:], blank], axis=1)
    row = rows((local, 128))
    for t in range(groups):
        top = first[t * local : (t + 1) * local]
        low = second[t * local : (t + 1) * local]
        for j in range(local):
            r = t * local + j
            new = jnp.where(row == 0, part[r : r + 1], 0.0) + jnp.where(row == 1, rope[r : r + 1], 0.0)
            tile = (low + new).astype(BF16)
            for c in range(kv_size // local):
                b = (c * local + j) * groups + t
                out[b, :, :128] = top
                out[b, :, 128:] = tile
    for copy in copies[5:]:
        copy.wait()


def rotate(values, cosine, sine):
    half = values.shape[1] // 2
    swapped = jnp.concatenate([values[:, half:], values[:, :half]], axis=1)
    return values * cosine + swapped * sine


def attend_kernel(
    got, near, far, lengths_, frequencies_, gain_, latents, ropes,
    out, lengths, frequencies, gain, cache, cache_rope,
    sums, lifted, turned, scored, weights, means, sems,
    *, factor, nope,
):
    kv = lax.axis_index(KV)
    tp = lax.axis_index("tp")
    kv_size = lax.axis_size(KV)
    groups = lax.axis_size("tp")
    local, positions, latent_width = cache.shape
    width = cache_rope.shape[1]
    small = []
    for n, (a, b) in enumerate(
        ((lengths_, lengths), (frequencies_, frequencies), (gain_, gain))
    ):
        small.append(pltpu.make_async_copy(a, b, sems.at[2 * local + n]))
        small[n].start()
    copies = []
    for s in range(local):
        a = pltpu.make_async_copy(latents.at[s], cache.at[s], sems.at[s])
        b = pltpu.make_async_copy(ropes.at[s], cache_rope.at[s], sems.at[local + s])
        a.start()
        b.start()
        copies.append((a, b))
    for h in range(groups):
        total = got[h].astype(F32)
        for k in range(1, kv_size):
            total = total + got[k * groups + h].astype(F32)
        sums[h] = total
    for copy in small:
        copy.wait()
    shape = (local, lengths.shape[1])
    length = jnp.sum(
        jnp.where(lanes(shape) == rows(shape) + tp * local, lengths[...], 0), axis=1, keepdims=True
    )
    lane = lanes((local, width))
    angles = length.astype(F32) * frequencies[...]
    cosine = jnp.cos(angles)
    sine = jnp.sin(angles)
    sine = jnp.where(lane < width // 2, -sine, sine)
    half = groups // 2
    y = tp // 2
    core = lax.rem(tp, 2)
    for i in range(groups):
        step = (0, half - 1, 1, 2)[i % half]
        head = 2 * lax.rem(y + step, half) + (core if i < half else 1 - core)
        q = sums[head]
        w = near if i < half else far
        lifted[i] = dot(q[:, :nope].astype(BF16), w[i % half, :latent_width, :], NT)
        turned[i] = rotate(q[:, nope : nope + width].astype(BF16).astype(F32), cosine, sine)
    raw = jnp.concatenate([sums[h][0:1, nope + width :] for h in range(groups)], axis=1)
    rope_raw = sums[0][1:2, nope + width :]
    for h in range(1, groups):
        rope_raw = rope_raw + sums[h][1:2, nope + width :]
    square = jnp.sum(raw * raw, axis=1, keepdims=True) / latent_width
    new_latent = (raw * lax.rsqrt(square + EPSILON) * gain[...]).astype(BF16).astype(F32)
    new_seq = lax.rem(kv, local)
    mine = rows((local, width)) == new_seq
    new_rope = rotate(
        rope_raw,
        jnp.sum(jnp.where(mine, cosine, 0.0), axis=0, keepdims=True),
        jnp.sum(jnp.where(mine, sine, 0.0), axis=0, keepdims=True),
    )
    new_rope = new_rope.astype(BF16).astype(F32)
    pairs = local * groups
    for s in range(local):
        q = lifted[:, s, :].astype(BF16)
        qr = turned[:, s, :].astype(BF16)
        fresh = jnp.sum(q.astype(F32) * new_latent, axis=1, keepdims=True) + jnp.sum(
            qr.astype(F32) * new_rope, axis=1, keepdims=True
        )
        for copy in copies[s]:
            copy.wait()
        r = s * groups
        scored[r : r + groups, :positions] = dot(q, cache[s], NT) + dot(qr, cache_rope[s], NN)
        scored[r : r + groups, positions:] = jnp.broadcast_to(fresh, (groups, 128))
    scores = scored[:, :positions] * factor
    row = rows((pairs, 1))
    sequence = row // groups
    limit = jnp.zeros((pairs, 1), jnp.int32)
    for s in range(local):
        limit = jnp.where(sequence == s, length[s : s + 1, :], limit)
    is_new = jnp.logical_and(sequence == new_seq, kv < local)
    new = jnp.where(is_new, scored[:, positions : positions + 1] * factor, NEGATIVE)
    visible = kv * positions + lanes((pairs, positions)) < limit
    top = jnp.max(jnp.where(visible, scores, NEGATIVE), axis=1, keepdims=True)
    top = jnp.maximum(top, new)
    weight = jnp.where(visible, jnp.exp(scores - top), 0.0)
    new_weight = jnp.where(is_new, jnp.exp(new - top), 0.0)
    total = jnp.sum(weight, axis=1, keepdims=True) + new_weight
    weights[...] = weight.astype(BF16)
    some = total > 0.0
    safe = jnp.where(some, total, 1.0)
    inverse = 1.0 / safe
    logs = jnp.where(some, top + jnp.log(safe), NEGATIVE)
    rounded = new_weight.astype(BF16).astype(F32)
    for s in range(local):
        r = slice(s * groups, (s + 1) * groups)
        mixed = dot(weights[r, :], cache[s], NN) + rounded[r] * new_latent
        means[s] = mixed * inverse[r]
    for i in range(groups):
        w = near if i < half else far
        x = means[:, i, :].astype(BF16)
        up = dot(x, w[i % half, latent_width : 2 * latent_width, :], NN).astype(BF16)
        for k in range(kv_size):
            out[k, i * local : (i + 1) * local, :] = up
    lane = lanes((local, 128))
    table = jnp.zeros((groups, 128), F32)
    for s in range(local):
        table = jnp.where(lanes((groups, 128)) == s, logs[s * groups : (s + 1) * groups], table)
    table = jnp.concatenate([table, jnp.zeros((128 - groups, 128), F32)], axis=0)
    table = jnp.transpose(table)[:local]
    high = table.astype(BF16).astype(F32)
    rest = table - high
    middle = rest.astype(BF16).astype(F32)
    low = (rest - middle).astype(BF16).astype(F32)
    packed = jnp.where(
        lane < groups,
        high,
        jnp.where(
            lane < 2 * groups,
            pltpu.roll(middle, groups, 1),
            jnp.where(lane < 3 * groups, pltpu.roll(low, 2 * groups, 1), 0.0),
        ),
    ).astype(BF16)
    for k in range(kv_size):
        out[k, groups * local :, :] = packed


def three_parts(value):
    high = value.astype(BF16).astype(F32)
    rest = value - high
    middle = rest.astype(BF16).astype(F32)
    low = (rest - middle).astype(BF16).astype(F32)
    return high, middle, low


def combine_kernel(got, near, far, out, *, kv_size, groups, local):
    logs = []
    for k in range(kv_size):
        x = got[k, groups * local :, :].astype(F32)
        logs.append(x + pltpu.roll(x, 128 - groups, 1) + pltpu.roll(x, 128 - 2 * groups, 1))
    top = functools.reduce(jnp.maximum, logs)
    shares = [jnp.exp(x - top) for x in logs]
    total = functools.reduce(jnp.add, shares)
    inverse = 1.0 / total
    shares = [x * inverse for x in shares]
    half = groups // 2
    blocks = near.shape[1]
    mixed = [jnp.zeros((local, out.shape[2]), F32) for _ in range(blocks)]
    for i in range(groups):
        head = jnp.zeros((local, 128), F32)
        for k in range(kv_size):
            part = got[k, i * local : (i + 1) * local, :].astype(F32)
            head = head + part * shares[k][:, i : i + 1]
        head = head.astype(BF16)
        w = near if i < half else far
        for n in range(blocks):
            mixed[n] = mixed[n] + dot(head, w[i % half, n], NN)
    squares = functools.reduce(jnp.add, [x * x for x in mixed])
    squares = jnp.sum(squares, axis=1, keepdims=True)
    high, middle, low = three_parts(squares)
    lane = lanes((local, out.shape[2]))
    parts = jnp.where(
        lane == 0, high, jnp.where(lane == 1, middle, jnp.where(lane == 2, low, 0.0))
    ).astype(BF16)
    own = mixed[0].astype(BF16)
    for d in range(out.shape[0]):
        out[d, :local, :] = own
        out[d, local:, :] = parts


def finish_kernel(got, gain, out, *, groups, local, model_width):
    place = lax.axis_index(KV[1])
    places = got.shape[0] // groups
    for t in range(groups):
        parts = functools.reduce(
            jnp.add, [got[n * groups + t, local:, :].astype(F32) for n in range(places)]
        )
        mean = jnp.sum(parts, axis=1, keepdims=True) / model_width
        own = got[place * groups + t, :local, :].astype(F32)
        out[t * local : (t + 1) * local, :] = (
            own * lax.rsqrt(mean + EPSILON) * gain[...]
        ).astype(BF16)


def exchange(value, axes):
    return lax.all_to_all(value, axes, split_axis=0, concat_axis=0, tiled=True)


def swap(value):
    return lax.ppermute(value, "tp", [(i, i ^ 1) for i in range(lax.axis_size("tp"))])


def along(own, axis, stride):
    size = lax.axis_size(axis)
    collected = [own]
    for step in (1, 3, 2):
        pairs = [(i, (i + stride * step) % size) for i in range(size)]
        collected.append(lax.ppermute(own, axis, pairs))
    return jnp.stack(collected)


def on_device(
    tokens,
    token_gain,
    w_query,
    w_down_kv,
    w_rope_key,
    latent_gain,
    w_key_up,
    w_value_up,
    w_out,
    out_gain,
    cache_latent,
    cache_rope,
    lengths,
):
    kv_size = lax.axis_size(KV)
    groups = lax.axis_size("tp")
    everyone = kv_size * groups
    seqs, width = tokens.shape
    local, positions, latent_width = cache_latent.shape
    rope = cache_rope.shape[2]
    nope = w_key_up.shape[2]
    value = w_value_up.shape[2]
    factor = (nope + rope) ** (-0.5)

    sent, own = pl.pallas_call(
        project_kernel,
        out_shape=(
            jax.ShapeDtypeStruct((everyone, local, 256), BF16),
            jax.ShapeDtypeStruct((2 * latent_width, nope), BF16),
        ),
        in_specs=[in_hbm()] * 7,
        out_specs=(in_vmem(),) * 2,
        scratch_shapes=[
            pltpu.VMEM((seqs, width), BF16),
            pltpu.VMEM((1, width), F32),
            pltpu.VMEM((nope + rope, width), BF16),
            pltpu.VMEM((width, latent_width), BF16),
            pltpu.VMEM((rope, width), BF16),
            pltpu.SemaphoreType.DMA((7,)),
        ],
        compiler_params=params(8),
        name="project",
    )(
        *keep_in_hbm(
            tokens,
            token_gain[None],
            w_query.T,
            w_down_kv,
            w_rope_key.T,
            w_key_up,
            w_value_up,
        )
    )

    near = along(own, "tp", 2)
    far = swap(near)
    columns = along(w_out, "kv_0", 1)
    near_out = along(columns, "tp", 2)
    far_out = swap(near_out)

    got = exchange(sent, ALL)
    powers = np.arange(0, rope, 2, dtype=np.float64) / rope
    frequencies = np.tile(1.0 / 10000.0**powers, 2)[None].astype(np.float32)
    sent = pl.pallas_call(
        functools.partial(attend_kernel, factor=factor, nope=nope),
        out_shape=jax.ShapeDtypeStruct((kv_size, groups * local + local, value), BF16),
        in_specs=[in_vmem()] * 3 + [in_hbm()] * 5,
        out_specs=in_vmem(),
        scratch_shapes=[
            pltpu.VMEM((1, seqs), jnp.int32),
            pltpu.VMEM((1, rope), F32),
            pltpu.VMEM((1, latent_width), F32),
            pltpu.VMEM((local, positions, latent_width), BF16),
            pltpu.VMEM((local, rope, positions), BF16),
            pltpu.VMEM((groups, local, 256), F32),
            pltpu.VMEM((groups, local, latent_width), F32),
            pltpu.VMEM((groups, local, rope), F32),
            pltpu.VMEM((local * groups, positions + 128), F32),
            pltpu.VMEM((local * groups, positions), BF16),
            pltpu.VMEM((local, groups, latent_width), F32),
            pltpu.SemaphoreType.DMA((2 * local + 3,)),
        ],
        compiler_params=params(24),
        name="attend",
    )(
        got,
        near,
        far,
        *keep_in_hbm(
            lengths[None],
            frequencies,
            latent_gain[None],
            cache_latent,
            cache_rope.transpose(0, 2, 1),
        ),
    )
    got = exchange(sent, KV)

    fewer = lax.axis_size(LAST)
    sent = pl.pallas_call(
        functools.partial(combine_kernel, kv_size=kv_size, groups=groups, local=local),
        out_shape=jax.ShapeDtypeStruct((fewer, 2 * local, w_out.shape[1]), BF16),
        in_specs=[in_vmem()] * 3,
        out_specs=in_vmem(),
        compiler_params=params(8),
        name="combine",
    )(got, near_out, far_out)
    got = exchange(sent, LAST)
    return pl.pallas_call(
        functools.partial(
            finish_kernel, groups=groups, local=local, model_width=width * kv_size
        ),
        out_shape=jax.ShapeDtypeStruct((seqs, w_out.shape[1]), BF16),
        in_specs=[in_vmem(), in_vmem()],
        out_specs=in_vmem(),
        compiler_params=params(8),
        name="finish",
    )(got, out_gain[None])


def solution(mesh):
    finer = Mesh(mesh.devices.reshape(4, 4, mesh.shape["tp"]), ("kv_0", "kv_1", "tp"))

    return jax.shard_map(
        on_device,
        mesh=finer,
        in_specs=(
            P(None, KV),
            P(KV),
            P(KV, "tp"),
            P(KV, None),
            P(KV, None),
            P(),
            P("tp", None, None),
            P("tp", None, None),
            P("tp", KV),
            P(KV),
            P("tp", KV, None),
            P("tp", KV, None),
            P(),
        ),
        out_specs=P(None, KV),
        check_vma=False,
    )
```

```python
import functools

import jax
import jax.numpy as jnp
import numpy as np
from jax import lax
from jax.experimental import pallas as pl
from jax.experimental.pallas import tpu as pltpu
from jax.sharding import Mesh
from jax.sharding import PartitionSpec as P


KV = ("kv_0", "kv_1")
ALL = ("kv_0", "kv_1", "tp")
EPSILON = 1e-06
NEGATIVE = -1e30
F32 = jnp.float32
BF16 = jnp.bfloat16

NT = (((1,), (1,)), ((), ()))
NN = (((1,), (0,)), ((), ()))


def dot(a, b, dims):
    return lax.dot_general(a, b, dims, preferred_element_type=F32)


def params(mib):
    return pltpu.CompilerParams(vmem_limit_bytes=mib * 1024 * 1024)


def in_vmem():
    return pl.BlockSpec(memory_space=pltpu.VMEM)


def in_hbm():
    return pl.BlockSpec(memory_space=pltpu.HBM)


def keep_in_hbm(*arrays):
    return [pltpu.with_memory_space_constraint(x, pltpu.HBM) for x in arrays]


def lanes(shape):
    return lax.broadcasted_iota(jnp.int32, shape, 1)


def rows(shape):
    return lax.broadcasted_iota(jnp.int32, shape, 0)


def collect_kernel(
    tokens_, gain_, wd_, wr_, wk, wv, wo, tokens, gain, wd, wr, own, sems
):
    deep = wk.shape[1]
    pairs = (
        (wk.at[0], own.at[pl.ds(0, deep)]),
        (wv.at[0], own.at[pl.ds(deep, deep)]),
        (wo, own.at[pl.ds(2 * deep, wo.shape[0])]),
        (tokens_, tokens),
        (gain_, gain),
        (wd_, wd),
        (wr_, wr),
    )
    copies = [pltpu.make_async_copy(x, y, sems.at[n]) for n, (x, y) in enumerate(pairs)]
    for copy in copies:
        copy.start()
    for copy in copies:
        copy.wait()


def project_kernel(tokens, gain, near, far, wd, wr, out, news):
    tp = lax.axis_index("tp")
    groups = lax.axis_size("tp")
    local = tokens.shape[0] // groups
    half = groups // 2
    width = wr.shape[0]
    mine = tokens[pl.ds(pl.multiple_of(tp * local, local), local), :]
    scaled = (mine.astype(F32) * gain[...]).astype(BF16)
    latent = dot(scaled, wd[...], NN)
    rope = dot(scaled, wr[...], NT)
    pieces = latent.shape[1] // 128
    for n in range(pieces):
        news[n] = latent[:, n * 128 : (n + 1) * 128]
    news[pieces] = jnp.concatenate([rope, jnp.zeros((local, 128 - width), F32)], axis=1)
    for n in range(pieces + 1, local):
        news[n] = jnp.zeros((local, 128), F32)
    queries = [
        dot(scaled, (near if i < half else far)[i % half], NT) for i in range(groups)
    ]
    tiles = [q[:, :128].astype(BF16) for q in queries] + [
        jnp.concatenate([queries[i][:, 128:], queries[i + half][:, 128:]], axis=1).astype(BF16)
        for i in range(half)
    ]
    copies = out.shape[0] // local
    for j in range(local):
        new = news[:, j, :].astype(BF16)
        for c in range(copies):
            k = c * local + j
            for n, tile in enumerate(tiles):
                out[k, n * local : (n + 1) * local, :] = tile
            out[k, len(tiles) * local :, :] = new


def rotate(values, cosine, sine):
    half = values.shape[1] // 2
    swapped = jnp.concatenate([values[:, half:], values[:, :half]], axis=1)
    return values * cosine + swapped * sine


def attend_kernel(
    got, near, far, lengths_, frequencies_, gain_, latents, ropes,
    out, lengths, frequencies, gain, cache, cache_rope,
    lifted, turned, scored, weights, means, sems,
    *, factor, nope,
):
    kv = lax.axis_index(KV)
    tp = lax.axis_index("tp")
    kv_size = lax.axis_size(KV)
    groups = lax.axis_size("tp")
    local, positions, latent_width = cache.shape
    width = cache_rope.shape[1]
    small = []
    for n, (a, b) in enumerate(
        ((lengths_, lengths), (frequencies_, frequencies), (gain_, gain))
    ):
        small.append(pltpu.make_async_copy(a, b, sems.at[2 * local + n]))
        small[n].start()
    copies = []
    for s in range(local):
        a = pltpu.make_async_copy(latents.at[s], cache.at[s], sems.at[s])
        b = pltpu.make_async_copy(ropes.at[s], cache_rope.at[s], sems.at[local + s])
        a.start()
        b.start()
        copies.append((a, b))
    def total(n):
        rows_of = slice(n * local, (n + 1) * local)
        result = got[0, rows_of, :].astype(F32)
        for k in range(1, kv_size):
            result = result + got[k, rows_of, :].astype(F32)
        return result

    for copy in small:
        copy.wait()
    shape = (local, lengths.shape[1])
    length = jnp.sum(
        jnp.where(lanes(shape) == rows(shape) + tp * local, lengths[...], 0), axis=1, keepdims=True
    )
    lane = lanes((local, width))
    angles = length.astype(F32) * frequencies[...]
    cosine = jnp.cos(angles)
    sine = jnp.sin(angles)
    sine = jnp.where(lane < width // 2, -sine, sine)
    half = groups // 2
    for i in range(groups):
        w = near if i < half else far
        lifted[i] = dot(total(i).astype(BF16), w[i % half, :latent_width, :], NT)
    for i in range(half):
        both = total(groups + i).astype(BF16).astype(F32)
        turned[i] = rotate(both[:, :width], cosine, sine)
        turned[i + half] = rotate(both[:, width:], cosine, sine)
    fresh = total(groups + half)
    pieces = latent_width // nope
    raw = jnp.concatenate([fresh[n : n + 1] for n in range(pieces)], axis=1)
    rope_raw = fresh[pieces : pieces + 1, :width]
    square = jnp.sum(raw * raw, axis=1, keepdims=True) / latent_width
    new_latent = (raw * lax.rsqrt(square + EPSILON) * gain[...]).astype(BF16).astype(F32)
    new_seq = lax.rem(kv, local)
    mine = rows((local, width)) == new_seq
    new_rope = rotate(
        rope_raw,
        jnp.sum(jnp.where(mine, cosine, 0.0), axis=0, keepdims=True),
        jnp.sum(jnp.where(mine, sine, 0.0), axis=0, keepdims=True),
    )
    new_rope = new_rope.astype(BF16).astype(F32)
    pairs = local * groups
    for s in range(local):
        q = lifted[:, s, :].astype(BF16)
        qr = turned[:, s, :].astype(BF16)
        fresh = jnp.sum(q.astype(F32) * new_latent, axis=1, keepdims=True) + jnp.sum(
            qr.astype(F32) * new_rope, axis=1, keepdims=True
        )
        for copy in copies[s]:
            copy.wait()
        r = s * groups
        scored[r : r + groups, :positions] = dot(q, cache[s], NT) + dot(qr, cache_rope[s], NN)
        scored[r : r + groups, positions:] = jnp.broadcast_to(fresh, (groups, 128))
    scores = scored[:, :positions] * factor
    row = rows((pairs, 1))
    sequence = row // groups
    limit = jnp.zeros((pairs, 1), jnp.int32)
    for s in range(local):
        limit = jnp.where(sequence == s, length[s : s + 1, :], limit)
    is_new = jnp.logical_and(sequence == new_seq, kv < local)
    new = jnp.where(is_new, scored[:, positions : positions + 1] * factor, NEGATIVE)
    visible = kv * positions + lanes((pairs, positions)) < limit
    top = jnp.max(jnp.where(visible, scores, NEGATIVE), axis=1, keepdims=True)
    top = jnp.maximum(top, new)
    weight = jnp.where(visible, jnp.exp(scores - top), 0.0)
    new_weight = jnp.where(is_new, jnp.exp(new - top), 0.0)
    total = jnp.sum(weight, axis=1, keepdims=True) + new_weight
    weights[...] = weight.astype(BF16)
    some = total > 0.0
    safe = jnp.where(some, total, 1.0)
    inverse = 1.0 / safe
    logs = jnp.where(some, top + jnp.log(safe), NEGATIVE)
    rounded = new_weight.astype(BF16).astype(F32)
    for s in range(local):
        r = slice(s * groups, (s + 1) * groups)
        mixed = dot(weights[r, :], cache[s], NN) + rounded[r] * new_latent
        means[s] = mixed * inverse[r]
    for i in range(groups):
        w = near if i < half else far
        x = means[:, i, :].astype(BF16)
        up = dot(x, w[i % half, latent_width : 2 * latent_width, :], NN).astype(BF16)
        for k in range(kv_size):
            out[k, i * local : (i + 1) * local, :] = up
    lane = lanes((local, 128))
    table = jnp.zeros((groups, 128), F32)
    for s in range(local):
        table = jnp.where(lanes((groups, 128)) == s, logs[s * groups : (s + 1) * groups], table)
    table = jnp.concatenate([table, jnp.zeros((128 - groups, 128), F32)], axis=0)
    table = jnp.transpose(table)[:local]
    high = table.astype(BF16).astype(F32)
    rest = table - high
    middle = rest.astype(BF16).astype(F32)
    low = (rest - middle).astype(BF16).astype(F32)
    packed = jnp.where(
        lane < groups,
        high,
        jnp.where(
            lane < 2 * groups,
            pltpu.roll(middle, groups, 1),
            jnp.where(lane < 3 * groups, pltpu.roll(low, 2 * groups, 1), 0.0),
        ),
    ).astype(BF16)
    for k in range(kv_size):
        out[k, groups * local :, :] = packed


def combine_kernel(got, near, far, out, *, kv_size, groups, local, first):
    logs = []
    for k in range(kv_size):
        x = got[k, groups * local :, :].astype(F32)
        logs.append(x + pltpu.roll(x, 128 - groups, 1) + pltpu.roll(x, 128 - 2 * groups, 1))
    top = functools.reduce(jnp.maximum, logs)
    shares = [jnp.exp(x - top) for x in logs]
    total = functools.reduce(jnp.add, shares)
    inverse = 1.0 / total
    shares = [x * inverse for x in shares]
    half = groups // 2
    mixed = jnp.zeros((local, out.shape[2]), F32)
    for i in range(groups):
        head = jnp.zeros((local, 128), F32)
        for k in range(kv_size):
            part = got[k, i * local : (i + 1) * local, :].astype(F32)
            head = head + part * shares[k][:, i : i + 1]
        w = near if i < half else far
        mixed = mixed + dot(head.astype(BF16), w[i % half, first:, :], NN)
    mixed = mixed.astype(BF16)
    for d in range(out.shape[0]):
        out[d] = mixed


def finish_kernel(got, gain, out, *, kv_size, groups, local):
    kv = lax.axis_index(KV)
    width = got.shape[2]
    for t in range(groups):
        squares = jnp.zeros((local, width), F32)
        for k in range(kv_size):
            x = got[k * groups + t].astype(F32)
            squares = squares + x * x
        mean = jnp.sum(squares, axis=1, keepdims=True) / (width * kv_size)
        own = got[kv * groups + t].astype(F32)
        out[t * local : (t + 1) * local, :] = (
            own * lax.rsqrt(mean + EPSILON) * gain[...]
        ).astype(BF16)


def exchange(value, axes):
    return lax.all_to_all(value, axes, split_axis=0, concat_axis=0, tiled=True)


def swap(value):
    return lax.ppermute(value, "tp", [(i, i ^ 1) for i in range(lax.axis_size("tp"))])


def along(own):
    size = lax.axis_size("tp")
    collected = [own]
    for step in (1, 3, 2):
        pairs = [(i, (i + 2 * step) % size) for i in range(size)]
        collected.append(lax.ppermute(own, "tp", pairs))
    return jnp.stack(collected)


def on_device(
    tokens,
    token_gain,
    w_query,
    w_down_kv,
    w_rope_key,
    latent_gain,
    w_key_up,
    w_value_up,
    w_out,
    out_gain,
    cache_latent,
    cache_rope,
    lengths,
):
    kv_size = lax.axis_size(KV)
    groups = lax.axis_size("tp")
    everyone = kv_size * groups
    seqs, width = tokens.shape
    local, positions, latent_width = cache_latent.shape
    rope = cache_rope.shape[2]
    nope = w_key_up.shape[2]
    value = w_value_up.shape[2]
    factor = (nope + rope) ** (-0.5)

    near_query = along(w_query.T)
    far_query = swap(near_query)
    tokens, gain, w_down, w_rope, own = pl.pallas_call(
        collect_kernel,
        out_shape=(
            jax.ShapeDtypeStruct(tokens.shape, BF16),
            jax.ShapeDtypeStruct((1, width), F32),
            jax.ShapeDtypeStruct(w_down_kv.shape, BF16),
            jax.ShapeDtypeStruct((rope, width), BF16),
            jax.ShapeDtypeStruct((2 * latent_width + value, nope), BF16),
        ),
        in_specs=[in_hbm()] * 7,
        out_specs=(in_vmem(),) * 5,
        scratch_shapes=[pltpu.SemaphoreType.DMA((7,))],
        compiler_params=params(8),
        name="collect",
    )(
        *keep_in_hbm(
            tokens,
            token_gain[None],
            w_down_kv,
            w_rope_key.T,
            w_key_up,
            w_value_up,
            w_out,
        )
    )
    near = along(own)
    far = swap(near)

    sent_rows = (groups + groups // 2 + 1) * local
    sent = pl.pallas_call(
        project_kernel,
        out_shape=jax.ShapeDtypeStruct((kv_size, sent_rows, 128), BF16),
        in_specs=[in_vmem()] * 6,
        out_specs=in_vmem(),
        scratch_shapes=[pltpu.VMEM((local, local, 128), F32)],
        compiler_params=params(8),
        name="project",
    )(tokens, gain, near_query, far_query, w_down, w_rope)
    got = exchange(sent, KV)
    powers = np.arange(0, rope, 2, dtype=np.float64) / rope
    frequencies = np.tile(1.0 / 10000.0**powers, 2)[None].astype(np.float32)
    sent = pl.pallas_call(
        functools.partial(attend_kernel, factor=factor, nope=nope),
        out_shape=jax.ShapeDtypeStruct((kv_size, groups * local + local, value), BF16),
        in_specs=[in_vmem()] * 3 + [in_hbm()] * 5,
        out_specs=in_vmem(),
        scratch_shapes=[
            pltpu.VMEM((1, seqs), jnp.int32),
            pltpu.VMEM((1, rope), F32),
            pltpu.VMEM((1, latent_width), F32),
            pltpu.VMEM((local, positions, latent_width), BF16),
            pltpu.VMEM((local, rope, positions), BF16),
            pltpu.VMEM((groups, local, latent_width), F32),
            pltpu.VMEM((groups, local, rope), F32),
            pltpu.VMEM((local * groups, positions + 128), F32),
            pltpu.VMEM((local * groups, positions), BF16),
            pltpu.VMEM((local, groups, latent_width), F32),
            pltpu.SemaphoreType.DMA((2 * local + 3,)),
        ],
        compiler_params=params(24),
        name="attend",
    )(
        got,
        near,
        far,
        *keep_in_hbm(
            lengths[None],
            frequencies,
            latent_gain[None],
            cache_latent,
            cache_rope.transpose(0, 2, 1),
        ),
    )
    got = exchange(sent, KV)

    sent = pl.pallas_call(
        functools.partial(
            combine_kernel,
            kv_size=kv_size,
            groups=groups,
            local=local,
            first=2 * latent_width,
        ),
        out_shape=jax.ShapeDtypeStruct((everyone, local, w_out.shape[1]), BF16),
        in_specs=[in_vmem()] * 3,
        out_specs=in_vmem(),
        compiler_params=params(8),
        name="combine",
    )(got, near, far)
    got = exchange(sent, ALL)
    return pl.pallas_call(
        functools.partial(finish_kernel, kv_size=kv_size, groups=groups, local=local),
        out_shape=jax.ShapeDtypeStruct((seqs, w_out.shape[1]), BF16),
        in_specs=[in_vmem(), in_vmem()],
        out_specs=in_vmem(),
        compiler_params=params(8),
        name="finish",
    )(got, out_gain[None])


def solution(mesh):
    finer = Mesh(mesh.devices.reshape(4, 4, mesh.shape["tp"]), ("kv_0", "kv_1", "tp"))

    return jax.shard_map(
        on_device,
        mesh=finer,
        in_specs=(
            P(None, KV),
            P(KV),
            P(KV, "tp"),
            P(KV, None),
            P(KV, None),
            P(),
            P("tp", None, None),
            P("tp", None, None),
            P("tp", KV),
            P(KV),
            P("tp", KV, None),
            P("tp", KV, None),
            P(),
        ),
        out_specs=P(None, KV),
        check_vma=False,
    )
```

```python
import functools

import jax
import jax.numpy as jnp
import numpy as np
from jax import lax
from jax.experimental import pallas as pl
from jax.experimental.pallas import tpu as pltpu
from jax.sharding import Mesh
from jax.sharding import PartitionSpec as P


KV = ("kv_0", "kv_1")
ALL = ("kv_0", "kv_1", "tp")
EPSILON = 1e-06
NEGATIVE = -1e30
F32 = jnp.float32
BF16 = jnp.bfloat16

NT = (((1,), (1,)), ((), ()))
NN = (((1,), (0,)), ((), ()))


def dot(a, b, dims):
    return lax.dot_general(a, b, dims, preferred_element_type=F32)


def params(mib):
    return pltpu.CompilerParams(vmem_limit_bytes=mib * 1024 * 1024)


def in_vmem():
    return pl.BlockSpec(memory_space=pltpu.VMEM)


def in_hbm():
    return pl.BlockSpec(memory_space=pltpu.HBM)


def keep_in_hbm(*arrays):
    return [pltpu.with_memory_space_constraint(x, pltpu.HBM) for x in arrays]


def lanes(shape):
    return lax.broadcasted_iota(jnp.int32, shape, 1)


def rows(shape):
    return lax.broadcasted_iota(jnp.int32, shape, 0)


def collect_kernel(
    tokens_, gain_, wd_, wr_, wq_, wk, wv, wo, tokens, gain, wd, wr, wq, own, sems
):
    deep = wk.shape[1]
    pairs = (
        (wk.at[0], own.at[pl.ds(0, deep)]),
        (wv.at[0], own.at[pl.ds(deep, deep)]),
        (wo, own.at[pl.ds(2 * deep, wo.shape[0])]),
        (tokens_, tokens),
        (gain_, gain),
        (wd_, wd),
        (wr_, wr),
        (wq_, wq),
    )
    copies = [pltpu.make_async_copy(x, y, sems.at[n]) for n, (x, y) in enumerate(pairs)]
    for copy in copies:
        copy.start()
    for copy in copies:
        copy.wait()


def project_kernel(tokens, gain, near, far, wd, wr, out, news):
    tp = lax.axis_index("tp")
    groups = lax.axis_size("tp")
    local = tokens.shape[0] // groups
    half = groups // 2
    width = wr.shape[0]
    mine = tokens[pl.ds(pl.multiple_of(tp * local, local), local), :]
    scaled = (mine.astype(F32) * gain[...]).astype(BF16)
    latent = dot(scaled, wd[...], NN)
    rope = dot(scaled, wr[...], NT)
    pieces = latent.shape[1] // 128
    for n in range(pieces):
        news[n] = latent[:, n * 128 : (n + 1) * 128]
    news[pieces] = jnp.concatenate([rope, jnp.zeros((local, 128 - width), F32)], axis=1)
    for n in range(pieces + 1, local):
        news[n] = jnp.zeros((local, 128), F32)
    queries = [
        dot(scaled, (near if i < half else far)[i % half], NT) for i in range(groups)
    ]
    tiles = [q[:, :128].astype(BF16) for q in queries] + [
        jnp.concatenate([queries[i][:, 128:], queries[i + half][:, 128:]], axis=1).astype(BF16)
        for i in range(half)
    ]
    copies = out.shape[0] // local
    for j in range(local):
        new = news[:, j, :].astype(BF16)
        for c in range(copies):
            k = c * local + j
            for n, tile in enumerate(tiles):
                out[k, n * local : (n + 1) * local, :] = tile
            out[k, len(tiles) * local :, :] = new


def rotate(values, cosine, sine):
    half = values.shape[1] // 2
    swapped = jnp.concatenate([values[:, half:], values[:, :half]], axis=1)
    return values * cosine + swapped * sine


def attend_kernel(
    got, near, far, lengths_, frequencies_, gain_, latents, ropes,
    out, lengths, frequencies, gain, cache, cache_rope,
    lifted, turned, scored, weights, means, sems,
    *, factor, nope,
):
    kv = lax.axis_index(KV)
    tp = lax.axis_index("tp")
    kv_size = lax.axis_size(KV)
    groups = lax.axis_size("tp")
    local, positions, latent_width = cache.shape
    width = cache_rope.shape[1]
    small = []
    for n, (a, b) in enumerate(
        ((lengths_, lengths), (frequencies_, frequencies), (gain_, gain))
    ):
        small.append(pltpu.make_async_copy(a, b, sems.at[2 * local + n]))
        small[n].start()
    copies = []
    for s in range(local):
        a = pltpu.make_async_copy(latents.at[s], cache.at[s], sems.at[s])
        b = pltpu.make_async_copy(ropes.at[s], cache_rope.at[s], sems.at[local + s])
        a.start()
        b.start()
        copies.append((a, b))
    def total(n):
        rows_of = slice(n * local, (n + 1) * local)
        result = got[0, rows_of, :].astype(F32)
        for k in range(1, kv_size):
            result = result + got[k, rows_of, :].astype(F32)
        return result

    for copy in small:
        copy.wait()
    shape = (local, lengths.shape[1])
    length = jnp.sum(
        jnp.where(lanes(shape) == rows(shape) + tp * local, lengths[...], 0), axis=1, keepdims=True
    )
    lane = lanes((local, width))
    angles = length.astype(F32) * frequencies[...]
    cosine = jnp.cos(angles)
    sine = jnp.sin(angles)
    sine = jnp.where(lane < width // 2, -sine, sine)
    half = groups // 2
    for i in range(groups):
        w = near if i < half else far
        lifted[i] = dot(total(i).astype(BF16), w[i % half, :latent_width, :], NT)
    for i in range(half):
        both = total(groups + i).astype(BF16).astype(F32)
        turned[i] = rotate(both[:, :width], cosine, sine)
        turned[i + half] = rotate(both[:, width:], cosine, sine)
    fresh = total(groups + half)
    pieces = latent_width // nope
    raw = jnp.concatenate([fresh[n : n + 1] for n in range(pieces)], axis=1)
    rope_raw = fresh[pieces : pieces + 1, :width]
    square = jnp.sum(raw * raw, axis=1, keepdims=True) / latent_width
    new_latent = (raw * lax.rsqrt(square + EPSILON) * gain[...]).astype(BF16).astype(F32)
    new_seq = lax.rem(kv, local)
    mine = rows((local, width)) == new_seq
    new_rope = rotate(
        rope_raw,
        jnp.sum(jnp.where(mine, cosine, 0.0), axis=0, keepdims=True),
        jnp.sum(jnp.where(mine, sine, 0.0), axis=0, keepdims=True),
    )
    new_rope = new_rope.astype(BF16).astype(F32)
    pairs = local * groups
    for s in range(local):
        q = lifted[:, s, :].astype(BF16)
        qr = turned[:, s, :].astype(BF16)
        fresh = jnp.sum(q.astype(F32) * new_latent, axis=1, keepdims=True) + jnp.sum(
            qr.astype(F32) * new_rope, axis=1, keepdims=True
        )
        for copy in copies[s]:
            copy.wait()
        r = s * groups
        scored[r : r + groups, :positions] = dot(q, cache[s], NT) + dot(qr, cache_rope[s], NN)
        scored[r : r + groups, positions:] = jnp.broadcast_to(fresh, (groups, 128))
    scores = scored[:, :positions] * factor
    row = rows((pairs, 1))
    sequence = row // groups
    limit = jnp.zeros((pairs, 1), jnp.int32)
    for s in range(local):
        limit = jnp.where(sequence == s, length[s : s + 1, :], limit)
    is_new = jnp.logical_and(sequence == new_seq, kv < local)
    new = jnp.where(is_new, scored[:, positions : positions + 1] * factor, NEGATIVE)
    visible = kv * positions + lanes((pairs, positions)) < limit
    top = jnp.max(jnp.where(visible, scores, NEGATIVE), axis=1, keepdims=True)
    top = jnp.maximum(top, new)
    weight = jnp.where(visible, jnp.exp(scores - top), 0.0)
    new_weight = jnp.where(is_new, jnp.exp(new - top), 0.0)
    total = jnp.sum(weight, axis=1, keepdims=True) + new_weight
    weights[...] = weight.astype(BF16)
    some = total > 0.0
    safe = jnp.where(some, total, 1.0)
    inverse = 1.0 / safe
    logs = jnp.where(some, top + jnp.log(safe), NEGATIVE)
    rounded = new_weight.astype(BF16).astype(F32)
    for s in range(local):
        r = slice(s * groups, (s + 1) * groups)
        mixed = dot(weights[r, :], cache[s], NN) + rounded[r] * new_latent
        means[s] = mixed * inverse[r]
    for i in range(groups):
        w = near if i < half else far
        x = means[:, i, :].astype(BF16)
        up = dot(x, w[i % half, latent_width : 2 * latent_width, :], NN).astype(BF16)
        for k in range(kv_size):
            out[k, i * local : (i + 1) * local, :] = up
    lane = lanes((local, 128))
    table = jnp.zeros((groups, 128), F32)
    for s in range(local):
        table = jnp.where(lanes((groups, 128)) == s, logs[s * groups : (s + 1) * groups], table)
    table = jnp.concatenate([table, jnp.zeros((128 - groups, 128), F32)], axis=0)
    table = jnp.transpose(table)[:local]
    high = table.astype(BF16).astype(F32)
    rest = table - high
    middle = rest.astype(BF16).astype(F32)
    low = (rest - middle).astype(BF16).astype(F32)
    packed = jnp.where(
        lane < groups,
        high,
        jnp.where(
            lane < 2 * groups,
            pltpu.roll(middle, groups, 1),
            jnp.where(lane < 3 * groups, pltpu.roll(low, 2 * groups, 1), 0.0),
        ),
    ).astype(BF16)
    for k in range(kv_size):
        out[k, groups * local :, :] = packed


def combine_kernel(got, near, far, out, *, kv_size, groups, local, first):
    logs = []
    for k in range(kv_size):
        x = got[k, groups * local :, :].astype(F32)
        logs.append(x + pltpu.roll(x, 128 - groups, 1) + pltpu.roll(x, 128 - 2 * groups, 1))
    top = functools.reduce(jnp.maximum, logs)
    shares = [jnp.exp(x - top) for x in logs]
    total = functools.reduce(jnp.add, shares)
    inverse = 1.0 / total
    shares = [x * inverse for x in shares]
    half = groups // 2
    mixed = jnp.zeros((local, out.shape[2]), F32)
    for i in range(groups):
        head = jnp.zeros((local, 128), F32)
        for k in range(kv_size):
            part = got[k, i * local : (i + 1) * local, :].astype(F32)
            head = head + part * shares[k][:, i : i + 1]
        w = near if i < half else far
        mixed = mixed + dot(head.astype(BF16), w[i % half, first:, :], NN)
    mixed = mixed.astype(BF16)
    for d in range(out.shape[0]):
        out[d] = mixed


def finish_kernel(got, gain, out, *, kv_size, groups, local):
    kv = lax.axis_index(KV)
    width = got.shape[2]
    for t in range(groups):
        squares = jnp.zeros((local, width), F32)
        for k in range(kv_size):
            x = got[k * groups + t].astype(F32)
            squares = squares + x * x
        mean = jnp.sum(squares, axis=1, keepdims=True) / (width * kv_size)
        own = got[kv * groups + t].astype(F32)
        out[t * local : (t + 1) * local, :] = (
            own * lax.rsqrt(mean + EPSILON) * gain[...]
        ).astype(BF16)


def exchange(value, axes):
    return lax.all_to_all(value, axes, split_axis=0, concat_axis=0, tiled=True)


def swap(value):
    return lax.ppermute(value, "tp", [(i, i ^ 1) for i in range(lax.axis_size("tp"))])


def along(own):
    size = lax.axis_size("tp")
    collected = []
    for step in (1, 3, 2):
        pairs = [(i, (i + 2 * step) % size) for i in range(size)]
        collected.append(lax.ppermute(own, "tp", pairs))
    return collected


def on_device(
    tokens,
    token_gain,
    w_query,
    w_down_kv,
    w_rope_key,
    latent_gain,
    w_key_up,
    w_value_up,
    w_out,
    out_gain,
    cache_latent,
    cache_rope,
    lengths,
):
    kv_size = lax.axis_size(KV)
    groups = lax.axis_size("tp")
    everyone = kv_size * groups
    seqs, width = tokens.shape
    local, positions, latent_width = cache_latent.shape
    rope = cache_rope.shape[2]
    nope = w_key_up.shape[2]
    value = w_value_up.shape[2]
    factor = (nope + rope) ** (-0.5)

    others = along(w_query.T)
    tokens, gain, w_down, w_rope, own_query, own = pl.pallas_call(
        collect_kernel,
        out_shape=(
            jax.ShapeDtypeStruct(tokens.shape, BF16),
            jax.ShapeDtypeStruct((1, width), F32),
            jax.ShapeDtypeStruct(w_down_kv.shape, BF16),
            jax.ShapeDtypeStruct((rope, width), BF16),
            jax.ShapeDtypeStruct((nope + rope, width), BF16),
            jax.ShapeDtypeStruct((2 * latent_width + value, nope), BF16),
        ),
        in_specs=[in_hbm()] * 8,
        out_specs=(in_vmem(),) * 6,
        scratch_shapes=[pltpu.SemaphoreType.DMA((8,))],
        compiler_params=params(8),
        name="collect",
    )(
        *keep_in_hbm(
            tokens,
            token_gain[None],
            w_down_kv,
            w_rope_key.T,
            w_query.T,
            w_key_up,
            w_value_up,
            w_out,
        )
    )
    near_query = jnp.stack([own_query] + others)
    far_query = swap(near_query)
    near = jnp.stack([own] + along(own))
    far = swap(near)

    sent_rows = (groups + groups // 2 + 1) * local
    sent = pl.pallas_call(
        project_kernel,
        out_shape=jax.ShapeDtypeStruct((kv_size, sent_rows, 128), BF16),
        in_specs=[in_vmem()] * 6,
        out_specs=in_vmem(),
        scratch_shapes=[pltpu.VMEM((local, local, 128), F32)],
        compiler_params=params(8),
        name="project",
    )(tokens, gain, near_query, far_query, w_down, w_rope)
    got = exchange(sent, KV)
    powers = np.arange(0, rope, 2, dtype=np.float64) / rope
    frequencies = np.tile(1.0 / 10000.0**powers, 2)[None].astype(np.float32)
    sent = pl.pallas_call(
        functools.partial(attend_kernel, factor=factor, nope=nope),
        out_shape=jax.ShapeDtypeStruct((kv_size, groups * local + local, value), BF16),
        in_specs=[in_vmem()] * 3 + [in_hbm()] * 5,
        out_specs=in_vmem(),
        scratch_shapes=[
            pltpu.VMEM((1, seqs), jnp.int32),
            pltpu.VMEM((1, rope), F32),
            pltpu.VMEM((1, latent_width), F32),
            pltpu.VMEM((local, positions, latent_width), BF16),
            pltpu.VMEM((local, rope, positions), BF16),
            pltpu.VMEM((groups, local, latent_width), F32),
            pltpu.VMEM((groups, local, rope), F32),
            pltpu.VMEM((local * groups, positions + 128), F32),
            pltpu.VMEM((local * groups, positions), BF16),
            pltpu.VMEM((local, groups, latent_width), F32),
            pltpu.SemaphoreType.DMA((2 * local + 3,)),
        ],
        compiler_params=params(24),
        name="attend",
    )(
        got,
        near,
        far,
        *keep_in_hbm(
            lengths[None],
            frequencies,
            latent_gain[None],
            cache_latent,
            cache_rope.transpose(0, 2, 1),
        ),
    )
    got = exchange(sent, KV)

    sent = pl.pallas_call(
        functools.partial(
            combine_kernel,
            kv_size=kv_size,
            groups=groups,
            local=local,
            first=2 * latent_width,
        ),
        out_shape=jax.ShapeDtypeStruct((everyone, local, w_out.shape[1]), BF16),
        in_specs=[in_vmem()] * 3,
        out_specs=in_vmem(),
        compiler_params=params(8),
        name="combine",
    )(got, near, far)
    got = exchange(sent, ALL)
    return pl.pallas_call(
        functools.partial(finish_kernel, kv_size=kv_size, groups=groups, local=local),
        out_shape=jax.ShapeDtypeStruct((seqs, w_out.shape[1]), BF16),
        in_specs=[in_vmem(), in_vmem()],
        out_specs=in_vmem(),
        compiler_params=params(8),
        name="finish",
    )(got, out_gain[None])


def solution(mesh):
    finer = Mesh(mesh.devices.reshape(4, 4, mesh.shape["tp"]), ("kv_0", "kv_1", "tp"))

    return jax.shard_map(
        on_device,
        mesh=finer,
        in_specs=(
            P(None, KV),
            P(KV),
            P(KV, "tp"),
            P(KV, None),
            P(KV, None),
            P(),
            P("tp", None, None),
            P("tp", None, None),
            P("tp", KV),
            P(KV),
            P("tp", KV, None),
            P("tp", KV, None),
            P(),
        ),
        out_specs=P(None, KV),
        check_vma=False,
    )
```

```python
import functools

import jax
import jax.numpy as jnp
import numpy as np
from jax import lax
from jax.experimental import pallas as pl
from jax.experimental.pallas import tpu as pltpu
from jax.sharding import Mesh
from jax.sharding import PartitionSpec as P


KV = ("kv_0", "kv_1")
ALL = ("kv_0", "kv_1", "tp")
EPSILON = 1e-06
NEGATIVE = -1e30
PARTS = 2
F32 = jnp.float32
BF16 = jnp.bfloat16

NT = (((1,), (1,)), ((), ()))
NN = (((1,), (0,)), ((), ()))


def dot(a, b, dims):
    return lax.dot_general(a, b, dims, preferred_element_type=F32)


def params(mib):
    return pltpu.CompilerParams(vmem_limit_bytes=mib * 1024 * 1024)


def in_vmem():
    return pl.BlockSpec(memory_space=pltpu.VMEM)


def in_hbm():
    return pl.BlockSpec(memory_space=pltpu.HBM)


def keep_in_hbm(*arrays):
    return [pltpu.with_memory_space_constraint(x, pltpu.HBM) for x in arrays]


def lanes(shape):
    return lax.broadcasted_iota(jnp.int32, shape, 1)


def rows(shape):
    return lax.broadcasted_iota(jnp.int32, shape, 0)


def collect_kernel(
    tokens_, gain_, wd_, wr_, wq_, wk, wv, wo, tokens, gain, wd, wr, wq, own, sems
):
    deep = wk.shape[1]
    pairs = (
        (wk.at[0], own.at[pl.ds(0, deep)]),
        (wv.at[0], own.at[pl.ds(deep, deep)]),
        (wo, own.at[pl.ds(2 * deep, wo.shape[0])]),
        (tokens_, tokens),
        (gain_, gain),
        (wd_, wd),
        (wr_, wr),
        (wq_, wq),
    )
    copies = [pltpu.make_async_copy(x, y, sems.at[n]) for n, (x, y) in enumerate(pairs)]
    for copy in copies:
        copy.start()
    for copy in copies:
        copy.wait()


def project_kernel(tokens, gain, near, far, wd, wr, out, news):
    tp = lax.axis_index("tp")
    groups = lax.axis_size("tp")
    local = tokens.shape[0] // groups
    half = groups // 2
    width = wr.shape[0]
    mine = tokens[pl.ds(pl.multiple_of(tp * local, local), local), :]
    scaled = (mine.astype(F32) * gain[...]).astype(BF16)
    latent = dot(scaled, wd[...], NN)
    rope = dot(scaled, wr[...], NT)
    pieces = latent.shape[1] // 128
    for n in range(pieces):
        news[n] = latent[:, n * 128 : (n + 1) * 128]
    news[pieces] = jnp.concatenate([rope, jnp.zeros((local, 128 - width), F32)], axis=1)
    for n in range(pieces + 1, local):
        news[n] = jnp.zeros((local, 128), F32)
    queries = [
        dot(scaled, (near if i < half else far)[i % half], NT) for i in range(groups)
    ]
    tiles = [q[:, :128].astype(BF16) for q in queries] + [
        jnp.concatenate([queries[i][:, 128:], queries[i + half][:, 128:]], axis=1).astype(BF16)
        for i in range(half)
    ]
    copies = out.shape[0] // local
    for j in range(local):
        new = news[:, j, :].astype(BF16)
        for c in range(copies):
            k = c * local + j
            for n, tile in enumerate(tiles):
                out[k, n * local : (n + 1) * local, :] = tile
            out[k, len(tiles) * local :, :] = new


def rotate(values, cosine, sine):
    half = values.shape[1] // 2
    swapped = jnp.concatenate([values[:, half:], values[:, :half]], axis=1)
    return values * cosine + swapped * sine


def attend_kernel(
    got, near, opposite, far, far_opposite, lengths_, frequencies_, gain_, latents, ropes,
    out, lengths, frequencies, gain, cache, cache_rope,
    lifted, turned, scored, weights, means, sems,
    *, factor, nope,
):
    kv = lax.axis_index(KV)
    tp = lax.axis_index("tp")
    kv_size = lax.axis_size(KV)
    groups = lax.axis_size("tp")
    local, positions, latent_width = cache.shape
    width = cache_rope.shape[1]
    small = []
    for n, (a, b) in enumerate(
        ((lengths_, lengths), (frequencies_, frequencies), (gain_, gain))
    ):
        small.append(pltpu.make_async_copy(a, b, sems.at[2 * local + n]))
        small[n].start()
    copies = []
    for s in range(local):
        a = pltpu.make_async_copy(latents.at[s], cache.at[s], sems.at[s])
        b = pltpu.make_async_copy(ropes.at[s], cache_rope.at[s], sems.at[local + s])
        a.start()
        b.start()
        copies.append((a, b))
    def total(n):
        rows_of = slice(n * local, (n + 1) * local)
        result = got[0, rows_of, :].astype(F32)
        for k in range(1, kv_size):
            result = result + got[k, rows_of, :].astype(F32)
        return result

    for copy in small:
        copy.wait()
    shape = (local, lengths.shape[1])
    length = jnp.sum(
        jnp.where(lanes(shape) == rows(shape) + tp * local, lengths[...], 0), axis=1, keepdims=True
    )
    lane = lanes((local, width))
    angles = length.astype(F32) * frequencies[...]
    cosine = jnp.cos(angles)
    sine = jnp.sin(angles)
    sine = jnp.where(lane < width // 2, -sine, sine)
    half = groups // 2
    for i in range(groups):
        w = weights_of((near, opposite, far, far_opposite), i)
        lifted[i] = dot(total(i).astype(BF16), w[:latent_width, :], NT)
    for i in range(half):
        both = total(groups + i).astype(BF16).astype(F32)
        turned[i] = rotate(both[:, :width], cosine, sine)
        turned[i + half] = rotate(both[:, width:], cosine, sine)
    fresh = total(groups + half)
    pieces = latent_width // nope
    raw = jnp.concatenate([fresh[n : n + 1] for n in range(pieces)], axis=1)
    rope_raw = fresh[pieces : pieces + 1, :width]
    square = jnp.sum(raw * raw, axis=1, keepdims=True) / latent_width
    new_latent = (raw * lax.rsqrt(square + EPSILON) * gain[...]).astype(BF16).astype(F32)
    new_seq = lax.rem(kv, local)
    mine = rows((local, width)) == new_seq
    new_rope = rotate(
        rope_raw,
        jnp.sum(jnp.where(mine, cosine, 0.0), axis=0, keepdims=True),
        jnp.sum(jnp.where(mine, sine, 0.0), axis=0, keepdims=True),
    )
    new_rope = new_rope.astype(BF16).astype(F32)
    table = jnp.zeros((groups, 128), F32)
    for start in range(0, local, local // PARTS):
        members = range(start, start + local // PARTS)
        pairs = len(members) * groups
        for s in members:
            q = lifted[:, s, :].astype(BF16)
            qr = turned[:, s, :].astype(BF16)
            own = jnp.sum(q.astype(F32) * new_latent, axis=1, keepdims=True) + jnp.sum(
                qr.astype(F32) * new_rope, axis=1, keepdims=True
            )
            for copy in copies[s]:
                copy.wait()
            r = slice(s * groups, (s + 1) * groups)
            scored[r, :positions] = dot(q, cache[s], NT) + dot(qr, cache_rope[s], NN)
            scored[r, positions:] = jnp.broadcast_to(own, (groups, 128))
        these = slice(start * groups, start * groups + pairs)
        scores = scored[these, :positions] * factor
        sequence = rows((pairs, 1)) // groups + start
        limit = jnp.zeros((pairs, 1), jnp.int32)
        for s in members:
            limit = jnp.where(sequence == s, length[s : s + 1, :], limit)
        is_new = jnp.logical_and(sequence == new_seq, kv < local)
        new = jnp.where(is_new, scored[these, positions : positions + 1] * factor, NEGATIVE)
        visible = kv * positions + lanes((pairs, positions)) < limit
        top = jnp.max(jnp.where(visible, scores, NEGATIVE), axis=1, keepdims=True)
        top = jnp.maximum(top, new)
        weight = jnp.where(visible, jnp.exp(scores - top), 0.0)
        new_weight = jnp.where(is_new, jnp.exp(new - top), 0.0)
        total_weight = jnp.sum(weight, axis=1, keepdims=True) + new_weight
        weights[these, :] = weight.astype(BF16)
        some = total_weight > 0.0
        safe = jnp.where(some, total_weight, 1.0)
        inverse = 1.0 / safe
        logs = jnp.where(some, top + jnp.log(safe), NEGATIVE)
        rounded = new_weight.astype(BF16).astype(F32)
        for n, s in enumerate(members):
            r = slice(n * groups, (n + 1) * groups)
            mixed = dot(weights[s * groups : (s + 1) * groups, :], cache[s], NN)
            means[s] = (mixed + rounded[r] * new_latent) * inverse[r]
            table = jnp.where(lanes((groups, 128)) == s, logs[r], table)
    for i in range(groups):
        w = weights_of((near, opposite, far, far_opposite), i)
        x = means[:, i, :].astype(BF16)
        up = dot(x, w[latent_width : 2 * latent_width, :], NN).astype(BF16)
        for k in range(kv_size):
            out[k, i * local : (i + 1) * local, :] = up
    lane = lanes((local, 128))
    table = jnp.concatenate([table, jnp.zeros((128 - groups, 128), F32)], axis=0)
    table = jnp.transpose(table)[:local]
    high = table.astype(BF16).astype(F32)
    rest = table - high
    middle = rest.astype(BF16).astype(F32)
    low = (rest - middle).astype(BF16).astype(F32)
    packed = jnp.where(
        lane < groups,
        high,
        jnp.where(
            lane < 2 * groups,
            pltpu.roll(middle, groups, 1),
            jnp.where(lane < 3 * groups, pltpu.roll(low, 2 * groups, 1), 0.0),
        ),
    ).astype(BF16)
    for k in range(kv_size):
        out[k, groups * local :, :] = packed


def weights_of(collected, i):
    near, opposite, far, far_opposite = collected
    places = near.shape[0] + 1
    stacked, single = (near, opposite) if i < places else (far, far_opposite)
    return single if i % places == places - 1 else stacked.at[i % places]


def combine_kernel(got, near, opposite, far, far_opposite, out, *, kv_size, groups, local, first):
    logs = []
    for k in range(kv_size):
        x = got[k, groups * local :, :].astype(F32)
        logs.append(x + pltpu.roll(x, 128 - groups, 1) + pltpu.roll(x, 128 - 2 * groups, 1))
    top = functools.reduce(jnp.maximum, logs)
    shares = [jnp.exp(x - top) for x in logs]
    total = functools.reduce(jnp.add, shares)
    inverse = 1.0 / total
    shares = [x * inverse for x in shares]
    mixed = jnp.zeros((local, out.shape[2]), F32)
    for i in range(groups):
        head = jnp.zeros((local, 128), F32)
        for k in range(kv_size):
            part = got[k, i * local : (i + 1) * local, :].astype(F32)
            head = head + part * shares[k][:, i : i + 1]
        w = weights_of((near, opposite, far, far_opposite), i)
        mixed = mixed + dot(head.astype(BF16), w[first:, :], NN)
    mixed = mixed.astype(BF16)
    for d in range(out.shape[0]):
        out[d] = mixed


def finish_kernel(got, gain, out, *, kv_size, groups, local):
    kv = lax.axis_index(KV)
    width = got.shape[2]
    for t in range(groups):
        squares = jnp.zeros((local, width), F32)
        for k in range(kv_size):
            x = got[k * groups + t].astype(F32)
            squares = squares + x * x
        mean = jnp.sum(squares, axis=1, keepdims=True) / (width * kv_size)
        own = got[kv * groups + t].astype(F32)
        out[t * local : (t + 1) * local, :] = (
            own * lax.rsqrt(mean + EPSILON) * gain[...]
        ).astype(BF16)


def exchange(value, axes):
    return lax.all_to_all(value, axes, split_axis=0, concat_axis=0, tiled=True)


def swap(value):
    return lax.ppermute(value, "tp", [(i, i ^ 1) for i in range(lax.axis_size("tp"))])


def along(own):
    size = lax.axis_size("tp")
    collected = []
    for step in (1, 3, 2):
        pairs = [(i, (i + 2 * step) % size) for i in range(size)]
        collected.append(lax.ppermute(own, "tp", pairs))
    return collected


def on_device(
    tokens,
    token_gain,
    w_query,
    w_down_kv,
    w_rope_key,
    latent_gain,
    w_key_up,
    w_value_up,
    w_out,
    out_gain,
    cache_latent,
    cache_rope,
    lengths,
):
    kv_size = lax.axis_size(KV)
    groups = lax.axis_size("tp")
    everyone = kv_size * groups
    seqs, width = tokens.shape
    local, positions, latent_width = cache_latent.shape
    rope = cache_rope.shape[2]
    nope = w_key_up.shape[2]
    value = w_value_up.shape[2]
    factor = (nope + rope) ** (-0.5)

    others = along(w_query.T)
    tokens, gain, w_down, w_rope, own_query, own = pl.pallas_call(
        collect_kernel,
        out_shape=(
            jax.ShapeDtypeStruct(tokens.shape, BF16),
            jax.ShapeDtypeStruct((1, width), F32),
            jax.ShapeDtypeStruct(w_down_kv.shape, BF16),
            jax.ShapeDtypeStruct((rope, width), BF16),
            jax.ShapeDtypeStruct((nope + rope, width), BF16),
            jax.ShapeDtypeStruct((2 * latent_width + value, nope), BF16),
        ),
        in_specs=[in_hbm()] * 8,
        out_specs=(in_vmem(),) * 6,
        scratch_shapes=[pltpu.SemaphoreType.DMA((8,))],
        compiler_params=params(8),
        name="collect",
    )(
        *keep_in_hbm(
            tokens,
            token_gain[None],
            w_down_kv,
            w_rope_key.T,
            w_query.T,
            w_key_up,
            w_value_up,
            w_out,
        )
    )
    near_query = jnp.stack([own_query] + others)
    far_query = swap(near_query)
    before, after, opposite = along(own)
    near = jnp.stack([own, before, after])
    far = swap(near)
    far_opposite = swap(opposite)
    collected = (near, opposite, far, far_opposite)

    sent_rows = (groups + groups // 2 + 1) * local
    sent = pl.pallas_call(
        project_kernel,
        out_shape=jax.ShapeDtypeStruct((kv_size, sent_rows, 128), BF16),
        in_specs=[in_vmem()] * 6,
        out_specs=in_vmem(),
        scratch_shapes=[pltpu.VMEM((local, local, 128), F32)],
        compiler_params=params(8),
        name="project",
    )(tokens, gain, near_query, far_query, w_down, w_rope)
    got = exchange(sent, KV)
    powers = np.arange(0, rope, 2, dtype=np.float64) / rope
    frequencies = np.tile(1.0 / 10000.0**powers, 2)[None].astype(np.float32)
    sent = pl.pallas_call(
        functools.partial(attend_kernel, factor=factor, nope=nope),
        out_shape=jax.ShapeDtypeStruct((kv_size, groups * local + local, value), BF16),
        in_specs=[in_vmem()] * 5 + [in_hbm()] * 5,
        out_specs=in_vmem(),
        scratch_shapes=[
            pltpu.VMEM((1, seqs), jnp.int32),
            pltpu.VMEM((1, rope), F32),
            pltpu.VMEM((1, latent_width), F32),
            pltpu.VMEM((local, positions, latent_width), BF16),
            pltpu.VMEM((local, rope, positions), BF16),
            pltpu.VMEM((groups, local, latent_width), F32),
            pltpu.VMEM((groups, local, rope), F32),
            pltpu.VMEM((local * groups, positions + 128), F32),
            pltpu.VMEM((local * groups, positions), BF16),
            pltpu.VMEM((local, groups, latent_width), F32),
            pltpu.SemaphoreType.DMA((2 * local + 3,)),
        ],
        compiler_params=params(24),
        name="attend",
    )(
        got,
        *collected,
        *keep_in_hbm(
            lengths[None],
            frequencies,
            latent_gain[None],
            cache_latent,
            cache_rope.transpose(0, 2, 1),
        ),
    )
    got = exchange(sent, KV)

    sent = pl.pallas_call(
        functools.partial(
            combine_kernel,
            kv_size=kv_size,
            groups=groups,
            local=local,
            first=2 * latent_width,
        ),
        out_shape=jax.ShapeDtypeStruct((everyone, local, w_out.shape[1]), BF16),
        in_specs=[in_vmem()] * 5,
        out_specs=in_vmem(),
        compiler_params=params(8),
        name="combine",
    )(got, *collected)
    got = exchange(sent, ALL)
    return pl.pallas_call(
        functools.partial(finish_kernel, kv_size=kv_size, groups=groups, local=local),
        out_shape=jax.ShapeDtypeStruct((seqs, w_out.shape[1]), BF16),
        in_specs=[in_vmem(), in_vmem()],
        out_specs=in_vmem(),
        compiler_params=params(8),
        name="finish",
    )(got, out_gain[None])


def solution(mesh):
    finer = Mesh(mesh.devices.reshape(4, 4, mesh.shape["tp"]), ("kv_0", "kv_1", "tp"))

    return jax.shard_map(
        on_device,
        mesh=finer,
        in_specs=(
            P(None, KV),
            P(KV),
            P(KV, "tp"),
            P(KV, None),
            P(KV, None),
            P(),
            P("tp", None, None),
            P("tp", None, None),
            P("tp", KV),
            P(KV),
            P("tp", KV, None),
            P("tp", KV, None),
            P(),
        ),
        out_specs=P(None, KV),
        check_vma=False,
    )
```

```python
import functools

import jax
import jax.numpy as jnp
import numpy as np
from jax import lax
from jax.experimental import pallas as pl
from jax.experimental.pallas import tpu as pltpu
from jax.sharding import Mesh
from jax.sharding import PartitionSpec as P


KV = ("kv_0", "kv_1")
TP = ("y", "core")
ALL = KV + TP
FIRST = KV + ("core",)
EPSILON = 1e-06
NEGATIVE = -1e30
PARTS = 2
F32 = jnp.float32
BF16 = jnp.bfloat16

NT = (((1,), (1,)), ((), ()))
NN = (((1,), (0,)), ((), ()))


def dot(a, b, dims):
    return lax.dot_general(a, b, dims, preferred_element_type=F32)


def params(mib):
    return pltpu.CompilerParams(vmem_limit_bytes=mib * 1024 * 1024)


def in_vmem():
    return pl.BlockSpec(memory_space=pltpu.VMEM)


def in_hbm():
    return pl.BlockSpec(memory_space=pltpu.HBM)


def keep_in_hbm(*arrays):
    return [pltpu.with_memory_space_constraint(x, pltpu.HBM) for x in arrays]


def lanes(shape):
    return lax.broadcasted_iota(jnp.int32, shape, 1)


def rows(shape):
    return lax.broadcasted_iota(jnp.int32, shape, 0)


def collect_kernel(
    tokens_, gain_, wd_, wr_, wq_, wk, wv, wo, tokens, gain, wd, wr, wq, own, sems
):
    deep = wk.shape[1]
    pairs = (
        (wk.at[0], own.at[pl.ds(0, deep)]),
        (wv.at[0], own.at[pl.ds(deep, deep)]),
        (wo, own.at[pl.ds(2 * deep, wo.shape[0])]),
        (tokens_, tokens),
        (gain_, gain),
        (wd_, wd),
        (wr_, wr),
        (wq_, wq),
    )
    copies = [pltpu.make_async_copy(x, y, sems.at[n]) for n, (x, y) in enumerate(pairs)]
    for copy in copies:
        copy.start()
    for copy in copies:
        copy.wait()


def project_kernel(tokens, gain, query_0, query_1, query_2, query_3, wd, wr, out, news):
    cores = lax.axis_size("core")
    local = news.shape[1] // cores
    chip = cores * local
    width = wr.shape[0]
    start = pl.multiple_of(lax.axis_index("y") * chip, chip)
    mine = tokens[pl.ds(start, chip), :]
    scaled = (mine.astype(F32) * gain[...]).astype(BF16)
    latent = dot(scaled, wd[...], NN)
    rope = dot(scaled, wr[...], NT)
    pieces = latent.shape[1] // 128
    for n in range(pieces):
        news[n] = latent[:, n * 128 : (n + 1) * 128]
    news[pieces] = jnp.concatenate([rope, jnp.zeros((chip, 128 - width), F32)], axis=1)
    for n in range(pieces + 1, local):
        news[n] = jnp.zeros((chip, 128), F32)
    queries = [dot(scaled, w[...], NT) for w in (query_0, query_1, query_2, query_3)]
    half = len(queries) // 2
    tiles = [q[:, :128] for q in queries] + [
        jnp.concatenate([queries[i][:, 128:], queries[i + half][:, 128:]], axis=1)
        for i in range(half)
    ]
    tiles = [
        [tile[c * local : (c + 1) * local].astype(BF16) for c in range(cores)] for tile in tiles
    ]
    for j in range(local):
        for c in range(cores):
            new = news[:, c * local + j, :].astype(BF16)
            for copy in range(out.shape[0] // cores // local):
                k = copy * local + j
                for n, tile in enumerate(tiles):
                    out[k * cores + c, n * local : (n + 1) * local, :] = tile[c]
                out[k * cores + c, len(tiles) * local :, :] = new


def rotate(values, cosine, sine):
    half = values.shape[1] // 2
    swapped = jnp.concatenate([values[:, half:], values[:, :half]], axis=1)
    return values * cosine + swapped * sine


def attend_kernel(
    got, near, opposite, far, far_opposite, lengths_, frequencies_, gain_, latents, ropes,
    out, lengths, frequencies, gain, cache, cache_rope,
    lifted, turned, scored, weights, means, sems,
    *, factor, nope,
):
    kv = lax.axis_index(KV)
    tp = lax.axis_index(TP)
    kv_size = lax.axis_size(KV)
    groups = lax.axis_size(TP)
    local, positions, latent_width = cache.shape
    width = cache_rope.shape[1]
    small = []
    for n, (a, b) in enumerate(
        ((lengths_, lengths), (frequencies_, frequencies), (gain_, gain))
    ):
        small.append(pltpu.make_async_copy(a, b, sems.at[2 * local + n]))
        small[n].start()
    copies = []
    for s in range(local):
        a = pltpu.make_async_copy(latents.at[s], cache.at[s], sems.at[s])
        b = pltpu.make_async_copy(ropes.at[s], cache_rope.at[s], sems.at[local + s])
        a.start()
        b.start()
        copies.append((a, b))
    cores = lax.axis_size("core")
    core = lax.axis_index("core")
    half = groups // 2

    def total(source, n):
        rows_of = slice(n * local, (n + 1) * local)
        result = got[source, rows_of, :].astype(F32)
        for k in range(1, kv_size):
            result = result + got[k * cores + source, rows_of, :].astype(F32)
        return result

    for copy in small:
        copy.wait()
    shape = (local, lengths.shape[1])
    length = jnp.sum(
        jnp.where(lanes(shape) == rows(shape) + tp * local, lengths[...], 0), axis=1, keepdims=True
    )
    lane = lanes((local, width))
    angles = length.astype(F32) * frequencies[...]
    cosine = jnp.cos(angles)
    sine = jnp.sin(angles)
    sine = jnp.where(lane < width // 2, -sine, sine)
    for i in range(groups):
        source = core if i < half else 1 - core
        w = weights_of((near, opposite, far, far_opposite), i)
        lifted[i] = dot(total(source, i % half).astype(BF16), w[:latent_width, :], NT)
    for i in range(groups):
        if i % half >= half // 2:
            continue
        source = core if i < half else 1 - core
        both = total(source, half + i % half).astype(BF16).astype(F32)
        turned[i] = rotate(both[:, :width], cosine, sine)
        turned[i + half // 2] = rotate(both[:, width:], cosine, sine)
    fresh = total(0, half + half // 2)
    pieces = latent_width // nope
    raw = jnp.concatenate([fresh[n : n + 1] for n in range(pieces)], axis=1)
    rope_raw = fresh[pieces : pieces + 1, :width]
    square = jnp.sum(raw * raw, axis=1, keepdims=True) / latent_width
    new_latent = (raw * lax.rsqrt(square + EPSILON) * gain[...]).astype(BF16).astype(F32)
    new_seq = lax.rem(kv, local)
    mine = rows((local, width)) == new_seq
    new_rope = rotate(
        rope_raw,
        jnp.sum(jnp.where(mine, cosine, 0.0), axis=0, keepdims=True),
        jnp.sum(jnp.where(mine, sine, 0.0), axis=0, keepdims=True),
    )
    new_rope = new_rope.astype(BF16).astype(F32)
    table = jnp.zeros((groups, 128), F32)
    for start in range(0, local, local // PARTS):
        members = range(start, start + local // PARTS)
        pairs = len(members) * groups
        for s in members:
            q = lifted[:, s, :].astype(BF16)
            qr = turned[:, s, :].astype(BF16)
            own = jnp.sum(q.astype(F32) * new_latent, axis=1, keepdims=True) + jnp.sum(
                qr.astype(F32) * new_rope, axis=1, keepdims=True
            )
            for copy in copies[s]:
                copy.wait()
            r = slice(s * groups, (s + 1) * groups)
            scored[r, :positions] = dot(q, cache[s], NT) + dot(qr, cache_rope[s], NN)
            scored[r, positions:] = jnp.broadcast_to(own, (groups, 128))
        these = slice(start * groups, start * groups + pairs)
        scores = scored[these, :positions] * factor
        sequence = rows((pairs, 1)) // groups + start
        limit = jnp.zeros((pairs, 1), jnp.int32)
        for s in members:
            limit = jnp.where(sequence == s, length[s : s + 1, :], limit)
        is_new = jnp.logical_and(sequence == new_seq, kv < local)
        new = jnp.where(is_new, scored[these, positions : positions + 1] * factor, NEGATIVE)
        visible = kv * positions + lanes((pairs, positions)) < limit
        top = jnp.max(jnp.where(visible, scores, NEGATIVE), axis=1, keepdims=True)
        top = jnp.maximum(top, new)
        weight = jnp.where(visible, jnp.exp(scores - top), 0.0)
        new_weight = jnp.where(is_new, jnp.exp(new - top), 0.0)
        total_weight = jnp.sum(weight, axis=1, keepdims=True) + new_weight
        weights[these, :] = weight.astype(BF16)
        some = total_weight > 0.0
        safe = jnp.where(some, total_weight, 1.0)
        inverse = 1.0 / safe
        logs = jnp.where(some, top + jnp.log(safe), NEGATIVE)
        rounded = new_weight.astype(BF16).astype(F32)
        for n, s in enumerate(members):
            r = slice(n * groups, (n + 1) * groups)
            mixed = dot(weights[s * groups : (s + 1) * groups, :], cache[s], NN)
            means[s] = (mixed + rounded[r] * new_latent) * inverse[r]
            table = jnp.where(lanes((groups, 128)) == s, logs[r], table)
    for i in range(groups):
        w = weights_of((near, opposite, far, far_opposite), i)
        x = means[:, i, :].astype(BF16)
        up = dot(x, w[latent_width : 2 * latent_width, :], NN).astype(BF16)
        for k in range(kv_size):
            out[k, i * local : (i + 1) * local, :] = up
    lane = lanes((local, 128))
    table = jnp.concatenate([table, jnp.zeros((128 - groups, 128), F32)], axis=0)
    table = jnp.transpose(table)[:local]
    high = table.astype(BF16).astype(F32)
    rest = table - high
    middle = rest.astype(BF16).astype(F32)
    low = (rest - middle).astype(BF16).astype(F32)
    packed = jnp.where(
        lane < groups,
        high,
        jnp.where(
            lane < 2 * groups,
            pltpu.roll(middle, groups, 1),
            jnp.where(lane < 3 * groups, pltpu.roll(low, 2 * groups, 1), 0.0),
        ),
    ).astype(BF16)
    for k in range(kv_size):
        out[k, groups * local :, :] = packed


def weights_of(collected, i):
    near, opposite, far, far_opposite = collected
    places = near.shape[0] + 1
    stacked, single = (near, opposite) if i < places else (far, far_opposite)
    return single if i % places == places - 1 else stacked.at[i % places]


def combine_kernel(got, near, opposite, far, far_opposite, out, *, kv_size, groups, local, first):
    logs = []
    for k in range(kv_size):
        x = got[k, groups * local :, :].astype(F32)
        logs.append(x + pltpu.roll(x, 128 - groups, 1) + pltpu.roll(x, 128 - 2 * groups, 1))
    top = functools.reduce(jnp.maximum, logs)
    shares = [jnp.exp(x - top) for x in logs]
    total = functools.reduce(jnp.add, shares)
    inverse = 1.0 / total
    shares = [x * inverse for x in shares]
    mixed = jnp.zeros((local, out.shape[2]), F32)
    for i in range(groups):
        head = jnp.zeros((local, 128), F32)
        for k in range(kv_size):
            part = got[k, i * local : (i + 1) * local, :].astype(F32)
            head = head + part * shares[k][:, i : i + 1]
        w = weights_of((near, opposite, far, far_opposite), i)
        mixed = mixed + dot(head.astype(BF16), w[first:, :], NN)
    mixed = mixed.astype(BF16)
    for d in range(out.shape[0]):
        out[d] = mixed


def finish_kernel(got, gain, out, *, kv_size, groups, local):
    kv = lax.axis_index(KV)
    width = got.shape[2]
    for t in range(groups):
        squares = jnp.zeros((local, width), F32)
        for k in range(kv_size):
            x = got[k * groups + t].astype(F32)
            squares = squares + x * x
        mean = jnp.sum(squares, axis=1, keepdims=True) / (width * kv_size)
        own = got[kv * groups + t].astype(F32)
        out[t * local : (t + 1) * local, :] = (
            own * lax.rsqrt(mean + EPSILON) * gain[...]
        ).astype(BF16)


def exchange(value, axes):
    return lax.all_to_all(value, axes, split_axis=0, concat_axis=0, tiled=True)


def swap(value):
    return lax.ppermute(value, TP, [(i, i ^ 1) for i in range(lax.axis_size(TP))])


def along(own):
    size = lax.axis_size(TP)
    collected = []
    for step in (1, 3, 2):
        pairs = [(i, (i + 2 * step) % size) for i in range(size)]
        collected.append(lax.ppermute(own, TP, pairs))
    return collected


def on_device(
    tokens,
    token_gain,
    w_query,
    w_down_kv,
    w_rope_key,
    latent_gain,
    w_key_up,
    w_value_up,
    w_out,
    out_gain,
    cache_latent,
    cache_rope,
    lengths,
):
    kv_size = lax.axis_size(KV)
    groups = lax.axis_size(TP)
    everyone = kv_size * groups
    seqs, width = tokens.shape
    local, positions, latent_width = cache_latent.shape
    rope = cache_rope.shape[2]
    nope = w_key_up.shape[2]
    value = w_value_up.shape[2]
    factor = (nope + rope) ** (-0.5)

    others = along(w_query.T)
    tokens, gain, w_down, w_rope, own_query, own = pl.pallas_call(
        collect_kernel,
        out_shape=(
            jax.ShapeDtypeStruct(tokens.shape, BF16),
            jax.ShapeDtypeStruct((1, width), F32),
            jax.ShapeDtypeStruct(w_down_kv.shape, BF16),
            jax.ShapeDtypeStruct((rope, width), BF16),
            jax.ShapeDtypeStruct((nope + rope, width), BF16),
            jax.ShapeDtypeStruct((2 * latent_width + value, nope), BF16),
        ),
        in_specs=[in_hbm()] * 8,
        out_specs=(in_vmem(),) * 6,
        scratch_shapes=[pltpu.SemaphoreType.DMA((8,))],
        compiler_params=params(8),
        name="collect",
    )(
        *keep_in_hbm(
            tokens,
            token_gain[None],
            w_down_kv,
            w_rope_key.T,
            w_query.T,
            w_key_up,
            w_value_up,
            w_out,
        )
    )
    before, after, opposite = along(own)
    near = jnp.stack([own, before, after])
    far = swap(near)
    far_opposite = swap(opposite)
    collected = (near, opposite, far, far_opposite)

    cores = lax.axis_size("core")
    sent_rows = (groups // 2 + groups // 4 + 1) * local
    sent = pl.pallas_call(
        project_kernel,
        out_shape=jax.ShapeDtypeStruct((kv_size * cores, sent_rows, 128), BF16),
        in_specs=[in_vmem()] * 8,
        out_specs=in_vmem(),
        scratch_shapes=[pltpu.VMEM((local, cores * local, 128), F32)],
        compiler_params=params(8),
        name="project",
    )(tokens, gain, own_query, *others, w_down, w_rope)
    got = exchange(sent, FIRST)
    powers = np.arange(0, rope, 2, dtype=np.float64) / rope
    frequencies = np.tile(1.0 / 10000.0**powers, 2)[None].astype(np.float32)
    sent = pl.pallas_call(
        functools.partial(attend_kernel, factor=factor, nope=nope),
        out_shape=jax.ShapeDtypeStruct((kv_size, groups * local + local, value), BF16),
        in_specs=[in_vmem()] * 5 + [in_hbm()] * 5,
        out_specs=in_vmem(),
        scratch_shapes=[
            pltpu.VMEM((1, seqs), jnp.int32),
            pltpu.VMEM((1, rope), F32),
            pltpu.VMEM((1, latent_width), F32),
            pltpu.VMEM((local, positions, latent_width), BF16),
            pltpu.VMEM((local, rope, positions), BF16),
            pltpu.VMEM((groups, local, latent_width), F32),
            pltpu.VMEM((groups, local, rope), F32),
            pltpu.VMEM((local * groups, positions + 128), F32),
            pltpu.VMEM((local * groups, positions), BF16),
            pltpu.VMEM((local, groups, latent_width), F32),
            pltpu.SemaphoreType.DMA((2 * local + 3,)),
        ],
        compiler_params=params(24),
        name="attend",
    )(
        got,
        *collected,
        *keep_in_hbm(
            lengths[None],
            frequencies,
            latent_gain[None],
            cache_latent,
            cache_rope.transpose(0, 2, 1),
        ),
    )
    got = exchange(sent, KV)

    sent = pl.pallas_call(
        functools.partial(
            combine_kernel,
            kv_size=kv_size,
            groups=groups,
            local=local,
            first=2 * latent_width,
        ),
        out_shape=jax.ShapeDtypeStruct((everyone, local, w_out.shape[1]), BF16),
        in_specs=[in_vmem()] * 5,
        out_specs=in_vmem(),
        compiler_params=params(8),
        name="combine",
    )(got, *collected)
    got = exchange(sent, ALL)
    return pl.pallas_call(
        functools.partial(finish_kernel, kv_size=kv_size, groups=groups, local=local),
        out_shape=jax.ShapeDtypeStruct((seqs, w_out.shape[1]), BF16),
        in_specs=[in_vmem(), in_vmem()],
        out_specs=in_vmem(),
        compiler_params=params(8),
        name="finish",
    )(got, out_gain[None])


def solution(mesh):
    finer = Mesh(mesh.devices.reshape(4, 4, mesh.shape["tp"] // 2, 2), ALL)

    return jax.shard_map(
        on_device,
        mesh=finer,
        in_specs=(
            P(None, KV),
            P(KV),
            P(KV, TP),
            P(KV, None),
            P(KV, None),
            P(),
            P(TP, None, None),
            P(TP, None, None),
            P(TP, KV),
            P(KV),
            P(TP, KV, None),
            P(TP, KV, None),
            P(),
        ),
        out_specs=P(None, KV),
        check_vma=False,
    )
```

```python
import functools

import jax
import jax.numpy as jnp
import numpy as np
from jax import lax
from jax.experimental import pallas as pl
from jax.experimental.pallas import tpu as pltpu
from jax.sharding import Mesh
from jax.sharding import PartitionSpec as P


KV = ("kv_0", "kv_1")
TP = ("y", "core")
ALL = KV + TP
FIRST = KV + ("core",)
EPSILON = 1e-06
NEGATIVE = -1e30
PARTS = 2
F32 = jnp.float32
BF16 = jnp.bfloat16

NT = (((1,), (1,)), ((), ()))
NN = (((1,), (0,)), ((), ()))


def dot(a, b, dims):
    return lax.dot_general(a, b, dims, preferred_element_type=F32)


def params(mib):
    return pltpu.CompilerParams(vmem_limit_bytes=mib * 1024 * 1024)


def in_vmem():
    return pl.BlockSpec(memory_space=pltpu.VMEM)


def in_hbm():
    return pl.BlockSpec(memory_space=pltpu.HBM)


def keep_in_hbm(*arrays):
    return [pltpu.with_memory_space_constraint(x, pltpu.HBM) for x in arrays]


def lanes(shape):
    return lax.broadcasted_iota(jnp.int32, shape, 1)


def rows(shape):
    return lax.broadcasted_iota(jnp.int32, shape, 0)


def collect_kernel(
    tokens_, gain_, wd_, wr_, wq_, wk, wv, wo, tokens, gain, wd, wr, wq, own, late, sems
):
    deep = wk.shape[1]
    pairs = (
        (wk.at[0], own.at[pl.ds(0, deep)]),
        (wv.at[0], own.at[pl.ds(deep, deep)]),
        (wo, own.at[pl.ds(2 * deep, wo.shape[0])]),
        (tokens_, tokens),
        (gain_, gain),
        (wd_, wd),
        (wr_, wr),
        (wq_, wq),
        (wv.at[0], late.at[pl.ds(0, deep)]),
        (wo, late.at[pl.ds(deep, wo.shape[0])]),
    )
    copies = [pltpu.make_async_copy(x, y, sems.at[n]) for n, (x, y) in enumerate(pairs)]
    for copy in copies:
        copy.start()
    for copy in copies:
        copy.wait()


def project_kernel(tokens, gain, query_0, query_1, query_2, query_3, wd, wr, out, news):
    cores = lax.axis_size("core")
    local = news.shape[1] // cores
    chip = cores * local
    width = wr.shape[0]
    start = pl.multiple_of(lax.axis_index("y") * chip, chip)
    mine = tokens[pl.ds(start, chip), :]
    scaled = (mine.astype(F32) * gain[...]).astype(BF16)
    latent = dot(scaled, wd[...], NN)
    rope = dot(scaled, wr[...], NT)
    pieces = latent.shape[1] // 128
    for n in range(pieces):
        news[n] = latent[:, n * 128 : (n + 1) * 128]
    news[pieces] = jnp.concatenate([rope, jnp.zeros((chip, 128 - width), F32)], axis=1)
    for n in range(pieces + 1, local):
        news[n] = jnp.zeros((chip, 128), F32)
    queries = [dot(scaled, w[...], NT) for w in (query_0, query_1, query_2, query_3)]
    half = len(queries) // 2
    tiles = [q[:, :128] for q in queries] + [
        jnp.concatenate([queries[i][:, 128:], queries[i + half][:, 128:]], axis=1)
        for i in range(half)
    ]
    tiles = [
        [tile[c * local : (c + 1) * local].astype(BF16) for c in range(cores)] for tile in tiles
    ]
    for j in range(local):
        for c in range(cores):
            new = news[:, c * local + j, :].astype(BF16)
            for copy in range(out.shape[0] // cores // local):
                k = copy * local + j
                for n, tile in enumerate(tiles):
                    out[k * cores + c, n * local : (n + 1) * local, :] = tile[c]
                out[k * cores + c, len(tiles) * local :, :] = new


def rotate(values, cosine, sine):
    half = values.shape[1] // 2
    swapped = jnp.concatenate([values[:, half:], values[:, :half]], axis=1)
    return values * cosine + swapped * sine


def attend_kernel(
    got, near, key, far, far_key, lengths_, frequencies_, gain_, latents, ropes,
    means, packed, lengths, frequencies, gain, cache, cache_rope,
    lifted, turned, scored, weights, sems,
    *, factor, nope,
):
    kv = lax.axis_index(KV)
    tp = lax.axis_index(TP)
    kv_size = lax.axis_size(KV)
    groups = lax.axis_size(TP)
    local, positions, latent_width = cache.shape
    width = cache_rope.shape[1]
    small = []
    for n, (a, b) in enumerate(
        ((lengths_, lengths), (frequencies_, frequencies), (gain_, gain))
    ):
        small.append(pltpu.make_async_copy(a, b, sems.at[2 * local + n]))
        small[n].start()
    copies = []
    for s in range(local):
        a = pltpu.make_async_copy(latents.at[s], cache.at[s], sems.at[s])
        b = pltpu.make_async_copy(ropes.at[s], cache_rope.at[s], sems.at[local + s])
        a.start()
        b.start()
        copies.append((a, b))
    cores = lax.axis_size("core")
    core = lax.axis_index("core")
    half = groups // 2

    def total(source, n):
        rows_of = slice(n * local, (n + 1) * local)
        result = got[source, rows_of, :].astype(F32)
        for k in range(1, kv_size):
            result = result + got[k * cores + source, rows_of, :].astype(F32)
        return result

    for copy in small:
        copy.wait()
    shape = (local, lengths.shape[1])
    length = jnp.sum(
        jnp.where(lanes(shape) == rows(shape) + tp * local, lengths[...], 0), axis=1, keepdims=True
    )
    lane = lanes((local, width))
    angles = length.astype(F32) * frequencies[...]
    cosine = jnp.cos(angles)
    sine = jnp.sin(angles)
    sine = jnp.where(lane < width // 2, -sine, sine)
    for i in range(groups):
        source = core if i < half else 1 - core
        w = weights_of((near, key, far, far_key), i, 0, latent_width)
        lifted[i] = dot(total(source, i % half).astype(BF16), w[...], NT)
    for i in range(groups):
        if i % half >= half // 2:
            continue
        source = core if i < half else 1 - core
        both = total(source, half + i % half).astype(BF16).astype(F32)
        turned[i] = rotate(both[:, :width], cosine, sine)
        turned[i + half // 2] = rotate(both[:, width:], cosine, sine)
    fresh = total(0, half + half // 2)
    pieces = latent_width // nope
    raw = jnp.concatenate([fresh[n : n + 1] for n in range(pieces)], axis=1)
    rope_raw = fresh[pieces : pieces + 1, :width]
    square = jnp.sum(raw * raw, axis=1, keepdims=True) / latent_width
    new_latent = (raw * lax.rsqrt(square + EPSILON) * gain[...]).astype(BF16).astype(F32)
    new_seq = lax.rem(kv, local)
    mine = rows((local, width)) == new_seq
    new_rope = rotate(
        rope_raw,
        jnp.sum(jnp.where(mine, cosine, 0.0), axis=0, keepdims=True),
        jnp.sum(jnp.where(mine, sine, 0.0), axis=0, keepdims=True),
    )
    new_rope = new_rope.astype(BF16).astype(F32)
    table = jnp.zeros((groups, 128), F32)
    for start in range(0, local, local // PARTS):
        members = range(start, start + local // PARTS)
        pairs = len(members) * groups
        for s in members:
            q = lifted[:, s, :].astype(BF16)
            qr = turned[:, s, :].astype(BF16)
            own = jnp.sum(q.astype(F32) * new_latent, axis=1, keepdims=True) + jnp.sum(
                qr.astype(F32) * new_rope, axis=1, keepdims=True
            )
            for copy in copies[s]:
                copy.wait()
            r = slice(s * groups, (s + 1) * groups)
            scored[r, :positions] = dot(q, cache[s], NT) + dot(qr, cache_rope[s], NN)
            scored[r, positions:] = jnp.broadcast_to(own, (groups, 128))
        these = slice(start * groups, start * groups + pairs)
        scores = scored[these, :positions] * factor
        sequence = rows((pairs, 1)) // groups + start
        limit = jnp.zeros((pairs, 1), jnp.int32)
        for s in members:
            limit = jnp.where(sequence == s, length[s : s + 1, :], limit)
        is_new = jnp.logical_and(sequence == new_seq, kv < local)
        new = jnp.where(is_new, scored[these, positions : positions + 1] * factor, NEGATIVE)
        visible = kv * positions + lanes((pairs, positions)) < limit
        top = jnp.max(jnp.where(visible, scores, NEGATIVE), axis=1, keepdims=True)
        top = jnp.maximum(top, new)
        weight = jnp.where(visible, jnp.exp(scores - top), 0.0)
        new_weight = jnp.where(is_new, jnp.exp(new - top), 0.0)
        total_weight = jnp.sum(weight, axis=1, keepdims=True) + new_weight
        weights[these, :] = weight.astype(BF16)
        some = total_weight > 0.0
        safe = jnp.where(some, total_weight, 1.0)
        inverse = 1.0 / safe
        logs = jnp.where(some, top + jnp.log(safe), NEGATIVE)
        rounded = new_weight.astype(BF16).astype(F32)
        for n, s in enumerate(members):
            r = slice(n * groups, (n + 1) * groups)
            mixed = dot(weights[s * groups : (s + 1) * groups, :], cache[s], NN)
            means[s] = (mixed + rounded[r] * new_latent) * inverse[r]
            table = jnp.where(lanes((groups, 128)) == s, logs[r], table)
    lane = lanes((local, 128))
    table = jnp.concatenate([table, jnp.zeros((128 - groups, 128), F32)], axis=0)
    table = jnp.transpose(table)[:local]
    high = table.astype(BF16).astype(F32)
    rest = table - high
    middle = rest.astype(BF16).astype(F32)
    low = (rest - middle).astype(BF16).astype(F32)
    packed[...] = jnp.where(
        lane < groups,
        high,
        jnp.where(
            lane < 2 * groups,
            pltpu.roll(middle, groups, 1),
            jnp.where(lane < 3 * groups, pltpu.roll(low, 2 * groups, 1), 0.0),
        ),
    ).astype(BF16)


def up_kernel(means, packed, near, late, far, far_late, out):
    local, groups, latent_width = means.shape
    kv_size = out.shape[0]
    for i in range(groups):
        w = weights_of((near, late, far, far_late), i, latent_width, latent_width)
        x = means[:, i, :].astype(BF16)
        up = dot(x, w[:latent_width, :], NN).astype(BF16)
        for k in range(kv_size):
            out[k, i * local : (i + 1) * local, :] = up
    logs = packed[...]
    for k in range(kv_size):
        out[k, groups * local :, :] = logs


def weights_of(collected, i, first, count):
    near, single, far, far_single = collected
    places = near.shape[0] + 1
    if i % places == places - 1:
        return single if i < places else far_single
    return (near if i < places else far).at[i % places, pl.ds(first, count)]


def combine_kernel(got, near, late, far, far_late, out, *, kv_size, groups, local, first):
    logs = []
    for k in range(kv_size):
        x = got[k, groups * local :, :].astype(F32)
        logs.append(x + pltpu.roll(x, 128 - groups, 1) + pltpu.roll(x, 128 - 2 * groups, 1))
    top = functools.reduce(jnp.maximum, logs)
    shares = [jnp.exp(x - top) for x in logs]
    total = functools.reduce(jnp.add, shares)
    inverse = 1.0 / total
    shares = [x * inverse for x in shares]
    mixed = jnp.zeros((local, out.shape[2]), F32)
    for i in range(groups):
        head = jnp.zeros((local, 128), F32)
        for k in range(kv_size):
            part = got[k, i * local : (i + 1) * local, :].astype(F32)
            head = head + part * shares[k][:, i : i + 1]
        w = weights_of((near, late, far, far_late), i, first, 128)
        single = w.shape[0] > 128
        rows_of = w[late.shape[0] - 128 :, :] if single else w[...]
        mixed = mixed + dot(head.astype(BF16), rows_of, NN)
    mixed = mixed.astype(BF16)
    for d in range(out.shape[0]):
        out[d] = mixed


def finish_kernel(got, gain, out, *, kv_size, groups, local):
    kv = lax.axis_index(KV)
    width = got.shape[2]
    for t in range(groups):
        squares = jnp.zeros((local, width), F32)
        for k in range(kv_size):
            x = got[k * groups + t].astype(F32)
            squares = squares + x * x
        mean = jnp.sum(squares, axis=1, keepdims=True) / (width * kv_size)
        own = got[kv * groups + t].astype(F32)
        out[t * local : (t + 1) * local, :] = (
            own * lax.rsqrt(mean + EPSILON) * gain[...]
        ).astype(BF16)


def exchange(value, axes):
    return lax.all_to_all(value, axes, split_axis=0, concat_axis=0, tiled=True)


def swap(value):
    return lax.ppermute(value, TP, [(i, i ^ 1) for i in range(lax.axis_size(TP))])


def along(own, steps):
    size = lax.axis_size(TP)
    collected = []
    for step in steps:
        pairs = [(i, (i + 2 * step) % size) for i in range(size)]
        collected.append(lax.ppermute(own, TP, pairs))
    return collected


def on_device(
    tokens,
    token_gain,
    w_query,
    w_down_kv,
    w_rope_key,
    latent_gain,
    w_key_up,
    w_value_up,
    w_out,
    out_gain,
    cache_latent,
    cache_rope,
    lengths,
):
    kv_size = lax.axis_size(KV)
    groups = lax.axis_size(TP)
    everyone = kv_size * groups
    seqs, width = tokens.shape
    local, positions, latent_width = cache_latent.shape
    rope = cache_rope.shape[2]
    nope = w_key_up.shape[2]
    value = w_value_up.shape[2]
    factor = (nope + rope) ** (-0.5)

    others = along(w_query.T, (1, 3, 2))
    tokens, gain, w_down, w_rope, own_query, own, late = pl.pallas_call(
        collect_kernel,
        out_shape=(
            jax.ShapeDtypeStruct(tokens.shape, BF16),
            jax.ShapeDtypeStruct((1, width), F32),
            jax.ShapeDtypeStruct(w_down_kv.shape, BF16),
            jax.ShapeDtypeStruct((rope, width), BF16),
            jax.ShapeDtypeStruct((nope + rope, width), BF16),
            jax.ShapeDtypeStruct((2 * latent_width + value, nope), BF16),
            jax.ShapeDtypeStruct((latent_width + value, nope), BF16),
        ),
        in_specs=[in_hbm()] * 8,
        out_specs=(in_vmem(),) * 7,
        scratch_shapes=[pltpu.SemaphoreType.DMA((10,))],
        compiler_params=params(8),
        name="collect",
    )(
        *keep_in_hbm(
            tokens,
            token_gain[None],
            w_down_kv,
            w_rope_key.T,
            w_query.T,
            w_key_up,
            w_value_up,
            w_out,
        )
    )
    near = jnp.stack([own] + along(own, (1, 3)))
    (key,) = along(w_key_up[0], (2,))
    (late,) = along(late, (2,))
    far = swap(near)
    far_key = swap(key)
    far_late = swap(late)

    cores = lax.axis_size("core")
    sent_rows = (groups // 2 + groups // 4 + 1) * local
    sent = pl.pallas_call(
        project_kernel,
        out_shape=jax.ShapeDtypeStruct((kv_size * cores, sent_rows, 128), BF16),
        in_specs=[in_vmem()] * 8,
        out_specs=in_vmem(),
        scratch_shapes=[pltpu.VMEM((local, cores * local, 128), F32)],
        compiler_params=params(8),
        name="project",
    )(tokens, gain, own_query, *others, w_down, w_rope)
    got = exchange(sent, FIRST)
    powers = np.arange(0, rope, 2, dtype=np.float64) / rope
    frequencies = np.tile(1.0 / 10000.0**powers, 2)[None].astype(np.float32)
    means, packed = pl.pallas_call(
        functools.partial(attend_kernel, factor=factor, nope=nope),
        out_shape=(
            jax.ShapeDtypeStruct((local, groups, latent_width), F32),
            jax.ShapeDtypeStruct((local, 128), BF16),
        ),
        in_specs=[in_vmem()] * 5 + [in_hbm()] * 5,
        out_specs=(in_vmem(),) * 2,
        scratch_shapes=[
            pltpu.VMEM((1, seqs), jnp.int32),
            pltpu.VMEM((1, rope), F32),
            pltpu.VMEM((1, latent_width), F32),
            pltpu.VMEM((local, positions, latent_width), BF16),
            pltpu.VMEM((local, rope, positions), BF16),
            pltpu.VMEM((groups, local, latent_width), F32),
            pltpu.VMEM((groups, local, rope), F32),
            pltpu.VMEM((local * groups, positions + 128), F32),
            pltpu.VMEM((local * groups, positions), BF16),
            pltpu.SemaphoreType.DMA((2 * local + 3,)),
        ],
        compiler_params=params(24),
        name="attend",
    )(
        got,
        near,
        key,
        far,
        far_key,
        *keep_in_hbm(
            lengths[None],
            frequencies,
            latent_gain[None],
            cache_latent,
            cache_rope.transpose(0, 2, 1),
        ),
    )
    sent = pl.pallas_call(
        up_kernel,
        out_shape=jax.ShapeDtypeStruct((kv_size, groups * local + local, value), BF16),
        in_specs=[in_vmem()] * 6,
        out_specs=in_vmem(),
        compiler_params=params(8),
        name="value_up",
    )(means, packed, near, late, far, far_late)
    got = exchange(sent, KV)

    sent = pl.pallas_call(
        functools.partial(
            combine_kernel,
            kv_size=kv_size,
            groups=groups,
            local=local,
            first=2 * latent_width,
        ),
        out_shape=jax.ShapeDtypeStruct((everyone, local, w_out.shape[1]), BF16),
        in_specs=[in_vmem()] * 5,
        out_specs=in_vmem(),
        compiler_params=params(8),
        name="combine",
    )(got, near, late, far, far_late)
    got = exchange(sent, ALL)
    return pl.pallas_call(
        functools.partial(finish_kernel, kv_size=kv_size, groups=groups, local=local),
        out_shape=jax.ShapeDtypeStruct((seqs, w_out.shape[1]), BF16),
        in_specs=[in_vmem(), in_vmem()],
        out_specs=in_vmem(),
        compiler_params=params(8),
        name="finish",
    )(got, out_gain[None])


def solution(mesh):
    finer = Mesh(mesh.devices.reshape(4, 4, mesh.shape["tp"] // 2, 2), ALL)

    return jax.shard_map(
        on_device,
        mesh=finer,
        in_specs=(
            P(None, KV),
            P(KV),
            P(KV, TP),
            P(KV, None),
            P(KV, None),
            P(),
            P(TP, None, None),
            P(TP, None, None),
            P(TP, KV),
            P(KV),
            P(TP, KV, None),
            P(TP, KV, None),
            P(),
        ),
        out_specs=P(None, KV),
        check_vma=False,
    )
```

```python
import functools

import jax
import jax.numpy as jnp
import numpy as np
from jax import lax
from jax.experimental import pallas as pl
from jax.experimental.pallas import tpu as pltpu
from jax.sharding import Mesh
from jax.sharding import PartitionSpec as P


KV = ("kv_0", "kv_1")
TP = ("y", "core")
ALL = KV + TP
LAST = ("core",) + KV + ("y",)
FIRST = KV + ("core",)
EPSILON = 1e-06
NEGATIVE = -1e30
PARTS = 2
F32 = jnp.float32
BF16 = jnp.bfloat16

NT = (((1,), (1,)), ((), ()))
NN = (((1,), (0,)), ((), ()))


def dot(a, b, dims):
    return lax.dot_general(a, b, dims, preferred_element_type=F32)


def params(mib):
    return pltpu.CompilerParams(vmem_limit_bytes=mib * 1024 * 1024)


def in_vmem():
    return pl.BlockSpec(memory_space=pltpu.VMEM)


def in_hbm():
    return pl.BlockSpec(memory_space=pltpu.HBM)


def keep_in_hbm(*arrays):
    return [pltpu.with_memory_space_constraint(x, pltpu.HBM) for x in arrays]


def lanes(shape):
    return lax.broadcasted_iota(jnp.int32, shape, 1)


def rows(shape):
    return lax.broadcasted_iota(jnp.int32, shape, 0)


def collect_kernel(
    tokens_, gain_, wd_, wr_, wq_, wk, wv, wo, tokens, gain, wd, wr, wq, own, sems
):
    deep = wk.shape[1]
    pairs = (
        (wk.at[0], own.at[pl.ds(0, deep)]),
        (wv.at[0], own.at[pl.ds(deep, deep)]),
        (wo, own.at[pl.ds(2 * deep, wo.shape[0])]),
        (tokens_, tokens),
        (gain_, gain),
        (wd_, wd),
        (wr_, wr),
        (wq_, wq),
    )
    copies = [pltpu.make_async_copy(x, y, sems.at[n]) for n, (x, y) in enumerate(pairs)]
    for copy in copies:
        copy.start()
    for copy in copies:
        copy.wait()


def project_kernel(tokens, gain, query_0, query_1, query_2, query_3, wd, wr, out, news):
    cores = lax.axis_size("core")
    local = news.shape[1] // cores
    chip = cores * local
    width = wr.shape[0]
    start = pl.multiple_of(lax.axis_index("y") * chip, chip)
    mine = tokens[pl.ds(start, chip), :]
    scaled = (mine.astype(F32) * gain[...]).astype(BF16)
    latent = dot(scaled, wd[...], NN)
    rope = dot(scaled, wr[...], NT)
    pieces = latent.shape[1] // 128
    for n in range(pieces):
        news[n] = latent[:, n * 128 : (n + 1) * 128]
    news[pieces] = jnp.concatenate([rope, jnp.zeros((chip, 128 - width), F32)], axis=1)
    for n in range(pieces + 1, local):
        news[n] = jnp.zeros((chip, 128), F32)
    queries = [dot(scaled, w[...], NT) for w in (query_0, query_1, query_2, query_3)]
    half = len(queries) // 2
    tiles = [q[:, :128] for q in queries] + [
        jnp.concatenate([queries[i][:, 128:], queries[i + half][:, 128:]], axis=1)
        for i in range(half)
    ]
    tiles = [
        [tile[c * local : (c + 1) * local].astype(BF16) for c in range(cores)] for tile in tiles
    ]
    for j in range(local):
        for c in range(cores):
            new = news[:, c * local + j, :].astype(BF16)
            for copy in range(out.shape[0] // cores // local):
                k = copy * local + j
                for n, tile in enumerate(tiles):
                    out[k * cores + c, n * local : (n + 1) * local, :] = tile[c]
                out[k * cores + c, len(tiles) * local :, :] = new


def rotate(values, cosine, sine):
    half = values.shape[1] // 2
    swapped = jnp.concatenate([values[:, half:], values[:, :half]], axis=1)
    return values * cosine + swapped * sine


def attend_kernel(
    got, near, opposite, far, far_opposite, lengths_, frequencies_, gain_, latents, ropes,
    out, lengths, frequencies, gain, cache, cache_rope,
    lifted, turned, scored, weights, means, sems,
    *, factor, nope,
):
    kv = lax.axis_index(KV)
    tp = lax.axis_index(TP)
    kv_size = lax.axis_size(KV)
    groups = lax.axis_size(TP)
    local, positions, latent_width = cache.shape
    width = cache_rope.shape[1]
    small = []
    for n, (a, b) in enumerate(
        ((lengths_, lengths), (frequencies_, frequencies), (gain_, gain))
    ):
        small.append(pltpu.make_async_copy(a, b, sems.at[2 * local + n]))
        small[n].start()
    copies = []
    for s in range(local):
        a = pltpu.make_async_copy(latents.at[s], cache.at[s], sems.at[s])
        b = pltpu.make_async_copy(ropes.at[s], cache_rope.at[s], sems.at[local + s])
        a.start()
        b.start()
        copies.append((a, b))
    cores = lax.axis_size("core")
    core = lax.axis_index("core")
    half = groups // 2

    def total(source, n):
        rows_of = slice(n * local, (n + 1) * local)
        result = got[source, rows_of, :].astype(F32)
        for k in range(1, kv_size):
            result = result + got[k * cores + source, rows_of, :].astype(F32)
        return result

    for copy in small:
        copy.wait()
    shape = (local, lengths.shape[1])
    length = jnp.sum(
        jnp.where(lanes(shape) == rows(shape) + tp * local, lengths[...], 0), axis=1, keepdims=True
    )
    lane = lanes((local, width))
    angles = length.astype(F32) * frequencies[...]
    cosine = jnp.cos(angles)
    sine = jnp.sin(angles)
    sine = jnp.where(lane < width // 2, -sine, sine)
    for i in range(groups):
        source = core if i < half else 1 - core
        w = weights_of((near, opposite, far, far_opposite), i)
        lifted[i] = dot(total(source, i % half).astype(BF16), w[:latent_width, :], NT)
    for i in range(groups):
        if i % half >= half // 2:
            continue
        source = core if i < half else 1 - core
        both = total(source, half + i % half).astype(BF16).astype(F32)
        turned[i] = rotate(both[:, :width], cosine, sine)
        turned[i + half // 2] = rotate(both[:, width:], cosine, sine)
    fresh = total(0, half + half // 2)
    pieces = latent_width // nope
    raw = jnp.concatenate([fresh[n : n + 1] for n in range(pieces)], axis=1)
    rope_raw = fresh[pieces : pieces + 1, :width]
    square = jnp.sum(raw * raw, axis=1, keepdims=True) / latent_width
    new_latent = (raw * lax.rsqrt(square + EPSILON) * gain[...]).astype(BF16).astype(F32)
    new_seq = lax.rem(kv, local)
    mine = rows((local, width)) == new_seq
    new_rope = rotate(
        rope_raw,
        jnp.sum(jnp.where(mine, cosine, 0.0), axis=0, keepdims=True),
        jnp.sum(jnp.where(mine, sine, 0.0), axis=0, keepdims=True),
    )
    new_rope = new_rope.astype(BF16).astype(F32)
    table = jnp.zeros((groups, 128), F32)
    for start in range(0, local, local // PARTS):
        members = range(start, start + local // PARTS)
        pairs = len(members) * groups
        for s in members:
            q = lifted[:, s, :].astype(BF16)
            qr = turned[:, s, :].astype(BF16)
            own = jnp.sum(q.astype(F32) * new_latent, axis=1, keepdims=True) + jnp.sum(
                qr.astype(F32) * new_rope, axis=1, keepdims=True
            )
            for copy in copies[s]:
                copy.wait()
            r = slice(s * groups, (s + 1) * groups)
            scored[r, :positions] = dot(q, cache[s], NT) + dot(qr, cache_rope[s], NN)
            scored[r, positions:] = jnp.broadcast_to(own, (groups, 128))
        these = slice(start * groups, start * groups + pairs)
        scores = scored[these, :positions] * factor
        sequence = rows((pairs, 1)) // groups + start
        limit = jnp.zeros((pairs, 1), jnp.int32)
        for s in members:
            limit = jnp.where(sequence == s, length[s : s + 1, :], limit)
        is_new = jnp.logical_and(sequence == new_seq, kv < local)
        new = jnp.where(is_new, scored[these, positions : positions + 1] * factor, NEGATIVE)
        visible = kv * positions + lanes((pairs, positions)) < limit
        top = jnp.max(jnp.where(visible, scores, NEGATIVE), axis=1, keepdims=True)
        top = jnp.maximum(top, new)
        weight = jnp.where(visible, jnp.exp(scores - top), 0.0)
        new_weight = jnp.where(is_new, jnp.exp(new - top), 0.0)
        total_weight = jnp.sum(weight, axis=1, keepdims=True) + new_weight
        weights[these, :] = weight.astype(BF16)
        some = total_weight > 0.0
        safe = jnp.where(some, total_weight, 1.0)
        inverse = 1.0 / safe
        logs = jnp.where(some, top + jnp.log(safe), NEGATIVE)
        rounded = new_weight.astype(BF16).astype(F32)
        for n, s in enumerate(members):
            r = slice(n * groups, (n + 1) * groups)
            mixed = dot(weights[s * groups : (s + 1) * groups, :], cache[s], NN)
            means[s] = (mixed + rounded[r] * new_latent) * inverse[r]
            table = jnp.where(lanes((groups, 128)) == s, logs[r], table)
    for i in range(groups):
        w = weights_of((near, opposite, far, far_opposite), i)
        x = means[:, i, :].astype(BF16)
        up = dot(x, w[latent_width : 2 * latent_width, :], NN).astype(BF16)
        for k in range(kv_size):
            out[k, i * local : (i + 1) * local, :] = up
    lane = lanes((local, 128))
    table = jnp.concatenate([table, jnp.zeros((128 - groups, 128), F32)], axis=0)
    table = jnp.transpose(table)[:local]
    high = table.astype(BF16).astype(F32)
    rest = table - high
    middle = rest.astype(BF16).astype(F32)
    low = (rest - middle).astype(BF16).astype(F32)
    packed = jnp.where(
        lane < groups,
        high,
        jnp.where(
            lane < 2 * groups,
            pltpu.roll(middle, groups, 1),
            jnp.where(lane < 3 * groups, pltpu.roll(low, 2 * groups, 1), 0.0),
        ),
    ).astype(BF16)
    for k in range(kv_size):
        out[k, groups * local :, :] = packed


def weights_of(collected, i):
    near, opposite, far, far_opposite = collected
    places = near.shape[0] + 1
    stacked, single = (near, opposite) if i < places else (far, far_opposite)
    return single if i % places == places - 1 else stacked.at[i % places]


def combine_kernel(got, near, opposite, far, far_opposite, out, *, kv_size, groups, local, first):
    logs = []
    for k in range(kv_size):
        x = got[k, groups * local :, :].astype(F32)
        logs.append(x + pltpu.roll(x, 128 - groups, 1) + pltpu.roll(x, 128 - 2 * groups, 1))
    top = functools.reduce(jnp.maximum, logs)
    shares = [jnp.exp(x - top) for x in logs]
    total = functools.reduce(jnp.add, shares)
    inverse = 1.0 / total
    shares = [x * inverse for x in shares]
    mixed = jnp.zeros((local, out.shape[2]), F32)
    for i in range(groups):
        head = jnp.zeros((local, 128), F32)
        for k in range(kv_size):
            part = got[k, i * local : (i + 1) * local, :].astype(F32)
            head = head + part * shares[k][:, i : i + 1]
        w = weights_of((near, opposite, far, far_opposite), i)
        mixed = mixed + dot(head.astype(BF16), w[first:, :], NN)
    mixed = mixed.astype(BF16)
    for d in range(out.shape[0]):
        out[d] = mixed


def finish_kernel(got, gain, out, *, kv_size, groups, local):
    kv = lax.axis_index(KV)
    cores = lax.axis_size("core")
    places = groups // cores
    width = got.shape[2]
    for t in range(groups):
        y, core = t // cores, t % cores
        squares = jnp.zeros((local, width), F32)
        for k in range(kv_size):
            x = got[(core * kv_size + k) * places + y].astype(F32)
            squares = squares + x * x
        mean = jnp.sum(squares, axis=1, keepdims=True) / (width * kv_size)
        own = got[(core * kv_size + kv) * places + y].astype(F32)
        out[t * local : (t + 1) * local, :] = (
            own * lax.rsqrt(mean + EPSILON) * gain[...]
        ).astype(BF16)


def exchange(value, axes):
    return lax.all_to_all(value, axes, split_axis=0, concat_axis=0, tiled=True)


def swap(value):
    return lax.ppermute(value, TP, [(i, i ^ 1) for i in range(lax.axis_size(TP))])


def along(own):
    size = lax.axis_size(TP)
    collected = []
    for step in (1, 3, 2):
        pairs = [(i, (i + (2 - 4 * (i % 2)) * step) % size) for i in range(size)]
        collected.append(lax.ppermute(own, TP, pairs))
    return collected


def on_device(
    tokens,
    token_gain,
    w_query,
    w_down_kv,
    w_rope_key,
    latent_gain,
    w_key_up,
    w_value_up,
    w_out,
    out_gain,
    cache_latent,
    cache_rope,
    lengths,
):
    kv_size = lax.axis_size(KV)
    groups = lax.axis_size(TP)
    everyone = kv_size * groups
    seqs, width = tokens.shape
    local, positions, latent_width = cache_latent.shape
    rope = cache_rope.shape[2]
    nope = w_key_up.shape[2]
    value = w_value_up.shape[2]
    factor = (nope + rope) ** (-0.5)

    others = along(w_query.T)
    tokens, gain, w_down, w_rope, own_query, own = pl.pallas_call(
        collect_kernel,
        out_shape=(
            jax.ShapeDtypeStruct(tokens.shape, BF16),
            jax.ShapeDtypeStruct((1, width), F32),
            jax.ShapeDtypeStruct(w_down_kv.shape, BF16),
            jax.ShapeDtypeStruct((rope, width), BF16),
            jax.ShapeDtypeStruct((nope + rope, width), BF16),
            jax.ShapeDtypeStruct((2 * latent_width + value, nope), BF16),
        ),
        in_specs=[in_hbm()] * 8,
        out_specs=(in_vmem(),) * 6,
        scratch_shapes=[pltpu.SemaphoreType.DMA((8,))],
        compiler_params=params(8),
        name="collect",
    )(
        *keep_in_hbm(
            tokens,
            token_gain[None],
            w_down_kv,
            w_rope_key.T,
            w_query.T,
            w_key_up,
            w_value_up,
            w_out,
        )
    )
    before, after, opposite = along(own)
    near = jnp.stack([own, before, after])
    far = swap(near)
    far_opposite = swap(opposite)
    collected = (near, opposite, far, far_opposite)

    cores = lax.axis_size("core")
    sent_rows = (groups // 2 + groups // 4 + 1) * local
    sent = pl.pallas_call(
        project_kernel,
        out_shape=jax.ShapeDtypeStruct((kv_size * cores, sent_rows, 128), BF16),
        in_specs=[in_vmem()] * 8,
        out_specs=in_vmem(),
        scratch_shapes=[pltpu.VMEM((local, cores * local, 128), F32)],
        compiler_params=params(8),
        name="project",
    )(tokens, gain, own_query, *others, w_down, w_rope)
    got = exchange(sent, FIRST)
    powers = np.arange(0, rope, 2, dtype=np.float64) / rope
    frequencies = np.tile(1.0 / 10000.0**powers, 2)[None].astype(np.float32)
    sent = pl.pallas_call(
        functools.partial(attend_kernel, factor=factor, nope=nope),
        out_shape=jax.ShapeDtypeStruct((kv_size, groups * local + local, value), BF16),
        in_specs=[in_vmem()] * 5 + [in_hbm()] * 5,
        out_specs=in_vmem(),
        scratch_shapes=[
            pltpu.VMEM((1, seqs), jnp.int32),
            pltpu.VMEM((1, rope), F32),
            pltpu.VMEM((1, latent_width), F32),
            pltpu.VMEM((local, positions, latent_width), BF16),
            pltpu.VMEM((local, rope, positions), BF16),
            pltpu.VMEM((groups, local, latent_width), F32),
            pltpu.VMEM((groups, local, rope), F32),
            pltpu.VMEM((local * groups, positions + 128), F32),
            pltpu.VMEM((local * groups, positions), BF16),
            pltpu.VMEM((local, groups, latent_width), F32),
            pltpu.SemaphoreType.DMA((2 * local + 3,)),
        ],
        compiler_params=params(24),
        name="attend",
    )(
        got,
        *collected,
        *keep_in_hbm(
            lengths[None],
            frequencies,
            latent_gain[None],
            cache_latent,
            cache_rope.transpose(0, 2, 1),
        ),
    )
    got = exchange(sent, KV)

    sent = pl.pallas_call(
        functools.partial(
            combine_kernel,
            kv_size=kv_size,
            groups=groups,
            local=local,
            first=2 * latent_width,
        ),
        out_shape=jax.ShapeDtypeStruct((everyone, local, w_out.shape[1]), BF16),
        in_specs=[in_vmem()] * 5,
        out_specs=in_vmem(),
        compiler_params=params(8),
        name="combine",
    )(got, *collected)
    got = exchange(sent, LAST)
    return pl.pallas_call(
        functools.partial(finish_kernel, kv_size=kv_size, groups=groups, local=local),
        out_shape=jax.ShapeDtypeStruct((seqs, w_out.shape[1]), BF16),
        in_specs=[in_vmem(), in_vmem()],
        out_specs=in_vmem(),
        compiler_params=params(8),
        name="finish",
    )(got, out_gain[None])


def solution(mesh):
    finer = Mesh(mesh.devices.reshape(4, 4, mesh.shape["tp"] // 2, 2), ALL)

    return jax.shard_map(
        on_device,
        mesh=finer,
        in_specs=(
            P(None, KV),
            P(KV),
            P(KV, TP),
            P(KV, None),
            P(KV, None),
            P(),
            P(TP, None, None),
            P(TP, None, None),
            P(TP, KV),
            P(KV),
            P(TP, KV, None),
            P(TP, KV, None),
            P(),
        ),
        out_specs=P(None, KV),
        check_vma=False,
    )
```

```python
import functools

import jax
import jax.numpy as jnp
import numpy as np
from jax import lax
from jax.experimental import pallas as pl
from jax.experimental.pallas import tpu as pltpu
from jax.sharding import Mesh
from jax.sharding import PartitionSpec as P


KV = ("kv_0", "kv_1")
TP = ("y", "core")
ALL = KV + TP
SPREAD = ("core",) + KV + ("y",)
EPSILON = 1e-06
NEGATIVE = -1e30
F32 = jnp.float32
BF16 = jnp.bfloat16

NT = (((1,), (1,)), ((), ()))
NN = (((1,), (0,)), ((), ()))


def dot(a, b, dims):
    return lax.dot_general(a, b, dims, preferred_element_type=F32)


def params(mib):
    return pltpu.CompilerParams(vmem_limit_bytes=mib * 1024 * 1024)


def in_vmem():
    return pl.BlockSpec(memory_space=pltpu.VMEM)


def in_hbm():
    return pl.BlockSpec(memory_space=pltpu.HBM)


def keep_in_hbm(*arrays):
    return [pltpu.with_memory_space_constraint(x, pltpu.HBM) for x in arrays]


def lanes(shape):
    return lax.broadcasted_iota(jnp.int32, shape, 1)


def rows(shape):
    return lax.broadcasted_iota(jnp.int32, shape, 0)


def block_of(kv, tp, kv_size):
    cores = lax.axis_size("core")
    return (tp % cores * kv_size + kv) * lax.axis_size("y") + tp // cores


def project_kernel(
    tokens, gain, wq, wd, wr, wk, wv, wo, out, own, tokens_, gain_, wq_, wd_, wr_, sems
):
    tp = lax.axis_index(TP)
    groups = lax.axis_size(TP)
    kv_size = lax.axis_size(KV)
    deep = wk.shape[1]
    pairs = (
        (tokens, tokens_),
        (gain, gain_),
        (wq, wq_),
        (wd, wd_),
        (wr, wr_),
        (wk.at[0], own.at[pl.ds(0, deep)]),
        (wv.at[0], own.at[pl.ds(deep, deep)]),
        (wo, own.at[pl.ds(2 * deep, wo.shape[0])]),
    )
    copies = [pltpu.make_async_copy(x, y, sems.at[n]) for n, (x, y) in enumerate(pairs)]
    for copy in copies:
        copy.start()
    for copy in copies[:5]:
        copy.wait()
    scaled = (tokens_[...].astype(F32) * gain_[...]).astype(BF16)
    query = dot(scaled, wq_[...], NT)
    latent = dot(scaled, wd_[...], NN)
    rope = dot(scaled, wr_[...], NT)
    seqs = scaled.shape[0]
    local = seqs // groups
    chunk = latent.shape[1] // groups
    part = latent[:, :chunk]
    for g in range(1, groups):
        part = jnp.where(tp == g, latent[:, g * chunk : (g + 1) * chunk], part)
    width = rope.shape[1]
    rope = jnp.where(lanes(rope.shape) // (width // groups) == tp, rope, 0.0)
    blank = jnp.zeros((seqs, 128 - width), F32)
    part = jnp.concatenate([blank, part], axis=1)
    rope = jnp.concatenate([blank, rope], axis=1)
    first = query[:, :128].astype(BF16)
    second = jnp.concatenate([query[:, 128:], blank], axis=1)
    row = rows((local, 128))
    for t in range(groups):
        top = first[t * local : (t + 1) * local]
        low = second[t * local : (t + 1) * local]
        for j in range(local):
            r = t * local + j
            new = jnp.where(row == 0, part[r : r + 1], 0.0) + jnp.where(row == 1, rope[r : r + 1], 0.0)
            tile = (low + new).astype(BF16)
            for c in range(kv_size // local):
                b = block_of(c * local + j, t, kv_size)
                out[b, :, :128] = top
                out[b, :, 128:] = tile
    for copy in copies[5:]:
        copy.wait()


def rotate(values, cosine, sine):
    half = values.shape[1] // 2
    swapped = jnp.concatenate([values[:, half:], values[:, :half]], axis=1)
    return values * cosine + swapped * sine


def attend_kernel(
    got, near, opposite, far, far_opposite, lengths_, frequencies_, gain_, latents, ropes,
    out, lengths, frequencies, gain, cache, cache_rope,
    sums, lifted, turned, scored, weights, means, sems,
    *, factor, nope,
):
    kv = lax.axis_index(KV)
    tp = lax.axis_index(TP)
    kv_size = lax.axis_size(KV)
    groups = lax.axis_size(TP)
    local, positions, latent_width = cache.shape
    width = cache_rope.shape[1]
    small = []
    for n, (a, b) in enumerate(
        ((lengths_, lengths), (frequencies_, frequencies), (gain_, gain))
    ):
        small.append(pltpu.make_async_copy(a, b, sems.at[2 * local + n]))
        small[n].start()
    copies = []
    for s in range(local):
        a = pltpu.make_async_copy(latents.at[s], cache.at[s], sems.at[s])
        b = pltpu.make_async_copy(ropes.at[s], cache_rope.at[s], sems.at[local + s])
        a.start()
        b.start()
        copies.append((a, b))
    for h in range(groups):
        total = got[block_of(0, h, kv_size)].astype(F32)
        for k in range(1, kv_size):
            total = total + got[block_of(k, h, kv_size)].astype(F32)
        sums[h] = total
    for copy in small:
        copy.wait()
    shape = (local, lengths.shape[1])
    length = jnp.sum(
        jnp.where(lanes(shape) == rows(shape) + tp * local, lengths[...], 0), axis=1, keepdims=True
    )
    lane = lanes((local, width))
    angles = length.astype(F32) * frequencies[...]
    cosine = jnp.cos(angles)
    sine = jnp.sin(angles)
    sine = jnp.where(lane < width // 2, -sine, sine)
    half = groups // 2
    y = tp // 2
    core = lax.rem(tp, 2)
    for i in range(groups):
        step = (0, half - 1, 1, 2)[i % half]
        head = 2 * lax.rem(y + step, half) + (core if i < half else 1 - core)
        q = sums[head]
        w = weights_of((near, opposite, far, far_opposite), i)
        lifted[i] = dot(q[:, :nope].astype(BF16), w[:latent_width, :], NT)
        turned[i] = rotate(q[:, nope : nope + width].astype(BF16).astype(F32), cosine, sine)
    raw = jnp.concatenate([sums[h][0:1, nope + width :] for h in range(groups)], axis=1)
    rope_raw = sums[0][1:2, nope + width :]
    for h in range(1, groups):
        rope_raw = rope_raw + sums[h][1:2, nope + width :]
    square = jnp.sum(raw * raw, axis=1, keepdims=True) / latent_width
    new_latent = (raw * lax.rsqrt(square + EPSILON) * gain[...]).astype(BF16).astype(F32)
    new_seq = lax.rem(kv, local)
    mine = rows((local, width)) == new_seq
    new_rope = rotate(
        rope_raw,
        jnp.sum(jnp.where(mine, cosine, 0.0), axis=0, keepdims=True),
        jnp.sum(jnp.where(mine, sine, 0.0), axis=0, keepdims=True),
    )
    new_rope = new_rope.astype(BF16).astype(F32)
    pairs = local * groups
    for s in range(local):
        q = lifted[:, s, :].astype(BF16)
        qr = turned[:, s, :].astype(BF16)
        fresh = jnp.sum(q.astype(F32) * new_latent, axis=1, keepdims=True) + jnp.sum(
            qr.astype(F32) * new_rope, axis=1, keepdims=True
        )
        for copy in copies[s]:
            copy.wait()
        r = s * groups
        scored[r : r + groups, :positions] = dot(q, cache[s], NT) + dot(qr, cache_rope[s], NN)
        scored[r : r + groups, positions:] = jnp.broadcast_to(fresh, (groups, 128))
    scores = scored[:, :positions] * factor
    row = rows((pairs, 1))
    sequence = row // groups
    limit = jnp.zeros((pairs, 1), jnp.int32)
    for s in range(local):
        limit = jnp.where(sequence == s, length[s : s + 1, :], limit)
    is_new = jnp.logical_and(sequence == new_seq, kv < local)
    new = jnp.where(is_new, scored[:, positions : positions + 1] * factor, NEGATIVE)
    visible = kv * positions + lanes((pairs, positions)) < limit
    top = jnp.max(jnp.where(visible, scores, NEGATIVE), axis=1, keepdims=True)
    top = jnp.maximum(top, new)
    weight = jnp.where(visible, jnp.exp(scores - top), 0.0)
    new_weight = jnp.where(is_new, jnp.exp(new - top), 0.0)
    total = jnp.sum(weight, axis=1, keepdims=True) + new_weight
    weights[...] = weight.astype(BF16)
    some = total > 0.0
    safe = jnp.where(some, total, 1.0)
    inverse = 1.0 / safe
    logs = jnp.where(some, top + jnp.log(safe), NEGATIVE)
    rounded = new_weight.astype(BF16).astype(F32)
    for s in range(local):
        r = slice(s * groups, (s + 1) * groups)
        mixed = dot(weights[r, :], cache[s], NN) + rounded[r] * new_latent
        means[s] = mixed * inverse[r]
    for i in range(groups):
        w = weights_of((near, opposite, far, far_opposite), i)
        x = means[:, i, :].astype(BF16)
        up = dot(x, w[latent_width : 2 * latent_width, :], NN).astype(BF16)
        for k in range(kv_size):
            out[k, i * local : (i + 1) * local, :] = up
    lane = lanes((local, 128))
    table = jnp.zeros((groups, 128), F32)
    for s in range(local):
        table = jnp.where(lanes((groups, 128)) == s, logs[s * groups : (s + 1) * groups], table)
    table = jnp.concatenate([table, jnp.zeros((128 - groups, 128), F32)], axis=0)
    table = jnp.transpose(table)[:local]
    high = table.astype(BF16).astype(F32)
    rest = table - high
    middle = rest.astype(BF16).astype(F32)
    low = (rest - middle).astype(BF16).astype(F32)
    packed = jnp.where(
        lane < groups,
        high,
        jnp.where(
            lane < 2 * groups,
            pltpu.roll(middle, groups, 1),
            jnp.where(lane < 3 * groups, pltpu.roll(low, 2 * groups, 1), 0.0),
        ),
    ).astype(BF16)
    for k in range(kv_size):
        out[k, groups * local :, :] = packed


def weights_of(collected, i):
    near, opposite, far, far_opposite = collected
    places = near.shape[0] + 1
    stacked, single = (near, opposite) if i < places else (far, far_opposite)
    return single if i % places == places - 1 else stacked.at[i % places]


def combine_kernel(got, near, opposite, far, far_opposite, out, *, kv_size, groups, local, first):
    logs = []
    for k in range(kv_size):
        x = got[k, groups * local :, :].astype(F32)
        logs.append(x + pltpu.roll(x, 128 - groups, 1) + pltpu.roll(x, 128 - 2 * groups, 1))
    top = functools.reduce(jnp.maximum, logs)
    shares = [jnp.exp(x - top) for x in logs]
    total = functools.reduce(jnp.add, shares)
    inverse = 1.0 / total
    shares = [x * inverse for x in shares]
    mixed = jnp.zeros((local, out.shape[2]), F32)
    for i in range(groups):
        head = jnp.zeros((local, 128), F32)
        for k in range(kv_size):
            part = got[k, i * local : (i + 1) * local, :].astype(F32)
            head = head + part * shares[k][:, i : i + 1]
        w = weights_of((near, opposite, far, far_opposite), i)
        mixed = mixed + dot(head.astype(BF16), w[first:, :], NN)
    mixed = mixed.astype(BF16)
    for d in range(out.shape[0]):
        out[d] = mixed


def finish_kernel(got, gain, out, *, kv_size, groups, local):
    kv = lax.axis_index(KV)
    width = got.shape[2]
    for t in range(groups):
        squares = jnp.zeros((local, width), F32)
        for k in range(kv_size):
            x = got[block_of(k, t, kv_size)].astype(F32)
            squares = squares + x * x
        mean = jnp.sum(squares, axis=1, keepdims=True) / (width * kv_size)
        own = got[block_of(kv, t, kv_size)].astype(F32)
        out[t * local : (t + 1) * local, :] = (
            own * lax.rsqrt(mean + EPSILON) * gain[...]
        ).astype(BF16)


def exchange(value, axes):
    return lax.all_to_all(value, axes, split_axis=0, concat_axis=0, tiled=True)


def swap(value):
    return lax.ppermute(value, TP, [(i, i ^ 1) for i in range(lax.axis_size(TP))])


def along(own):
    size = lax.axis_size(TP)
    collected = []
    for step in (1, 3, 2):
        pairs = [(i, (i + 2 * step) % size) for i in range(size)]
        collected.append(lax.ppermute(own, TP, pairs))
    return collected


def on_device(
    tokens,
    token_gain,
    w_query,
    w_down_kv,
    w_rope_key,
    latent_gain,
    w_key_up,
    w_value_up,
    w_out,
    out_gain,
    cache_latent,
    cache_rope,
    lengths,
):
    kv_size = lax.axis_size(KV)
    groups = lax.axis_size(TP)
    everyone = kv_size * groups
    seqs, width = tokens.shape
    local, positions, latent_width = cache_latent.shape
    rope = cache_rope.shape[2]
    nope = w_key_up.shape[2]
    value = w_value_up.shape[2]
    factor = (nope + rope) ** (-0.5)

    sent, own = pl.pallas_call(
        project_kernel,
        out_shape=(
            jax.ShapeDtypeStruct((everyone, local, 256), BF16),
            jax.ShapeDtypeStruct((2 * latent_width + value, nope), BF16),
        ),
        in_specs=[in_hbm()] * 8,
        out_specs=(in_vmem(),) * 2,
        scratch_shapes=[
            pltpu.VMEM((seqs, width), BF16),
            pltpu.VMEM((1, width), F32),
            pltpu.VMEM((nope + rope, width), BF16),
            pltpu.VMEM((width, latent_width), BF16),
            pltpu.VMEM((rope, width), BF16),
            pltpu.SemaphoreType.DMA((8,)),
        ],
        compiler_params=params(8),
        name="project",
    )(
        *keep_in_hbm(
            tokens,
            token_gain[None],
            w_query.T,
            w_down_kv,
            w_rope_key.T,
            w_key_up,
            w_value_up,
            w_out,
        )
    )

    before, after, opposite = along(own)
    near = jnp.stack([own, before, after])
    far = swap(near)
    far_opposite = swap(opposite)
    collected = (near, opposite, far, far_opposite)

    got = exchange(sent, SPREAD)
    powers = np.arange(0, rope, 2, dtype=np.float64) / rope
    frequencies = np.tile(1.0 / 10000.0**powers, 2)[None].astype(np.float32)
    sent = pl.pallas_call(
        functools.partial(attend_kernel, factor=factor, nope=nope),
        out_shape=jax.ShapeDtypeStruct((kv_size, groups * local + local, value), BF16),
        in_specs=[in_vmem()] * 5 + [in_hbm()] * 5,
        out_specs=in_vmem(),
        scratch_shapes=[
            pltpu.VMEM((1, seqs), jnp.int32),
            pltpu.VMEM((1, rope), F32),
            pltpu.VMEM((1, latent_width), F32),
            pltpu.VMEM((local, positions, latent_width), BF16),
            pltpu.VMEM((local, rope, positions), BF16),
            pltpu.VMEM((groups, local, 256), F32),
            pltpu.VMEM((groups, local, latent_width), F32),
            pltpu.VMEM((groups, local, rope), F32),
            pltpu.VMEM((local * groups, positions + 128), F32),
            pltpu.VMEM((local * groups, positions), BF16),
            pltpu.VMEM((local, groups, latent_width), F32),
            pltpu.SemaphoreType.DMA((2 * local + 3,)),
        ],
        compiler_params=params(24),
        name="attend",
    )(
        got,
        *collected,
        *keep_in_hbm(
            lengths[None],
            frequencies,
            latent_gain[None],
            cache_latent,
            cache_rope.transpose(0, 2, 1),
        ),
    )
    got = exchange(sent, KV)

    sent = pl.pallas_call(
        functools.partial(
            combine_kernel,
            kv_size=kv_size,
            groups=groups,
            local=local,
            first=2 * latent_width,
        ),
        out_shape=jax.ShapeDtypeStruct((everyone, local, w_out.shape[1]), BF16),
        in_specs=[in_vmem()] * 5,
        out_specs=in_vmem(),
        compiler_params=params(8),
        name="combine",
    )(got, *collected)
    got = exchange(sent, SPREAD)
    return pl.pallas_call(
        functools.partial(finish_kernel, kv_size=kv_size, groups=groups, local=local),
        out_shape=jax.ShapeDtypeStruct((seqs, w_out.shape[1]), BF16),
        in_specs=[in_vmem(), in_vmem()],
        out_specs=in_vmem(),
        compiler_params=params(8),
        name="finish",
    )(got, out_gain[None])


def solution(mesh):
    finer = Mesh(mesh.devices.reshape(4, 4, mesh.shape["tp"] // 2, 2), ALL)

    return jax.shard_map(
        on_device,
        mesh=finer,
        in_specs=(
            P(None, KV),
            P(KV),
            P(KV, TP),
            P(KV, None),
            P(KV, None),
            P(),
            P(TP, None, None),
            P(TP, None, None),
            P(TP, KV),
            P(KV),
            P(TP, KV, None),
            P(TP, KV, None),
            P(),
        ),
        out_specs=P(None, KV),
        check_vma=False,
    )
```

```python
import functools

import jax
import jax.numpy as jnp
import numpy as np
from jax import lax
from jax.experimental import pallas as pl
from jax.experimental.pallas import tpu as pltpu
from jax.sharding import Mesh
from jax.sharding import PartitionSpec as P


KV = ("kv_0", "kv_1")
TP = ("y", "core")
ALL = KV + TP
SPREAD = ("core",) + KV + ("y",)
EPSILON = 1e-06
NEGATIVE = -1e30
F32 = jnp.float32
BF16 = jnp.bfloat16

NT = (((1,), (1,)), ((), ()))
NN = (((1,), (0,)), ((), ()))


def dot(a, b, dims):
    return lax.dot_general(a, b, dims, preferred_element_type=F32)


def params(mib):
    return pltpu.CompilerParams(vmem_limit_bytes=mib * 1024 * 1024)


def in_vmem():
    return pl.BlockSpec(memory_space=pltpu.VMEM)


def in_hbm():
    return pl.BlockSpec(memory_space=pltpu.HBM)


def keep_in_hbm(*arrays):
    return [pltpu.with_memory_space_constraint(x, pltpu.HBM) for x in arrays]


def lanes(shape):
    return lax.broadcasted_iota(jnp.int32, shape, 1)


def rows(shape):
    return lax.broadcasted_iota(jnp.int32, shape, 0)


def block_of(kv, tp, kv_size):
    cores = lax.axis_size("core")
    return (tp % cores * kv_size + kv) * lax.axis_size("y") + tp // cores


def project_kernel(
    tokens, gain, wq, wd, wr, wk, wv, wo, out, own, tokens_, gain_, wq_, wd_, wr_, sems
):
    tp = lax.axis_index(TP)
    groups = lax.axis_size(TP)
    kv_size = lax.axis_size(KV)
    deep = wk.shape[1]
    pairs = (
        (tokens, tokens_),
        (gain, gain_),
        (wq, wq_),
        (wd, wd_),
        (wr, wr_),
        (wk.at[0], own.at[pl.ds(0, deep)]),
        (wv.at[0], own.at[pl.ds(deep, deep)]),
        (wo, own.at[pl.ds(2 * deep, wo.shape[0])]),
    )
    copies = [pltpu.make_async_copy(x, y, sems.at[n]) for n, (x, y) in enumerate(pairs)]
    for copy in copies:
        copy.start()
    for copy in copies[:5]:
        copy.wait()
    scaled = (tokens_[...].astype(F32) * gain_[...]).astype(BF16)
    query = dot(scaled, wq_[...], NT)
    latent = dot(scaled, wd_[...], NN)
    rope = dot(scaled, wr_[...], NT)
    seqs = scaled.shape[0]
    local = seqs // groups
    chunk = latent.shape[1] // groups
    part = latent[:, :chunk]
    for g in range(1, groups):
        part = jnp.where(tp == g, latent[:, g * chunk : (g + 1) * chunk], part)
    width = rope.shape[1]
    rope = jnp.where(lanes(rope.shape) // (width // groups) == tp, rope, 0.0)
    blank = jnp.zeros((seqs, 128 - width), F32)
    part = jnp.concatenate([blank, part], axis=1)
    rope = jnp.concatenate([blank, rope], axis=1)
    first = query[:, :128].astype(BF16)
    second = jnp.concatenate([query[:, 128:], blank], axis=1)
    row = rows((local, 128))
    for t in range(groups):
        top = first[t * local : (t + 1) * local]
        low = second[t * local : (t + 1) * local]
        for j in range(local):
            r = t * local + j
            new = jnp.where(row == 0, part[r : r + 1], 0.0) + jnp.where(row == 1, rope[r : r + 1], 0.0)
            tile = (low + new).astype(BF16)
            for c in range(kv_size // local):
                b = block_of(c * local + j, t, kv_size)
                out[b, :, :128] = top
                out[b, :, 128:] = tile
    for copy in copies[5:]:
        copy.wait()


def bring_kernel(latents, lengths_, frequencies_, gain_, early, lengths, frequencies, gain, sems):
    pairs = (
        (latents.at[pl.ds(0, 1)], early),
        (lengths_, lengths),
        (frequencies_, frequencies),
        (gain_, gain),
    )
    copies = [pltpu.make_async_copy(x, y, sems.at[n]) for n, (x, y) in enumerate(pairs)]
    for copy in copies:
        copy.start()
    for copy in copies:
        copy.wait()


def rotate(values, cosine, sine):
    half = values.shape[1] // 2
    swapped = jnp.concatenate([values[:, half:], values[:, :half]], axis=1)
    return values * cosine + swapped * sine


def attend_kernel(
    got, near, opposite, far, far_opposite, early, lengths, frequencies, gain, latents, ropes,
    out, cache, cache_rope,
    sums, lifted, turned, scored, weights, means, sems,
    *, factor, nope,
):
    kv = lax.axis_index(KV)
    tp = lax.axis_index(TP)
    kv_size = lax.axis_size(KV)
    groups = lax.axis_size(TP)
    local, _, positions = cache_rope.shape
    latent_width = cache.shape[2]
    width = cache_rope.shape[1]
    copies = []
    for s in range(local):
        b = pltpu.make_async_copy(ropes.at[s], cache_rope.at[s], sems.at[local + s])
        b.start()
        copies.append([b])
        if s > 0:
            a = pltpu.make_async_copy(latents.at[s], cache.at[s - 1], sems.at[s])
            a.start()
            copies[s].append(a)

    def cached(s):
        return cache[s - 1] if s > 0 else early[0]

    for h in range(groups):
        total = got[block_of(0, h, kv_size)].astype(F32)
        for k in range(1, kv_size):
            total = total + got[block_of(k, h, kv_size)].astype(F32)
        sums[h] = total
    shape = (local, lengths.shape[1])
    length = jnp.sum(
        jnp.where(lanes(shape) == rows(shape) + tp * local, lengths[...], 0), axis=1, keepdims=True
    )
    lane = lanes((local, width))
    angles = length.astype(F32) * frequencies[...]
    cosine = jnp.cos(angles)
    sine = jnp.sin(angles)
    sine = jnp.where(lane < width // 2, -sine, sine)
    half = groups // 2
    y = tp // 2
    core = lax.rem(tp, 2)
    for i in range(groups):
        step = (0, half - 1, 1, 2)[i % half]
        head = 2 * lax.rem(y + step, half) + (core if i < half else 1 - core)
        q = sums[head]
        w = weights_of((near, opposite, far, far_opposite), i)
        lifted[i] = dot(q[:, :nope].astype(BF16), w[:latent_width, :], NT)
        turned[i] = rotate(q[:, nope : nope + width].astype(BF16).astype(F32), cosine, sine)
    raw = jnp.concatenate([sums[h][0:1, nope + width :] for h in range(groups)], axis=1)
    rope_raw = sums[0][1:2, nope + width :]
    for h in range(1, groups):
        rope_raw = rope_raw + sums[h][1:2, nope + width :]
    square = jnp.sum(raw * raw, axis=1, keepdims=True) / latent_width
    new_latent = (raw * lax.rsqrt(square + EPSILON) * gain[...]).astype(BF16).astype(F32)
    new_seq = lax.rem(kv, local)
    mine = rows((local, width)) == new_seq
    new_rope = rotate(
        rope_raw,
        jnp.sum(jnp.where(mine, cosine, 0.0), axis=0, keepdims=True),
        jnp.sum(jnp.where(mine, sine, 0.0), axis=0, keepdims=True),
    )
    new_rope = new_rope.astype(BF16).astype(F32)
    pairs = local * groups
    for s in range(local):
        q = lifted[:, s, :].astype(BF16)
        qr = turned[:, s, :].astype(BF16)
        fresh = jnp.sum(q.astype(F32) * new_latent, axis=1, keepdims=True) + jnp.sum(
            qr.astype(F32) * new_rope, axis=1, keepdims=True
        )
        for copy in copies[s]:
            copy.wait()
        r = s * groups
        scored[r : r + groups, :positions] = dot(q, cached(s), NT) + dot(qr, cache_rope[s], NN)
        scored[r : r + groups, positions:] = jnp.broadcast_to(fresh, (groups, 128))
    scores = scored[:, :positions] * factor
    row = rows((pairs, 1))
    sequence = row // groups
    limit = jnp.zeros((pairs, 1), jnp.int32)
    for s in range(local):
        limit = jnp.where(sequence == s, length[s : s + 1, :], limit)
    is_new = jnp.logical_and(sequence == new_seq, kv < local)
    new = jnp.where(is_new, scored[:, positions : positions + 1] * factor, NEGATIVE)
    visible = kv * positions + lanes((pairs, positions)) < limit
    top = jnp.max(jnp.where(visible, scores, NEGATIVE), axis=1, keepdims=True)
    top = jnp.maximum(top, new)
    weight = jnp.where(visible, jnp.exp(scores - top), 0.0)
    new_weight = jnp.where(is_new, jnp.exp(new - top), 0.0)
    total = jnp.sum(weight, axis=1, keepdims=True) + new_weight
    weights[...] = weight.astype(BF16)
    some = total > 0.0
    safe = jnp.where(some, total, 1.0)
    inverse = 1.0 / safe
    logs = jnp.where(some, top + jnp.log(safe), NEGATIVE)
    rounded = new_weight.astype(BF16).astype(F32)
    for s in range(local):
        r = slice(s * groups, (s + 1) * groups)
        mixed = dot(weights[r, :], cached(s), NN) + rounded[r] * new_latent
        means[s] = mixed * inverse[r]
    for i in range(groups):
        w = weights_of((near, opposite, far, far_opposite), i)
        x = means[:, i, :].astype(BF16)
        up = dot(x, w[latent_width : 2 * latent_width, :], NN).astype(BF16)
        for k in range(kv_size):
            out[k, i * local : (i + 1) * local, :] = up
    lane = lanes((local, 128))
    table = jnp.zeros((groups, 128), F32)
    for s in range(local):
        table = jnp.where(lanes((groups, 128)) == s, logs[s * groups : (s + 1) * groups], table)
    table = jnp.concatenate([table, jnp.zeros((128 - groups, 128), F32)], axis=0)
    table = jnp.transpose(table)[:local]
    high = table.astype(BF16).astype(F32)
    rest = table - high
    middle = rest.astype(BF16).astype(F32)
    low = (rest - middle).astype(BF16).astype(F32)
    packed = jnp.where(
        lane < groups,
        high,
        jnp.where(
            lane < 2 * groups,
            pltpu.roll(middle, groups, 1),
            jnp.where(lane < 3 * groups, pltpu.roll(low, 2 * groups, 1), 0.0),
        ),
    ).astype(BF16)
    for k in range(kv_size):
        out[k, groups * local :, :] = packed


def weights_of(collected, i):
    near, opposite, far, far_opposite = collected
    places = near.shape[0] + 1
    stacked, single = (near, opposite) if i < places else (far, far_opposite)
    return single if i % places == places - 1 else stacked.at[i % places]


def combine_kernel(got, near, opposite, far, far_opposite, out, *, kv_size, groups, local, first):
    logs = []
    for k in range(kv_size):
        x = got[k, groups * local :, :].astype(F32)
        logs.append(x + pltpu.roll(x, 128 - groups, 1) + pltpu.roll(x, 128 - 2 * groups, 1))
    top = functools.reduce(jnp.maximum, logs)
    shares = [jnp.exp(x - top) for x in logs]
    total = functools.reduce(jnp.add, shares)
    inverse = 1.0 / total
    shares = [x * inverse for x in shares]
    mixed = jnp.zeros((local, out.shape[2]), F32)
    for i in range(groups):
        head = jnp.zeros((local, 128), F32)
        for k in range(kv_size):
            part = got[k, i * local : (i + 1) * local, :].astype(F32)
            head = head + part * shares[k][:, i : i + 1]
        w = weights_of((near, opposite, far, far_opposite), i)
        mixed = mixed + dot(head.astype(BF16), w[first:, :], NN)
    mixed = mixed.astype(BF16)
    for d in range(out.shape[0]):
        out[d] = mixed


def finish_kernel(got, gain, out, *, kv_size, groups, local):
    kv = lax.axis_index(KV)
    width = got.shape[2]
    for t in range(groups):
        squares = jnp.zeros((local, width), F32)
        for k in range(kv_size):
            x = got[block_of(k, t, kv_size)].astype(F32)
            squares = squares + x * x
        mean = jnp.sum(squares, axis=1, keepdims=True) / (width * kv_size)
        own = got[block_of(kv, t, kv_size)].astype(F32)
        out[t * local : (t + 1) * local, :] = (
            own * lax.rsqrt(mean + EPSILON) * gain[...]
        ).astype(BF16)


def exchange(value, axes):
    return lax.all_to_all(value, axes, split_axis=0, concat_axis=0, tiled=True)


def swap(value):
    return lax.ppermute(value, TP, [(i, i ^ 1) for i in range(lax.axis_size(TP))])


def along(own):
    size = lax.axis_size(TP)
    collected = []
    for step in (1, 3, 2):
        pairs = [(i, (i + 2 * step) % size) for i in range(size)]
        collected.append(lax.ppermute(own, TP, pairs))
    return collected


def on_device(
    tokens,
    token_gain,
    w_query,
    w_down_kv,
    w_rope_key,
    latent_gain,
    w_key_up,
    w_value_up,
    w_out,
    out_gain,
    cache_latent,
    cache_rope,
    lengths,
):
    kv_size = lax.axis_size(KV)
    groups = lax.axis_size(TP)
    everyone = kv_size * groups
    seqs, width = tokens.shape
    local, positions, latent_width = cache_latent.shape
    rope = cache_rope.shape[2]
    nope = w_key_up.shape[2]
    value = w_value_up.shape[2]
    factor = (nope + rope) ** (-0.5)

    sent, own = pl.pallas_call(
        project_kernel,
        out_shape=(
            jax.ShapeDtypeStruct((everyone, local, 256), BF16),
            jax.ShapeDtypeStruct((2 * latent_width + value, nope), BF16),
        ),
        in_specs=[in_hbm()] * 8,
        out_specs=(in_vmem(),) * 2,
        scratch_shapes=[
            pltpu.VMEM((seqs, width), BF16),
            pltpu.VMEM((1, width), F32),
            pltpu.VMEM((nope + rope, width), BF16),
            pltpu.VMEM((width, latent_width), BF16),
            pltpu.VMEM((rope, width), BF16),
            pltpu.SemaphoreType.DMA((8,)),
        ],
        compiler_params=params(8),
        name="project",
    )(
        *keep_in_hbm(
            tokens,
            token_gain[None],
            w_query.T,
            w_down_kv,
            w_rope_key.T,
            w_key_up,
            w_value_up,
            w_out,
        )
    )

    before, after, opposite = along(own)
    near = jnp.stack([own, before, after])
    far = swap(near)
    far_opposite = swap(opposite)
    collected = (near, opposite, far, far_opposite)

    got = exchange(sent, SPREAD)
    powers = np.arange(0, rope, 2, dtype=np.float64) / rope
    frequencies = np.tile(1.0 / 10000.0**powers, 2)[None].astype(np.float32)
    brought = pl.pallas_call(
        bring_kernel,
        out_shape=(
            jax.ShapeDtypeStruct((1, positions, latent_width), BF16),
            jax.ShapeDtypeStruct((1, seqs), jnp.int32),
            jax.ShapeDtypeStruct((1, rope), F32),
            jax.ShapeDtypeStruct((1, latent_width), F32),
        ),
        in_specs=[in_hbm()] * 4,
        out_specs=(in_vmem(),) * 4,
        scratch_shapes=[pltpu.SemaphoreType.DMA((4,))],
        compiler_params=params(8),
        name="bring",
    )(*keep_in_hbm(cache_latent, lengths[None], frequencies, latent_gain[None]))
    sent = pl.pallas_call(
        functools.partial(attend_kernel, factor=factor, nope=nope),
        out_shape=jax.ShapeDtypeStruct((kv_size, groups * local + local, value), BF16),
        in_specs=[in_vmem()] * 9 + [in_hbm()] * 2,
        out_specs=in_vmem(),
        scratch_shapes=[
            pltpu.VMEM((local - 1, positions, latent_width), BF16),
            pltpu.VMEM((local, rope, positions), BF16),
            pltpu.VMEM((groups, local, 256), F32),
            pltpu.VMEM((groups, local, latent_width), F32),
            pltpu.VMEM((groups, local, rope), F32),
            pltpu.VMEM((local * groups, positions + 128), F32),
            pltpu.VMEM((local * groups, positions), BF16),
            pltpu.VMEM((local, groups, latent_width), F32),
            pltpu.SemaphoreType.DMA((2 * local,)),
        ],
        compiler_params=params(24),
        name="attend",
    )(
        got,
        *collected,
        *brought,
        *keep_in_hbm(cache_latent, cache_rope.transpose(0, 2, 1)),
    )
    got = exchange(sent, KV)

    sent = pl.pallas_call(
        functools.partial(
            combine_kernel,
            kv_size=kv_size,
            groups=groups,
            local=local,
            first=2 * latent_width,
        ),
        out_shape=jax.ShapeDtypeStruct((everyone, local, w_out.shape[1]), BF16),
        in_specs=[in_vmem()] * 5,
        out_specs=in_vmem(),
        compiler_params=params(8),
        name="combine",
    )(got, *collected)
    got = exchange(sent, SPREAD)
    return pl.pallas_call(
        functools.partial(finish_kernel, kv_size=kv_size, groups=groups, local=local),
        out_shape=jax.ShapeDtypeStruct((seqs, w_out.shape[1]), BF16),
        in_specs=[in_vmem(), in_vmem()],
        out_specs=in_vmem(),
        compiler_params=params(8),
        name="finish",
    )(got, out_gain[None])


def solution(mesh):
    finer = Mesh(mesh.devices.reshape(4, 4, mesh.shape["tp"] // 2, 2), ALL)

    return jax.shard_map(
        on_device,
        mesh=finer,
        in_specs=(
            P(None, KV),
            P(KV),
            P(KV, TP),
            P(KV, None),
            P(KV, None),
            P(),
            P(TP, None, None),
            P(TP, None, None),
            P(TP, KV),
            P(KV),
            P(TP, KV, None),
            P(TP, KV, None),
            P(),
        ),
        out_specs=P(None, KV),
        check_vma=False,
    )
```

```python
import functools

import jax
import jax.numpy as jnp
import numpy as np
from jax import lax
from jax.experimental import pallas as pl
from jax.experimental.pallas import tpu as pltpu
from jax.sharding import Mesh
from jax.sharding import PartitionSpec as P


KV = ("kv_0", "kv_1")
TP = ("y", "core")
ALL = KV + TP
SPREAD = ("core",) + KV + ("y",)
EPSILON = 1e-06
NEGATIVE = -1e30
F32 = jnp.float32
BF16 = jnp.bfloat16

NT = (((1,), (1,)), ((), ()))
NN = (((1,), (0,)), ((), ()))


def dot(a, b, dims):
    return lax.dot_general(a, b, dims, preferred_element_type=F32)


def params(mib):
    return pltpu.CompilerParams(vmem_limit_bytes=mib * 1024 * 1024)


def in_vmem():
    return pl.BlockSpec(memory_space=pltpu.VMEM)


def in_hbm():
    return pl.BlockSpec(memory_space=pltpu.HBM)


def keep_in_hbm(*arrays):
    return [pltpu.with_memory_space_constraint(x, pltpu.HBM) for x in arrays]


def lanes(shape):
    return lax.broadcasted_iota(jnp.int32, shape, 1)


def rows(shape):
    return lax.broadcasted_iota(jnp.int32, shape, 0)


def block_of(kv, tp, kv_size):
    cores = lax.axis_size("core")
    return (tp % cores * kv_size + kv) * lax.axis_size("y") + tp // cores


def project_kernel(
    tokens, gain, wq, wd, wr, wk, wv, wo, out, own, tokens_, gain_, wq_, wd_, wr_, sems
):
    tp = lax.axis_index(TP)
    groups = lax.axis_size(TP)
    kv_size = lax.axis_size(KV)
    deep = wk.shape[1]
    pairs = (
        (tokens, tokens_),
        (gain, gain_),
        (wq, wq_),
        (wd, wd_),
        (wr, wr_),
        (wk.at[0], own.at[pl.ds(0, deep)]),
        (wv.at[0], own.at[pl.ds(deep, deep)]),
        (wo, own.at[pl.ds(2 * deep, wo.shape[0])]),
    )
    copies = [pltpu.make_async_copy(x, y, sems.at[n]) for n, (x, y) in enumerate(pairs)]
    for copy in copies:
        copy.start()
    for copy in copies[:5]:
        copy.wait()
    scaled = (tokens_[...].astype(F32) * gain_[...]).astype(BF16)
    query = dot(scaled, wq_[...], NT)
    latent = dot(scaled, wd_[...], NN)
    rope = dot(scaled, wr_[...], NT)
    seqs = scaled.shape[0]
    local = seqs // groups
    chunk = latent.shape[1] // groups
    part = latent[:, :chunk]
    for g in range(1, groups):
        part = jnp.where(tp == g, latent[:, g * chunk : (g + 1) * chunk], part)
    width = rope.shape[1]
    rope = jnp.where(lanes(rope.shape) // (width // groups) == tp, rope, 0.0)
    blank = jnp.zeros((seqs, 128 - width), F32)
    part = jnp.concatenate([blank, part], axis=1)
    rope = jnp.concatenate([blank, rope], axis=1)
    first = query[:, :128].astype(BF16)
    second = jnp.concatenate([query[:, 128:], blank], axis=1)
    row = rows((local, 128))
    for t in range(groups):
        top = first[t * local : (t + 1) * local]
        low = second[t * local : (t + 1) * local]
        for j in range(local):
            r = t * local + j
            new = jnp.where(row == 0, part[r : r + 1], 0.0) + jnp.where(row == 1, rope[r : r + 1], 0.0)
            tile = (low + new).astype(BF16)
            for c in range(kv_size // local):
                b = block_of(c * local + j, t, kv_size)
                out[b, :, :128] = top
                out[b, :, 128:] = tile
    for copy in copies[5:]:
        copy.wait()


def bring_kernel(latents, lengths_, frequencies_, gain_, early, lengths, frequencies, gain, sems):
    pairs = (
        (latents.at[pl.ds(0, 1)], early),
        (lengths_, lengths),
        (frequencies_, frequencies),
        (gain_, gain),
    )
    copies = [pltpu.make_async_copy(x, y, sems.at[n]) for n, (x, y) in enumerate(pairs)]
    for copy in copies:
        copy.start()
    for copy in copies:
        copy.wait()


def rotate(values, cosine, sine):
    half = values.shape[1] // 2
    swapped = jnp.concatenate([values[:, half:], values[:, :half]], axis=1)
    return values * cosine + swapped * sine


def attend_kernel(
    got, near, last, far, far_last, early, lengths, frequencies, gain, latents, ropes,
    out, cache, cache_rope,
    sums, lifted, turned, scored, weights, means, sems,
    *, factor, nope,
):
    kv = lax.axis_index(KV)
    tp = lax.axis_index(TP)
    kv_size = lax.axis_size(KV)
    groups = lax.axis_size(TP)
    local, _, positions = cache_rope.shape
    latent_width = cache.shape[2]
    width = cache_rope.shape[1]
    copies = []
    for s in range(local):
        b = pltpu.make_async_copy(ropes.at[s], cache_rope.at[s], sems.at[local + s])
        b.start()
        copies.append([b])
        if s > 0:
            a = pltpu.make_async_copy(latents.at[s], cache.at[s - 1], sems.at[s])
            a.start()
            copies[s].append(a)

    def cached(s):
        return cache[s - 1] if s > 0 else early[0]

    for h in range(groups):
        total = got[block_of(0, h, kv_size)].astype(F32)
        for k in range(1, kv_size):
            total = total + got[block_of(k, h, kv_size)].astype(F32)
        sums[h] = total
    shape = (local, lengths.shape[1])
    length = jnp.sum(
        jnp.where(lanes(shape) == rows(shape) + tp * local, lengths[...], 0), axis=1, keepdims=True
    )
    lane = lanes((local, width))
    angles = length.astype(F32) * frequencies[...]
    cosine = jnp.cos(angles)
    sine = jnp.sin(angles)
    sine = jnp.where(lane < width // 2, -sine, sine)
    half = groups // 2
    y = tp // 2
    core = lax.rem(tp, 2)
    for i in range(groups):
        step = (0, 2, half - 1, 1)[i % half]
        head = 2 * lax.rem(y + step, half) + (core if i < half else 1 - core)
        q = sums[head]
        w = weights_of((near, last, far, far_last), i)
        lifted[i] = dot(q[:, :nope].astype(BF16), w[:latent_width, :], NT)
        turned[i] = rotate(q[:, nope : nope + width].astype(BF16).astype(F32), cosine, sine)
    raw = jnp.concatenate([sums[h][0:1, nope + width :] for h in range(groups)], axis=1)
    rope_raw = sums[0][1:2, nope + width :]
    for h in range(1, groups):
        rope_raw = rope_raw + sums[h][1:2, nope + width :]
    square = jnp.sum(raw * raw, axis=1, keepdims=True) / latent_width
    new_latent = (raw * lax.rsqrt(square + EPSILON) * gain[...]).astype(BF16).astype(F32)
    new_seq = lax.rem(kv, local)
    mine = rows((local, width)) == new_seq
    new_rope = rotate(
        rope_raw,
        jnp.sum(jnp.where(mine, cosine, 0.0), axis=0, keepdims=True),
        jnp.sum(jnp.where(mine, sine, 0.0), axis=0, keepdims=True),
    )
    new_rope = new_rope.astype(BF16).astype(F32)
    pairs = local * groups
    for s in range(local):
        q = lifted[:, s, :].astype(BF16)
        qr = turned[:, s, :].astype(BF16)
        fresh = jnp.sum(q.astype(F32) * new_latent, axis=1, keepdims=True) + jnp.sum(
            qr.astype(F32) * new_rope, axis=1, keepdims=True
        )
        for copy in copies[s]:
            copy.wait()
        r = s * groups
        scored[r : r + groups, :positions] = dot(q, cached(s), NT) + dot(qr, cache_rope[s], NN)
        scored[r : r + groups, positions:] = jnp.broadcast_to(fresh, (groups, 128))
    scores = scored[:, :positions] * factor
    row = rows((pairs, 1))
    sequence = row // groups
    limit = jnp.zeros((pairs, 1), jnp.int32)
    for s in range(local):
        limit = jnp.where(sequence == s, length[s : s + 1, :], limit)
    is_new = jnp.logical_and(sequence == new_seq, kv < local)
    new = jnp.where(is_new, scored[:, positions : positions + 1] * factor, NEGATIVE)
    visible = kv * positions + lanes((pairs, positions)) < limit
    top = jnp.max(jnp.where(visible, scores, NEGATIVE), axis=1, keepdims=True)
    top = jnp.maximum(top, new)
    weight = jnp.where(visible, jnp.exp(scores - top), 0.0)
    new_weight = jnp.where(is_new, jnp.exp(new - top), 0.0)
    total = jnp.sum(weight, axis=1, keepdims=True) + new_weight
    weights[...] = weight.astype(BF16)
    some = total > 0.0
    safe = jnp.where(some, total, 1.0)
    inverse = 1.0 / safe
    logs = jnp.where(some, top + jnp.log(safe), NEGATIVE)
    rounded = new_weight.astype(BF16).astype(F32)
    for s in range(local):
        r = slice(s * groups, (s + 1) * groups)
        mixed = dot(weights[r, :], cached(s), NN) + rounded[r] * new_latent
        means[s] = mixed * inverse[r]
    for i in range(groups):
        w = weights_of((near, last, far, far_last), i)
        x = means[:, i, :].astype(BF16)
        up = dot(x, w[latent_width : 2 * latent_width, :], NN).astype(BF16)
        for k in range(kv_size):
            out[k, i * local : (i + 1) * local, :] = up
    lane = lanes((local, 128))
    table = jnp.zeros((groups, 128), F32)
    for s in range(local):
        table = jnp.where(lanes((groups, 128)) == s, logs[s * groups : (s + 1) * groups], table)
    table = jnp.concatenate([table, jnp.zeros((128 - groups, 128), F32)], axis=0)
    table = jnp.transpose(table)[:local]
    high = table.astype(BF16).astype(F32)
    rest = table - high
    middle = rest.astype(BF16).astype(F32)
    low = (rest - middle).astype(BF16).astype(F32)
    packed = jnp.where(
        lane < groups,
        high,
        jnp.where(
            lane < 2 * groups,
            pltpu.roll(middle, groups, 1),
            jnp.where(lane < 3 * groups, pltpu.roll(low, 2 * groups, 1), 0.0),
        ),
    ).astype(BF16)
    for k in range(kv_size):
        out[k, groups * local :, :] = packed


def weights_of(collected, i):
    near, last, far, far_last = collected
    places = near.shape[0] + 1
    stacked, single = (near, last) if i < places else (far, far_last)
    return single if i % places == places - 1 else stacked.at[i % places]


def combine_kernel(got, near, last, far, far_last, out, *, kv_size, groups, local, first):
    logs = []
    for k in range(kv_size):
        x = got[k, groups * local :, :].astype(F32)
        logs.append(x + pltpu.roll(x, 128 - groups, 1) + pltpu.roll(x, 128 - 2 * groups, 1))
    top = functools.reduce(jnp.maximum, logs)
    shares = [jnp.exp(x - top) for x in logs]
    total = functools.reduce(jnp.add, shares)
    inverse = 1.0 / total
    shares = [x * inverse for x in shares]
    mixed = jnp.zeros((local, out.shape[2]), F32)
    for i in range(groups):
        head = jnp.zeros((local, 128), F32)
        for k in range(kv_size):
            part = got[k, i * local : (i + 1) * local, :].astype(F32)
            head = head + part * shares[k][:, i : i + 1]
        w = weights_of((near, last, far, far_last), i)
        mixed = mixed + dot(head.astype(BF16), w[first:, :], NN)
    mixed = mixed.astype(BF16)
    for d in range(out.shape[0]):
        out[d] = mixed


def finish_kernel(got, gain, out, *, kv_size, groups, local):
    kv = lax.axis_index(KV)
    width = got.shape[2]
    for t in range(groups):
        squares = jnp.zeros((local, width), F32)
        for k in range(kv_size):
            x = got[block_of(k, t, kv_size)].astype(F32)
            squares = squares + x * x
        mean = jnp.sum(squares, axis=1, keepdims=True) / (width * kv_size)
        own = got[block_of(kv, t, kv_size)].astype(F32)
        out[t * local : (t + 1) * local, :] = (
            own * lax.rsqrt(mean + EPSILON) * gain[...]
        ).astype(BF16)


def exchange(value, axes):
    return lax.all_to_all(value, axes, split_axis=0, concat_axis=0, tiled=True)


def swap(value):
    return lax.ppermute(value, TP, [(i, i ^ 1) for i in range(lax.axis_size(TP))])


def along(own):
    size = lax.axis_size(TP)
    collected = []
    for step in (1, 3, 2):
        pairs = [(i, (i + 2 * step) % size) for i in range(size)]
        collected.append(lax.ppermute(own, TP, pairs))
    return collected


def on_device(
    tokens,
    token_gain,
    w_query,
    w_down_kv,
    w_rope_key,
    latent_gain,
    w_key_up,
    w_value_up,
    w_out,
    out_gain,
    cache_latent,
    cache_rope,
    lengths,
):
    kv_size = lax.axis_size(KV)
    groups = lax.axis_size(TP)
    everyone = kv_size * groups
    seqs, width = tokens.shape
    local, positions, latent_width = cache_latent.shape
    rope = cache_rope.shape[2]
    nope = w_key_up.shape[2]
    value = w_value_up.shape[2]
    factor = (nope + rope) ** (-0.5)

    sent, own = pl.pallas_call(
        project_kernel,
        out_shape=(
            jax.ShapeDtypeStruct((everyone, local, 256), BF16),
            jax.ShapeDtypeStruct((2 * latent_width + value, nope), BF16),
        ),
        in_specs=[in_hbm()] * 8,
        out_specs=(in_vmem(),) * 2,
        scratch_shapes=[
            pltpu.VMEM((seqs, width), BF16),
            pltpu.VMEM((1, width), F32),
            pltpu.VMEM((nope + rope, width), BF16),
            pltpu.VMEM((width, latent_width), BF16),
            pltpu.VMEM((rope, width), BF16),
            pltpu.SemaphoreType.DMA((8,)),
        ],
        compiler_params=params(8),
        name="project",
    )(
        *keep_in_hbm(
            tokens,
            token_gain[None],
            w_query.T,
            w_down_kv,
            w_rope_key.T,
            w_key_up,
            w_value_up,
            w_out,
        )
    )

    before, after, opposite = along(own)
    near = jnp.stack([own, opposite, before])
    far = swap(near)
    far_last = swap(after)
    collected = (near, after, far, far_last)

    got = exchange(sent, SPREAD)
    powers = np.arange(0, rope, 2, dtype=np.float64) / rope
    frequencies = np.tile(1.0 / 10000.0**powers, 2)[None].astype(np.float32)
    brought = pl.pallas_call(
        bring_kernel,
        out_shape=(
            jax.ShapeDtypeStruct((1, positions, latent_width), BF16),
            jax.ShapeDtypeStruct((1, seqs), jnp.int32),
            jax.ShapeDtypeStruct((1, rope), F32),
            jax.ShapeDtypeStruct((1, latent_width), F32),
        ),
        in_specs=[in_hbm()] * 4,
        out_specs=(in_vmem(),) * 4,
        scratch_shapes=[pltpu.SemaphoreType.DMA((4,))],
        compiler_params=params(8),
        name="bring",
    )(*keep_in_hbm(cache_latent, lengths[None], frequencies, latent_gain[None]))
    sent = pl.pallas_call(
        functools.partial(attend_kernel, factor=factor, nope=nope),
        out_shape=jax.ShapeDtypeStruct((kv_size, groups * local + local, value), BF16),
        in_specs=[in_vmem()] * 9 + [in_hbm()] * 2,
        out_specs=in_vmem(),
        scratch_shapes=[
            pltpu.VMEM((local - 1, positions, latent_width), BF16),
            pltpu.VMEM((local, rope, positions), BF16),
            pltpu.VMEM((groups, local, 256), F32),
            pltpu.VMEM((groups, local, latent_width), F32),
            pltpu.VMEM((groups, local, rope), F32),
            pltpu.VMEM((local * groups, positions + 128), F32),
            pltpu.VMEM((local * groups, positions), BF16),
            pltpu.VMEM((local, groups, latent_width), F32),
            pltpu.SemaphoreType.DMA((2 * local,)),
        ],
        compiler_params=params(24),
        name="attend",
    )(
        got,
        *collected,
        *brought,
        *keep_in_hbm(cache_latent, cache_rope.transpose(0, 2, 1)),
    )
    got = exchange(sent, KV)

    sent = pl.pallas_call(
        functools.partial(
            combine_kernel,
            kv_size=kv_size,
            groups=groups,
            local=local,
            first=2 * latent_width,
        ),
        out_shape=jax.ShapeDtypeStruct((everyone, local, w_out.shape[1]), BF16),
        in_specs=[in_vmem()] * 5,
        out_specs=in_vmem(),
        compiler_params=params(8),
        name="combine",
    )(got, *collected)
    got = exchange(sent, SPREAD)
    return pl.pallas_call(
        functools.partial(finish_kernel, kv_size=kv_size, groups=groups, local=local),
        out_shape=jax.ShapeDtypeStruct((seqs, w_out.shape[1]), BF16),
        in_specs=[in_vmem(), in_vmem()],
        out_specs=in_vmem(),
        compiler_params=params(8),
        name="finish",
    )(got, out_gain[None])


def solution(mesh):
    finer = Mesh(mesh.devices.reshape(4, 4, mesh.shape["tp"] // 2, 2), ALL)

    return jax.shard_map(
        on_device,
        mesh=finer,
        in_specs=(
            P(None, KV),
            P(KV),
            P(KV, TP),
            P(KV, None),
            P(KV, None),
            P(),
            P(TP, None, None),
            P(TP, None, None),
            P(TP, KV),
            P(KV),
            P(TP, KV, None),
            P(TP, KV, None),
            P(),
        ),
        out_specs=P(None, KV),
        check_vma=False,
    )
```

```python
import functools

import jax
import jax.numpy as jnp
import numpy as np
from jax import lax
from jax.experimental import pallas as pl
from jax.experimental.pallas import tpu as pltpu
from jax.sharding import Mesh
from jax.sharding import PartitionSpec as P


KV = ("kv_0", "kv_1")
TP = ("y", "core")
ALL = KV + TP
SPREAD = ("core",) + KV + ("y",)
EPSILON = 1e-06
NEGATIVE = -1e30
F32 = jnp.float32
BF16 = jnp.bfloat16

NT = (((1,), (1,)), ((), ()))
NN = (((1,), (0,)), ((), ()))


def dot(a, b, dims):
    return lax.dot_general(a, b, dims, preferred_element_type=F32)


def params(mib):
    return pltpu.CompilerParams(vmem_limit_bytes=mib * 1024 * 1024)


def in_vmem():
    return pl.BlockSpec(memory_space=pltpu.VMEM)


def in_hbm():
    return pl.BlockSpec(memory_space=pltpu.HBM)


def keep_in_hbm(*arrays):
    return [pltpu.with_memory_space_constraint(x, pltpu.HBM) for x in arrays]


def lanes(shape):
    return lax.broadcasted_iota(jnp.int32, shape, 1)


def rows(shape):
    return lax.broadcasted_iota(jnp.int32, shape, 0)


def block_of(kv, tp, kv_size):
    cores = lax.axis_size("core")
    return (tp % cores * kv_size + kv) * lax.axis_size("y") + tp // cores


def project_kernel(
    tokens, gain, wq, wd, wr, wk, wv, wo, out, own, tokens_, gain_, wq_, wd_, wr_, sems
):
    tp = lax.axis_index(TP)
    groups = lax.axis_size(TP)
    kv_size = lax.axis_size(KV)
    deep = wk.shape[1]
    pairs = (
        (tokens, tokens_),
        (gain, gain_),
        (wq, wq_),
        (wd, wd_),
        (wr, wr_),
        (wk.at[0], own.at[pl.ds(0, deep)]),
        (wv.at[0], own.at[pl.ds(deep, deep)]),
        (wo, own.at[pl.ds(2 * deep, wo.shape[0])]),
    )
    copies = [pltpu.make_async_copy(x, y, sems.at[n]) for n, (x, y) in enumerate(pairs)]
    for copy in copies:
        copy.start()
    for copy in copies[:5]:
        copy.wait()
    scaled = (tokens_[...].astype(F32) * gain_[...]).astype(BF16)
    query = dot(scaled, wq_[...], NT)
    latent = dot(scaled, wd_[...], NN)
    rope = dot(scaled, wr_[...], NT)
    seqs = scaled.shape[0]
    local = seqs // groups
    chunk = latent.shape[1] // groups
    part = latent[:, :chunk]
    for g in range(1, groups):
        part = jnp.where(tp == g, latent[:, g * chunk : (g + 1) * chunk], part)
    width = rope.shape[1]
    rope = jnp.where(lanes(rope.shape) // (width // groups) == tp, rope, 0.0)
    blank = jnp.zeros((seqs, 128 - width), F32)
    part = jnp.concatenate([blank, part], axis=1)
    rope = jnp.concatenate([blank, rope], axis=1)
    first = query[:, :128].astype(BF16)
    second = jnp.concatenate([query[:, 128:], blank], axis=1)
    row = rows((local, 128))
    for t in range(groups):
        top = first[t * local : (t + 1) * local]
        low = second[t * local : (t + 1) * local]
        for j in range(local):
            r = t * local + j
            new = jnp.where(row == 0, part[r : r + 1], 0.0) + jnp.where(row == 1, rope[r : r + 1], 0.0)
            tile = (low + new).astype(BF16)
            for c in range(kv_size // local):
                b = block_of(c * local + j, t, kv_size)
                out[b, :, :128] = top
                out[b, :, 128:] = tile
    for copy in copies[5:]:
        copy.wait()


def bring_kernel(latents, lengths_, frequencies_, gain_, early, lengths, frequencies, gain, sems):
    pairs = (
        (latents.at[pl.ds(0, 1)], early),
        (lengths_, lengths),
        (frequencies_, frequencies),
        (gain_, gain),
    )
    copies = [pltpu.make_async_copy(x, y, sems.at[n]) for n, (x, y) in enumerate(pairs)]
    for copy in copies:
        copy.start()
    for copy in copies:
        copy.wait()


def rotate(values, cosine, sine):
    half = values.shape[1] // 2
    swapped = jnp.concatenate([values[:, half:], values[:, :half]], axis=1)
    return values * cosine + swapped * sine


def attend_kernel(
    got, near, opposite, far, far_opposite, early, lengths, frequencies, gain, latents, ropes,
    out, cache, cache_rope,
    sums, lifted, turned, scored, weights, means, sems,
    *, factor, nope,
):
    kv = lax.axis_index(KV)
    tp = lax.axis_index(TP)
    kv_size = lax.axis_size(KV)
    groups = lax.axis_size(TP)
    local, _, positions = cache_rope.shape
    latent_width = cache.shape[2]
    width = cache_rope.shape[1]
    copies = []
    for s in range(local):
        b = pltpu.make_async_copy(ropes.at[s], cache_rope.at[s], sems.at[local + s])
        b.start()
        copies.append([b])
        if s > 0:
            a = pltpu.make_async_copy(latents.at[s], cache.at[s - 1], sems.at[s])
            a.start()
            copies[s].append(a)

    def cached(s):
        return cache[s - 1] if s > 0 else early[0]

    for h in range(groups):
        total = got[block_of(0, h, kv_size)].astype(F32)
        for k in range(1, kv_size):
            total = total + got[block_of(k, h, kv_size)].astype(F32)
        sums[h] = total
    shape = (local, lengths.shape[1])
    length = jnp.sum(
        jnp.where(lanes(shape) == rows(shape) + tp * local, lengths[...], 0), axis=1, keepdims=True
    )
    lane = lanes((local, width))
    angles = length.astype(F32) * frequencies[...]
    cosine = jnp.cos(angles)
    sine = jnp.sin(angles)
    sine = jnp.where(lane < width // 2, -sine, sine)
    half = groups // 2
    y = tp // 2
    core = lax.rem(tp, 2)
    for i in range(groups):
        source = core if i < half else 1 - core
        step = (0, -1, 1, 2)[i % half] * (1 - 2 * source)
        head = 2 * lax.rem(y + half + step, half) + source
        q = sums[head]
        w = weights_of((near, opposite, far, far_opposite), i)
        lifted[i] = dot(q[:, :nope].astype(BF16), w[:latent_width, :], NT)
        turned[i] = rotate(q[:, nope : nope + width].astype(BF16).astype(F32), cosine, sine)
    raw = jnp.concatenate([sums[h][0:1, nope + width :] for h in range(groups)], axis=1)
    rope_raw = sums[0][1:2, nope + width :]
    for h in range(1, groups):
        rope_raw = rope_raw + sums[h][1:2, nope + width :]
    square = jnp.sum(raw * raw, axis=1, keepdims=True) / latent_width
    new_latent = (raw * lax.rsqrt(square + EPSILON) * gain[...]).astype(BF16).astype(F32)
    new_seq = lax.rem(kv, local)
    mine = rows((local, width)) == new_seq
    new_rope = rotate(
        rope_raw,
        jnp.sum(jnp.where(mine, cosine, 0.0), axis=0, keepdims=True),
        jnp.sum(jnp.where(mine, sine, 0.0), axis=0, keepdims=True),
    )
    new_rope = new_rope.astype(BF16).astype(F32)
    pairs = local * groups
    for s in range(local):
        q = lifted[:, s, :].astype(BF16)
        qr = turned[:, s, :].astype(BF16)
        fresh = jnp.sum(q.astype(F32) * new_latent, axis=1, keepdims=True) + jnp.sum(
            qr.astype(F32) * new_rope, axis=1, keepdims=True
        )
        for copy in copies[s]:
            copy.wait()
        r = s * groups
        scored[r : r + groups, :positions] = dot(q, cached(s), NT) + dot(qr, cache_rope[s], NN)
        scored[r : r + groups, positions:] = jnp.broadcast_to(fresh, (groups, 128))
    scores = scored[:, :positions] * factor
    row = rows((pairs, 1))
    sequence = row // groups
    limit = jnp.zeros((pairs, 1), jnp.int32)
    for s in range(local):
        limit = jnp.where(sequence == s, length[s : s + 1, :], limit)
    is_new = jnp.logical_and(sequence == new_seq, kv < local)
    new = jnp.where(is_new, scored[:, positions : positions + 1] * factor, NEGATIVE)
    visible = kv * positions + lanes((pairs, positions)) < limit
    top = jnp.max(jnp.where(visible, scores, NEGATIVE), axis=1, keepdims=True)
    top = jnp.maximum(top, new)
    weight = jnp.where(visible, jnp.exp(scores - top), 0.0)
    new_weight = jnp.where(is_new, jnp.exp(new - top), 0.0)
    total = jnp.sum(weight, axis=1, keepdims=True) + new_weight
    weights[...] = weight.astype(BF16)
    some = total > 0.0
    safe = jnp.where(some, total, 1.0)
    inverse = 1.0 / safe
    logs = jnp.where(some, top + jnp.log(safe), NEGATIVE)
    rounded = new_weight.astype(BF16).astype(F32)
    for s in range(local):
        r = slice(s * groups, (s + 1) * groups)
        mixed = dot(weights[r, :], cached(s), NN) + rounded[r] * new_latent
        means[s] = mixed * inverse[r]
    for i in range(groups):
        w = weights_of((near, opposite, far, far_opposite), i)
        x = means[:, i, :].astype(BF16)
        up = dot(x, w[latent_width : 2 * latent_width, :], NN).astype(BF16)
        for k in range(kv_size):
            out[k, i * local : (i + 1) * local, :] = up
    lane = lanes((local, 128))
    table = jnp.zeros((groups, 128), F32)
    for s in range(local):
        table = jnp.where(lanes((groups, 128)) == s, logs[s * groups : (s + 1) * groups], table)
    table = jnp.concatenate([table, jnp.zeros((128 - groups, 128), F32)], axis=0)
    table = jnp.transpose(table)[:local]
    high = table.astype(BF16).astype(F32)
    rest = table - high
    middle = rest.astype(BF16).astype(F32)
    low = (rest - middle).astype(BF16).astype(F32)
    packed = jnp.where(
        lane < groups,
        high,
        jnp.where(
            lane < 2 * groups,
            pltpu.roll(middle, groups, 1),
            jnp.where(lane < 3 * groups, pltpu.roll(low, 2 * groups, 1), 0.0),
        ),
    ).astype(BF16)
    for k in range(kv_size):
        out[k, groups * local :, :] = packed


def weights_of(collected, i):
    near, opposite, far, far_opposite = collected
    places = near.shape[0] + 1
    stacked, single = (near, opposite) if i < places else (far, far_opposite)
    return single if i % places == places - 1 else stacked.at[i % places]


def combine_kernel(got, near, opposite, far, far_opposite, out, *, kv_size, groups, local, first):
    logs = []
    for k in range(kv_size):
        x = got[k, groups * local :, :].astype(F32)
        logs.append(x + pltpu.roll(x, 128 - groups, 1) + pltpu.roll(x, 128 - 2 * groups, 1))
    top = functools.reduce(jnp.maximum, logs)
    shares = [jnp.exp(x - top) for x in logs]
    total = functools.reduce(jnp.add, shares)
    inverse = 1.0 / total
    shares = [x * inverse for x in shares]
    mixed = jnp.zeros((local, out.shape[2]), F32)
    for i in range(groups):
        head = jnp.zeros((local, 128), F32)
        for k in range(kv_size):
            part = got[k, i * local : (i + 1) * local, :].astype(F32)
            head = head + part * shares[k][:, i : i + 1]
        w = weights_of((near, opposite, far, far_opposite), i)
        mixed = mixed + dot(head.astype(BF16), w[first:, :], NN)
    mixed = mixed.astype(BF16)
    for d in range(out.shape[0]):
        out[d] = mixed


def finish_kernel(got, gain, out, *, kv_size, groups, local):
    kv = lax.axis_index(KV)
    width = got.shape[2]
    for t in range(groups):
        squares = jnp.zeros((local, width), F32)
        for k in range(kv_size):
            x = got[block_of(k, t, kv_size)].astype(F32)
            squares = squares + x * x
        mean = jnp.sum(squares, axis=1, keepdims=True) / (width * kv_size)
        own = got[block_of(kv, t, kv_size)].astype(F32)
        out[t * local : (t + 1) * local, :] = (
            own * lax.rsqrt(mean + EPSILON) * gain[...]
        ).astype(BF16)


def exchange(value, axes):
    return lax.all_to_all(value, axes, split_axis=0, concat_axis=0, tiled=True)


def swap(value):
    return lax.ppermute(value, TP, [(i, i ^ 1) for i in range(lax.axis_size(TP))])


def along(own):
    size = lax.axis_size(TP)
    collected = []
    for step in (1, 3, 2):
        pairs = [(i, (i + (2 - 4 * (i % 2)) * step) % size) for i in range(size)]
        collected.append(lax.ppermute(own, TP, pairs))
    return collected


def on_device(
    tokens,
    token_gain,
    w_query,
    w_down_kv,
    w_rope_key,
    latent_gain,
    w_key_up,
    w_value_up,
    w_out,
    out_gain,
    cache_latent,
    cache_rope,
    lengths,
):
    kv_size = lax.axis_size(KV)
    groups = lax.axis_size(TP)
    everyone = kv_size * groups
    seqs, width = tokens.shape
    local, positions, latent_width = cache_latent.shape
    rope = cache_rope.shape[2]
    nope = w_key_up.shape[2]
    value = w_value_up.shape[2]
    factor = (nope + rope) ** (-0.5)

    sent, own = pl.pallas_call(
        project_kernel,
        out_shape=(
            jax.ShapeDtypeStruct((everyone, local, 256), BF16),
            jax.ShapeDtypeStruct((2 * latent_width + value, nope), BF16),
        ),
        in_specs=[in_hbm()] * 8,
        out_specs=(in_vmem(),) * 2,
        scratch_shapes=[
            pltpu.VMEM((seqs, width), BF16),
            pltpu.VMEM((1, width), F32),
            pltpu.VMEM((nope + rope, width), BF16),
            pltpu.VMEM((width, latent_width), BF16),
            pltpu.VMEM((rope, width), BF16),
            pltpu.SemaphoreType.DMA((8,)),
        ],
        compiler_params=params(8),
        name="project",
    )(
        *keep_in_hbm(
            tokens,
            token_gain[None],
            w_query.T,
            w_down_kv,
            w_rope_key.T,
            w_key_up,
            w_value_up,
            w_out,
        )
    )

    before, after, opposite = along(own)
    near = jnp.stack([own, before, after])
    far = swap(near)
    far_opposite = swap(opposite)
    collected = (near, opposite, far, far_opposite)

    got = exchange(sent, SPREAD)
    powers = np.arange(0, rope, 2, dtype=np.float64) / rope
    frequencies = np.tile(1.0 / 10000.0**powers, 2)[None].astype(np.float32)
    brought = pl.pallas_call(
        bring_kernel,
        out_shape=(
            jax.ShapeDtypeStruct((1, positions, latent_width), BF16),
            jax.ShapeDtypeStruct((1, seqs), jnp.int32),
            jax.ShapeDtypeStruct((1, rope), F32),
            jax.ShapeDtypeStruct((1, latent_width), F32),
        ),
        in_specs=[in_hbm()] * 4,
        out_specs=(in_vmem(),) * 4,
        scratch_shapes=[pltpu.SemaphoreType.DMA((4,))],
        compiler_params=params(8),
        name="bring",
    )(*keep_in_hbm(cache_latent, lengths[None], frequencies, latent_gain[None]))
    sent = pl.pallas_call(
        functools.partial(attend_kernel, factor=factor, nope=nope),
        out_shape=jax.ShapeDtypeStruct((kv_size, groups * local + local, value), BF16),
        in_specs=[in_vmem()] * 9 + [in_hbm()] * 2,
        out_specs=in_vmem(),
        scratch_shapes=[
            pltpu.VMEM((local - 1, positions, latent_width), BF16),
            pltpu.VMEM((local, rope, positions), BF16),
            pltpu.VMEM((groups, local, 256), F32),
            pltpu.VMEM((groups, local, latent_width), F32),
            pltpu.VMEM((groups, local, rope), F32),
            pltpu.VMEM((local * groups, positions + 128), F32),
            pltpu.VMEM((local * groups, positions), BF16),
            pltpu.VMEM((local, groups, latent_width), F32),
            pltpu.SemaphoreType.DMA((2 * local,)),
        ],
        compiler_params=params(24),
        name="attend",
    )(
        got,
        *collected,
        *brought,
        *keep_in_hbm(cache_latent, cache_rope.transpose(0, 2, 1)),
    )
    got = exchange(sent, KV)

    sent = pl.pallas_call(
        functools.partial(
            combine_kernel,
            kv_size=kv_size,
            groups=groups,
            local=local,
            first=2 * latent_width,
        ),
        out_shape=jax.ShapeDtypeStruct((everyone, local, w_out.shape[1]), BF16),
        in_specs=[in_vmem()] * 5,
        out_specs=in_vmem(),
        compiler_params=params(8),
        name="combine",
    )(got, *collected)
    got = exchange(sent, SPREAD)
    return pl.pallas_call(
        functools.partial(finish_kernel, kv_size=kv_size, groups=groups, local=local),
        out_shape=jax.ShapeDtypeStruct((seqs, w_out.shape[1]), BF16),
        in_specs=[in_vmem(), in_vmem()],
        out_specs=in_vmem(),
        compiler_params=params(8),
        name="finish",
    )(got, out_gain[None])


def solution(mesh):
    finer = Mesh(mesh.devices.reshape(4, 4, mesh.shape["tp"] // 2, 2), ALL)

    return jax.shard_map(
        on_device,
        mesh=finer,
        in_specs=(
            P(None, KV),
            P(KV),
            P(KV, TP),
            P(KV, None),
            P(KV, None),
            P(),
            P(TP, None, None),
            P(TP, None, None),
            P(TP, KV),
            P(KV),
            P(TP, KV, None),
            P(TP, KV, None),
            P(),
        ),
        out_specs=P(None, KV),
        check_vma=False,
    )
```

```python
import functools

import jax
import jax.numpy as jnp
import numpy as np
from jax import lax
from jax.experimental import pallas as pl
from jax.experimental.pallas import tpu as pltpu
from jax.sharding import Mesh
from jax.sharding import PartitionSpec as P


KV = ("kv_0", "kv_1")
TP = ("y", "core")
ALL = KV + TP
SPREAD = ("core",) + KV + ("y",)
EPSILON = 1e-06
NEGATIVE = -1e30
F32 = jnp.float32
BF16 = jnp.bfloat16

NT = (((1,), (1,)), ((), ()))
NN = (((1,), (0,)), ((), ()))


def dot(a, b, dims):
    return lax.dot_general(a, b, dims, preferred_element_type=F32)


def params(mib):
    return pltpu.CompilerParams(vmem_limit_bytes=mib * 1024 * 1024)


def in_vmem():
    return pl.BlockSpec(memory_space=pltpu.VMEM)


def in_hbm():
    return pl.BlockSpec(memory_space=pltpu.HBM)


def keep_in_hbm(*arrays):
    return [pltpu.with_memory_space_constraint(x, pltpu.HBM) for x in arrays]


def lanes(shape):
    return lax.broadcasted_iota(jnp.int32, shape, 1)


def rows(shape):
    return lax.broadcasted_iota(jnp.int32, shape, 0)


def block_of(kv, tp, kv_size):
    cores = lax.axis_size("core")
    return (tp % cores * kv_size + kv) * lax.axis_size("y") + tp // cores


def project_kernel(
    tokens, gain, wq, wd, wr, wk, wv, wo, out, own, tokens_, gain_, wq_, wd_, wr_, sems
):
    tp = lax.axis_index(TP)
    groups = lax.axis_size(TP)
    kv_size = lax.axis_size(KV)
    deep = wk.shape[1]
    pairs = (
        (tokens, tokens_),
        (gain, gain_),
        (wq, wq_),
        (wd, wd_),
        (wr, wr_),
        (wk.at[0], own.at[pl.ds(0, deep)]),
        (wv.at[0], own.at[pl.ds(deep, deep)]),
        (wo, own.at[pl.ds(2 * deep, wo.shape[0])]),
    )
    copies = [pltpu.make_async_copy(x, y, sems.at[n]) for n, (x, y) in enumerate(pairs)]
    for copy in copies:
        copy.start()
    for copy in copies[:5]:
        copy.wait()
    scaled = (tokens_[...].astype(F32) * gain_[...]).astype(BF16)
    query = dot(scaled, wq_[...], NT)
    latent = dot(scaled, wd_[...], NN)
    rope = dot(scaled, wr_[...], NT)
    seqs = scaled.shape[0]
    local = seqs // groups
    chunk = latent.shape[1] // groups
    part = latent[:, :chunk]
    for g in range(1, groups):
        part = jnp.where(tp == g, latent[:, g * chunk : (g + 1) * chunk], part)
    width = rope.shape[1]
    rope = jnp.where(lanes(rope.shape) // (width // groups) == tp, rope, 0.0)
    first = query[:, :128].astype(BF16)
    fresh = jnp.concatenate([part, rope], axis=1)
    nothing = jnp.zeros((1, 128), F32)
    for t in range(groups):
        turn = query[t * local : (t + 1) * local, 128:]
        turn = jnp.concatenate([turn[: local // 2], turn[local // 2 :]], axis=1).astype(BF16)
        tiles = [first[t * local + n : t * local + n + 2] for n in range(0, local, 2)]
        tiles += [turn[n : n + 2] for n in range(0, local // 2, 2)]
        for j in range(local):
            r = t * local + j
            new = jnp.concatenate([fresh[r : r + 1], nothing], axis=0).astype(BF16)
            for c in range(kv_size // local):
                b = block_of(c * local + j, t, kv_size)
                for n, tile in enumerate(tiles + [new]):
                    out[b, :, n * 128 : (n + 1) * 128] = tile
    for copy in copies[5:]:
        copy.wait()


def bring_kernel(latents, lengths_, frequencies_, gain_, early, lengths, frequencies, gain, sems):
    pairs = (
        (latents.at[pl.ds(0, 1)], early),
        (lengths_, lengths),
        (frequencies_, frequencies),
        (gain_, gain),
    )
    copies = [pltpu.make_async_copy(x, y, sems.at[n]) for n, (x, y) in enumerate(pairs)]
    for copy in copies:
        copy.start()
    for copy in copies:
        copy.wait()


def rotate(values, cosine, sine):
    half = values.shape[1] // 2
    swapped = jnp.concatenate([values[:, half:], values[:, :half]], axis=1)
    return values * cosine + swapped * sine


def attend_kernel(
    got, near, opposite, far, far_opposite, early, lengths, frequencies, gain, latents, ropes,
    out, cache, cache_rope,
    sums, lifted, turned, scored, weights, means, sems,
    *, factor, nope,
):
    kv = lax.axis_index(KV)
    tp = lax.axis_index(TP)
    kv_size = lax.axis_size(KV)
    groups = lax.axis_size(TP)
    local, _, positions = cache_rope.shape
    latent_width = cache.shape[2]
    width = cache_rope.shape[1]
    copies = []
    for s in range(local):
        b = pltpu.make_async_copy(ropes.at[s], cache_rope.at[s], sems.at[local + s])
        b.start()
        copies.append([b])
        if s > 0:
            a = pltpu.make_async_copy(latents.at[s], cache.at[s - 1], sems.at[s])
            a.start()
            copies[s].append(a)

    def cached(s):
        return cache[s - 1] if s > 0 else early[0]

    for h in range(groups):
        total = got[block_of(0, h, kv_size)].astype(F32)
        for k in range(1, kv_size):
            total = total + got[block_of(k, h, kv_size)].astype(F32)
        pieces = [total[:, n * 128 : (n + 1) * 128] for n in range(7)]
        turn = jnp.concatenate(pieces[4:6], axis=0)
        sums[h, :, :nope] = jnp.concatenate(pieces[:4], axis=0)
        sums[h, :, nope : nope + width] = jnp.concatenate(
            [turn[:, :width], turn[:, width:]], axis=0
        )
        sums[h, 0:1, nope + width :] = pieces[6][0:1, :width]
        sums[h, 1:2, nope + width :] = pieces[6][0:1, width:]
    shape = (local, lengths.shape[1])
    length = jnp.sum(
        jnp.where(lanes(shape) == rows(shape) + tp * local, lengths[...], 0), axis=1, keepdims=True
    )
    lane = lanes((local, width))
    angles = length.astype(F32) * frequencies[...]
    cosine = jnp.cos(angles)
    sine = jnp.sin(angles)
    sine = jnp.where(lane < width // 2, -sine, sine)
    half = groups // 2
    y = tp // 2
    core = lax.rem(tp, 2)
    for i in range(groups):
        step = (0, half - 1, 1, 2)[i % half]
        head = 2 * lax.rem(y + step, half) + (core if i < half else 1 - core)
        q = sums[head]
        w = weights_of((near, opposite, far, far_opposite), i)
        lifted[i] = dot(q[:, :nope].astype(BF16), w[:latent_width, :], NT)
        turned[i] = rotate(q[:, nope : nope + width].astype(BF16).astype(F32), cosine, sine)
    raw = jnp.concatenate([sums[h][0:1, nope + width :] for h in range(groups)], axis=1)
    rope_raw = sums[0][1:2, nope + width :]
    for h in range(1, groups):
        rope_raw = rope_raw + sums[h][1:2, nope + width :]
    square = jnp.sum(raw * raw, axis=1, keepdims=True) / latent_width
    new_latent = (raw * lax.rsqrt(square + EPSILON) * gain[...]).astype(BF16).astype(F32)
    new_seq = lax.rem(kv, local)
    mine = rows((local, width)) == new_seq
    new_rope = rotate(
        rope_raw,
        jnp.sum(jnp.where(mine, cosine, 0.0), axis=0, keepdims=True),
        jnp.sum(jnp.where(mine, sine, 0.0), axis=0, keepdims=True),
    )
    new_rope = new_rope.astype(BF16).astype(F32)
    pairs = local * groups
    for s in range(local):
        q = lifted[:, s, :].astype(BF16)
        qr = turned[:, s, :].astype(BF16)
        fresh = jnp.sum(q.astype(F32) * new_latent, axis=1, keepdims=True) + jnp.sum(
            qr.astype(F32) * new_rope, axis=1, keepdims=True
        )
        for copy in copies[s]:
            copy.wait()
        r = s * groups
        scored[r : r + groups, :positions] = dot(q, cached(s), NT) + dot(qr, cache_rope[s], NN)
        scored[r : r + groups, positions:] = jnp.broadcast_to(fresh, (groups, 128))
    scores = scored[:, :positions] * factor
    row = rows((pairs, 1))
    sequence = row // groups
    limit = jnp.zeros((pairs, 1), jnp.int32)
    for s in range(local):
        limit = jnp.where(sequence == s, length[s : s + 1, :], limit)
    is_new = jnp.logical_and(sequence == new_seq, kv < local)
    new = jnp.where(is_new, scored[:, positions : positions + 1] * factor, NEGATIVE)
    visible = kv * positions + lanes((pairs, positions)) < limit
    top = jnp.max(jnp.where(visible, scores, NEGATIVE), axis=1, keepdims=True)
    top = jnp.maximum(top, new)
    weight = jnp.where(visible, jnp.exp(scores - top), 0.0)
    new_weight = jnp.where(is_new, jnp.exp(new - top), 0.0)
    total = jnp.sum(weight, axis=1, keepdims=True) + new_weight
    weights[...] = weight.astype(BF16)
    some = total > 0.0
    safe = jnp.where(some, total, 1.0)
    inverse = 1.0 / safe
    logs = jnp.where(some, top + jnp.log(safe), NEGATIVE)
    rounded = new_weight.astype(BF16).astype(F32)
    for s in range(local):
        r = slice(s * groups, (s + 1) * groups)
        mixed = dot(weights[r, :], cached(s), NN) + rounded[r] * new_latent
        means[s] = mixed * inverse[r]
    for i in range(groups):
        w = weights_of((near, opposite, far, far_opposite), i)
        x = means[:, i, :].astype(BF16)
        up = dot(x, w[latent_width : 2 * latent_width, :], NN).astype(BF16)
        for k in range(kv_size):
            out[k, i * local : (i + 1) * local, :] = up
    lane = lanes((local, 128))
    table = jnp.zeros((groups, 128), F32)
    for s in range(local):
        table = jnp.where(lanes((groups, 128)) == s, logs[s * groups : (s + 1) * groups], table)
    table = jnp.concatenate([table, jnp.zeros((128 - groups, 128), F32)], axis=0)
    table = jnp.transpose(table)[:local]
    high = table.astype(BF16).astype(F32)
    rest = table - high
    middle = rest.astype(BF16).astype(F32)
    low = (rest - middle).astype(BF16).astype(F32)
    packed = jnp.where(
        lane < groups,
        high,
        jnp.where(
            lane < 2 * groups,
            pltpu.roll(middle, groups, 1),
            jnp.where(lane < 3 * groups, pltpu.roll(low, 2 * groups, 1), 0.0),
        ),
    ).astype(BF16)
    for k in range(kv_size):
        out[k, groups * local :, :] = packed


def weights_of(collected, i):
    near, opposite, far, far_opposite = collected
    places = near.shape[0] + 1
    stacked, single = (near, opposite) if i < places else (far, far_opposite)
    return single if i % places == places - 1 else stacked.at[i % places]


def combine_kernel(got, near, opposite, far, far_opposite, out, *, kv_size, groups, local, first):
    logs = []
    for k in range(kv_size):
        x = got[k, groups * local :, :].astype(F32)
        logs.append(x + pltpu.roll(x, 128 - groups, 1) + pltpu.roll(x, 128 - 2 * groups, 1))
    top = functools.reduce(jnp.maximum, logs)
    shares = [jnp.exp(x - top) for x in logs]
    total = functools.reduce(jnp.add, shares)
    inverse = 1.0 / total
    shares = [x * inverse for x in shares]
    mixed = jnp.zeros((local, out.shape[2]), F32)
    for i in range(groups):
        head = jnp.zeros((local, 128), F32)
        for k in range(kv_size):
            part = got[k, i * local : (i + 1) * local, :].astype(F32)
            head = head + part * shares[k][:, i : i + 1]
        w = weights_of((near, opposite, far, far_opposite), i)
        mixed = mixed + dot(head.astype(BF16), w[first:, :], NN)
    mixed = mixed.astype(BF16)
    for d in range(out.shape[0]):
        out[d] = mixed


def finish_kernel(got, gain, out, *, kv_size, groups, local):
    kv = lax.axis_index(KV)
    width = got.shape[2]
    for t in range(groups):
        squares = jnp.zeros((local, width), F32)
        for k in range(kv_size):
            x = got[block_of(k, t, kv_size)].astype(F32)
            squares = squares + x * x
        mean = jnp.sum(squares, axis=1, keepdims=True) / (width * kv_size)
        own = got[block_of(kv, t, kv_size)].astype(F32)
        out[t * local : (t + 1) * local, :] = (
            own * lax.rsqrt(mean + EPSILON) * gain[...]
        ).astype(BF16)


def exchange(value, axes):
    return lax.all_to_all(value, axes, split_axis=0, concat_axis=0, tiled=True)


def swap(value):
    return lax.ppermute(value, TP, [(i, i ^ 1) for i in range(lax.axis_size(TP))])


def along(own):
    size = lax.axis_size(TP)
    collected = []
    for step in (1, 3, 2):
        pairs = [(i, (i + 2 * step) % size) for i in range(size)]
        collected.append(lax.ppermute(own, TP, pairs))
    return collected


def on_device(
    tokens,
    token_gain,
    w_query,
    w_down_kv,
    w_rope_key,
    latent_gain,
    w_key_up,
    w_value_up,
    w_out,
    out_gain,
    cache_latent,
    cache_rope,
    lengths,
):
    kv_size = lax.axis_size(KV)
    groups = lax.axis_size(TP)
    everyone = kv_size * groups
    seqs, width = tokens.shape
    local, positions, latent_width = cache_latent.shape
    rope = cache_rope.shape[2]
    nope = w_key_up.shape[2]
    value = w_value_up.shape[2]
    factor = (nope + rope) ** (-0.5)

    sent, own = pl.pallas_call(
        project_kernel,
        out_shape=(
            jax.ShapeDtypeStruct((everyone, 2, 896), BF16),
            jax.ShapeDtypeStruct((2 * latent_width + value, nope), BF16),
        ),
        in_specs=[in_hbm()] * 8,
        out_specs=(in_vmem(),) * 2,
        scratch_shapes=[
            pltpu.VMEM((seqs, width), BF16),
            pltpu.VMEM((1, width), F32),
            pltpu.VMEM((nope + rope, width), BF16),
            pltpu.VMEM((width, latent_width), BF16),
            pltpu.VMEM((rope, width), BF16),
            pltpu.SemaphoreType.DMA((8,)),
        ],
        compiler_params=params(8),
        name="project",
    )(
        *keep_in_hbm(
            tokens,
            token_gain[None],
            w_query.T,
            w_down_kv,
            w_rope_key.T,
            w_key_up,
            w_value_up,
            w_out,
        )
    )

    before, after, opposite = along(own)
    near = jnp.stack([own, before, after])
    far = swap(near)
    far_opposite = swap(opposite)
    collected = (near, opposite, far, far_opposite)

    got = exchange(sent, SPREAD)
    powers = np.arange(0, rope, 2, dtype=np.float64) / rope
    frequencies = np.tile(1.0 / 10000.0**powers, 2)[None].astype(np.float32)
    brought = pl.pallas_call(
        bring_kernel,
        out_shape=(
            jax.ShapeDtypeStruct((1, positions, latent_width), BF16),
            jax.ShapeDtypeStruct((1, seqs), jnp.int32),
            jax.ShapeDtypeStruct((1, rope), F32),
            jax.ShapeDtypeStruct((1, latent_width), F32),
        ),
        in_specs=[in_hbm()] * 4,
        out_specs=(in_vmem(),) * 4,
        scratch_shapes=[pltpu.SemaphoreType.DMA((4,))],
        compiler_params=params(8),
        name="bring",
    )(*keep_in_hbm(cache_latent, lengths[None], frequencies, latent_gain[None]))
    sent = pl.pallas_call(
        functools.partial(attend_kernel, factor=factor, nope=nope),
        out_shape=jax.ShapeDtypeStruct((kv_size, groups * local + local, value), BF16),
        in_specs=[in_vmem()] * 9 + [in_hbm()] * 2,
        out_specs=in_vmem(),
        scratch_shapes=[
            pltpu.VMEM((local - 1, positions, latent_width), BF16),
            pltpu.VMEM((local, rope, positions), BF16),
            pltpu.VMEM((groups, local, 256), F32),
            pltpu.VMEM((groups, local, latent_width), F32),
            pltpu.VMEM((groups, local, rope), F32),
            pltpu.VMEM((local * groups, positions + 128), F32),
            pltpu.VMEM((local * groups, positions), BF16),
            pltpu.VMEM((local, groups, latent_width), F32),
            pltpu.SemaphoreType.DMA((2 * local,)),
        ],
        compiler_params=params(24),
        name="attend",
    )(
        got,
        *collected,
        *brought,
        *keep_in_hbm(cache_latent, cache_rope.transpose(0, 2, 1)),
    )
    got = exchange(sent, KV)

    sent = pl.pallas_call(
        functools.partial(
            combine_kernel,
            kv_size=kv_size,
            groups=groups,
            local=local,
            first=2 * latent_width,
        ),
        out_shape=jax.ShapeDtypeStruct((everyone, local, w_out.shape[1]), BF16),
        in_specs=[in_vmem()] * 5,
        out_specs=in_vmem(),
        compiler_params=params(8),
        name="combine",
    )(got, *collected)
    got = exchange(sent, SPREAD)
    return pl.pallas_call(
        functools.partial(finish_kernel, kv_size=kv_size, groups=groups, local=local),
        out_shape=jax.ShapeDtypeStruct((seqs, w_out.shape[1]), BF16),
        in_specs=[in_vmem(), in_vmem()],
        out_specs=in_vmem(),
        compiler_params=params(8),
        name="finish",
    )(got, out_gain[None])


def solution(mesh):
    finer = Mesh(mesh.devices.reshape(4, 4, mesh.shape["tp"] // 2, 2), ALL)

    return jax.shard_map(
        on_device,
        mesh=finer,
        in_specs=(
            P(None, KV),
            P(KV),
            P(KV, TP),
            P(KV, None),
            P(KV, None),
            P(),
            P(TP, None, None),
            P(TP, None, None),
            P(TP, KV),
            P(KV),
            P(TP, KV, None),
            P(TP, KV, None),
            P(),
        ),
        out_specs=P(None, KV),
        check_vma=False,
    )
```

```python
import functools

import jax
import jax.numpy as jnp
import numpy as np
from jax import lax
from jax.experimental import pallas as pl
from jax.experimental.pallas import tpu as pltpu
from jax.sharding import Mesh
from jax.sharding import PartitionSpec as P


KV = ("kv_0", "kv_1")
TP = ("y", "core")
ALL = KV + TP
SPREAD = ("core",) + KV + ("y",)
EPSILON = 1e-06
NEGATIVE = -1e30
F32 = jnp.float32
BF16 = jnp.bfloat16

NT = (((1,), (1,)), ((), ()))
NN = (((1,), (0,)), ((), ()))


def dot(a, b, dims):
    return lax.dot_general(a, b, dims, preferred_element_type=F32)


def params(mib):
    return pltpu.CompilerParams(vmem_limit_bytes=mib * 1024 * 1024)


def in_vmem():
    return pl.BlockSpec(memory_space=pltpu.VMEM)


def in_hbm():
    return pl.BlockSpec(memory_space=pltpu.HBM)


def keep_in_hbm(*arrays):
    return [pltpu.with_memory_space_constraint(x, pltpu.HBM) for x in arrays]


def lanes(shape):
    return lax.broadcasted_iota(jnp.int32, shape, 1)


def rows(shape):
    return lax.broadcasted_iota(jnp.int32, shape, 0)


def block_of(kv, tp, kv_size):
    cores = lax.axis_size("core")
    return (tp % cores * kv_size + kv) * lax.axis_size("y") + tp // cores


def project_kernel(
    tokens, gain, wq, wd, wr, wk, wv, wo, out, own, tokens_, gain_, wq_, wd_, wr_, sems
):
    tp = lax.axis_index(TP)
    groups = lax.axis_size(TP)
    kv_size = lax.axis_size(KV)
    deep = wk.shape[1]
    pairs = (
        (tokens, tokens_),
        (gain, gain_),
        (wq, wq_),
        (wd, wd_),
        (wr, wr_),
        (wk.at[0], own.at[pl.ds(0, deep)]),
        (wv.at[0], own.at[pl.ds(deep, deep)]),
        (wo, own.at[pl.ds(2 * deep, wo.shape[0])]),
    )
    copies = [pltpu.make_async_copy(x, y, sems.at[n]) for n, (x, y) in enumerate(pairs)]
    for copy in copies:
        copy.start()
    for copy in copies[:5]:
        copy.wait()
    scaled = (tokens_[...].astype(F32) * gain_[...]).astype(BF16)
    query = dot(scaled, wq_[...], NT)
    latent = dot(scaled, wd_[...], NN)
    rope = dot(scaled, wr_[...], NT)
    seqs = scaled.shape[0]
    local = seqs // groups
    chunk = latent.shape[1] // groups
    part = latent[:, :chunk]
    for g in range(1, groups):
        part = jnp.where(tp == g, latent[:, g * chunk : (g + 1) * chunk], part)
    width = rope.shape[1]
    rope = jnp.where(lanes(rope.shape) // (width // groups) == tp, rope, 0.0)
    first = query[:, :128].astype(BF16)
    fresh = jnp.concatenate([part, rope], axis=1)
    nothing = jnp.zeros((1, 128), F32)
    for t in range(groups):
        turn = query[t * local : (t + 1) * local, 128:]
        turn = jnp.concatenate([turn[: local // 2], turn[local // 2 :]], axis=1).astype(BF16)
        tiles = [first[t * local + n : t * local + n + 2] for n in range(0, local, 2)]
        tiles += [turn[n : n + 2] for n in range(0, local // 2, 2)]
        for j in range(local):
            r = t * local + j
            new = jnp.concatenate([fresh[r : r + 1], nothing], axis=0).astype(BF16)
            for c in range(kv_size // local):
                b = block_of(c * local + j, t, kv_size)
                for n, tile in enumerate(tiles + [new]):
                    out[b, :, n * 128 : (n + 1) * 128] = tile
    for copy in copies[5:]:
        copy.wait()


def rotate(values, cosine, sine):
    half = values.shape[1] // 2
    swapped = jnp.concatenate([values[:, half:], values[:, :half]], axis=1)
    return values * cosine + swapped * sine


def attend_kernel(
    got, near, opposite, far, far_opposite, lengths_, frequencies_, gain_, latents, ropes,
    out, lengths, frequencies, gain, cache, cache_rope,
    sums, lifted, turned, scored, weights, means, sems,
    *, factor, nope,
):
    kv = lax.axis_index(KV)
    tp = lax.axis_index(TP)
    kv_size = lax.axis_size(KV)
    groups = lax.axis_size(TP)
    local, positions, latent_width = cache.shape
    width = cache_rope.shape[1]
    small = []
    for n, (a, b) in enumerate(
        ((lengths_, lengths), (frequencies_, frequencies), (gain_, gain))
    ):
        small.append(pltpu.make_async_copy(a, b, sems.at[2 * local + n]))
        small[n].start()
    copies = []
    for s in range(local):
        a = pltpu.make_async_copy(latents.at[s], cache.at[s], sems.at[s])
        b = pltpu.make_async_copy(ropes.at[s], cache_rope.at[s], sems.at[local + s])
        a.start()
        b.start()
        copies.append((a, b))
    for h in range(groups):
        total = got[block_of(0, h, kv_size)].astype(F32)
        for k in range(1, kv_size):
            total = total + got[block_of(k, h, kv_size)].astype(F32)
        pieces = [total[:, n * 128 : (n + 1) * 128] for n in range(7)]
        turn = jnp.concatenate(pieces[4:6], axis=0)
        sums[h, :, :nope] = jnp.concatenate(pieces[:4], axis=0)
        sums[h, :, nope : nope + width] = jnp.concatenate(
            [turn[:, :width], turn[:, width:]], axis=0
        )
        sums[h, 0:1, nope + width :] = pieces[6][0:1, :width]
        sums[h, 1:2, nope + width :] = pieces[6][0:1, width:]
    for copy in small:
        copy.wait()
    shape = (local, lengths.shape[1])
    length = jnp.sum(
        jnp.where(lanes(shape) == rows(shape) + tp * local, lengths[...], 0), axis=1, keepdims=True
    )
    lane = lanes((local, width))
    angles = length.astype(F32) * frequencies[...]
    cosine = jnp.cos(angles)
    sine = jnp.sin(angles)
    sine = jnp.where(lane < width // 2, -sine, sine)
    half = groups // 2
    y = tp // 2
    core = lax.rem(tp, 2)
    for i in range(groups):
        step = (0, half - 1, 1, 2)[i % half]
        head = 2 * lax.rem(y + step, half) + (core if i < half else 1 - core)
        q = sums[head]
        w = weights_of((near, opposite, far, far_opposite), i)
        lifted[i] = dot(q[:, :nope].astype(BF16), w[:latent_width, :], NT)
        turned[i] = rotate(q[:, nope : nope + width].astype(BF16).astype(F32), cosine, sine)
    raw = jnp.concatenate([sums[h][0:1, nope + width :] for h in range(groups)], axis=1)
    rope_raw = sums[0][1:2, nope + width :]
    for h in range(1, groups):
        rope_raw = rope_raw + sums[h][1:2, nope + width :]
    square = jnp.sum(raw * raw, axis=1, keepdims=True) / latent_width
    new_latent = (raw * lax.rsqrt(square + EPSILON) * gain[...]).astype(BF16).astype(F32)
    new_seq = lax.rem(kv, local)
    mine = rows((local, width)) == new_seq
    new_rope = rotate(
        rope_raw,
        jnp.sum(jnp.where(mine, cosine, 0.0), axis=0, keepdims=True),
        jnp.sum(jnp.where(mine, sine, 0.0), axis=0, keepdims=True),
    )
    new_rope = new_rope.astype(BF16).astype(F32)
    pairs = local * groups
    for s in range(local):
        q = lifted[:, s, :].astype(BF16)
        qr = turned[:, s, :].astype(BF16)
        fresh = jnp.sum(q.astype(F32) * new_latent, axis=1, keepdims=True) + jnp.sum(
            qr.astype(F32) * new_rope, axis=1, keepdims=True
        )
        for copy in copies[s]:
            copy.wait()
        r = s * groups
        scored[r : r + groups, :positions] = dot(q, cache[s], NT) + dot(qr, cache_rope[s], NN)
        scored[r : r + groups, positions:] = jnp.broadcast_to(fresh, (groups, 128))
    scores = scored[:, :positions] * factor
    row = rows((pairs, 1))
    sequence = row // groups
    limit = jnp.zeros((pairs, 1), jnp.int32)
    for s in range(local):
        limit = jnp.where(sequence == s, length[s : s + 1, :], limit)
    is_new = jnp.logical_and(sequence == new_seq, kv < local)
    new = jnp.where(is_new, scored[:, positions : positions + 1] * factor, NEGATIVE)
    visible = kv * positions + lanes((pairs, positions)) < limit
    top = jnp.max(jnp.where(visible, scores, NEGATIVE), axis=1, keepdims=True)
    top = jnp.maximum(top, new)
    weight = jnp.where(visible, jnp.exp(scores - top), 0.0)
    new_weight = jnp.where(is_new, jnp.exp(new - top), 0.0)
    total = jnp.sum(weight, axis=1, keepdims=True) + new_weight
    weights[...] = weight.astype(BF16)
    some = total > 0.0
    safe = jnp.where(some, total, 1.0)
    inverse = 1.0 / safe
    logs = jnp.where(some, top + jnp.log(safe), NEGATIVE)
    rounded = new_weight.astype(BF16).astype(F32)
    for s in range(local):
        r = slice(s * groups, (s + 1) * groups)
        mixed = dot(weights[r, :], cache[s], NN) + rounded[r] * new_latent
        means[s] = mixed * inverse[r]
    for i in range(groups):
        w = weights_of((near, opposite, far, far_opposite), i)
        x = means[:, i, :].astype(BF16)
        up = dot(x, w[latent_width : 2 * latent_width, :], NN).astype(BF16)
        for k in range(kv_size):
            out[k, i * local : (i + 1) * local, :] = up
    lane = lanes((local, 128))
    table = jnp.zeros((groups, 128), F32)
    for s in range(local):
        table = jnp.where(lanes((groups, 128)) == s, logs[s * groups : (s + 1) * groups], table)
    table = jnp.concatenate([table, jnp.zeros((128 - groups, 128), F32)], axis=0)
    table = jnp.transpose(table)[:local]
    high = table.astype(BF16).astype(F32)
    rest = table - high
    middle = rest.astype(BF16).astype(F32)
    low = (rest - middle).astype(BF16).astype(F32)
    packed = jnp.where(
        lane < groups,
        high,
        jnp.where(
            lane < 2 * groups,
            pltpu.roll(middle, groups, 1),
            jnp.where(lane < 3 * groups, pltpu.roll(low, 2 * groups, 1), 0.0),
        ),
    ).astype(BF16)
    for k in range(kv_size):
        out[k, groups * local :, :] = packed


def weights_of(collected, i):
    near, opposite, far, far_opposite = collected
    places = near.shape[0] + 1
    stacked, single = (near, opposite) if i < places else (far, far_opposite)
    return single if i % places == places - 1 else stacked.at[i % places]


def combine_kernel(got, near, opposite, far, far_opposite, out, *, kv_size, groups, local, first):
    logs = []
    for k in range(kv_size):
        x = got[k, groups * local :, :].astype(F32)
        logs.append(x + pltpu.roll(x, 128 - groups, 1) + pltpu.roll(x, 128 - 2 * groups, 1))
    top = functools.reduce(jnp.maximum, logs)
    shares = [jnp.exp(x - top) for x in logs]
    total = functools.reduce(jnp.add, shares)
    inverse = 1.0 / total
    shares = [x * inverse for x in shares]
    mixed = jnp.zeros((local, out.shape[2]), F32)
    for i in range(groups):
        head = jnp.zeros((local, 128), F32)
        for k in range(kv_size):
            part = got[k, i * local : (i + 1) * local, :].astype(F32)
            head = head + part * shares[k][:, i : i + 1]
        w = weights_of((near, opposite, far, far_opposite), i)
        mixed = mixed + dot(head.astype(BF16), w[first:, :], NN)
    mixed = mixed.astype(BF16)
    for d in range(out.shape[0]):
        out[d] = mixed


def finish_kernel(got, gain, out, *, kv_size, groups, local):
    kv = lax.axis_index(KV)
    width = got.shape[2]
    for t in range(groups):
        squares = jnp.zeros((local, width), F32)
        for k in range(kv_size):
            x = got[block_of(k, t, kv_size)].astype(F32)
            squares = squares + x * x
        mean = jnp.sum(squares, axis=1, keepdims=True) / (width * kv_size)
        own = got[block_of(kv, t, kv_size)].astype(F32)
        out[t * local : (t + 1) * local, :] = (
            own * lax.rsqrt(mean + EPSILON) * gain[...]
        ).astype(BF16)


def exchange(value, axes):
    return lax.all_to_all(value, axes, split_axis=0, concat_axis=0, tiled=True)


def swap(value):
    return lax.ppermute(value, TP, [(i, i ^ 1) for i in range(lax.axis_size(TP))])


def along(own):
    size = lax.axis_size(TP)
    collected = []
    for step in (1, 3, 2):
        pairs = [(i, (i + 2 * step) % size) for i in range(size)]
        collected.append(lax.ppermute(own, TP, pairs))
    return collected


def on_device(
    tokens,
    token_gain,
    w_query,
    w_down_kv,
    w_rope_key,
    latent_gain,
    w_key_up,
    w_value_up,
    w_out,
    out_gain,
    cache_latent,
    cache_rope,
    lengths,
):
    kv_size = lax.axis_size(KV)
    groups = lax.axis_size(TP)
    everyone = kv_size * groups
    seqs, width = tokens.shape
    local, positions, latent_width = cache_latent.shape
    rope = cache_rope.shape[2]
    nope = w_key_up.shape[2]
    value = w_value_up.shape[2]
    factor = (nope + rope) ** (-0.5)

    sent, own = pl.pallas_call(
        project_kernel,
        out_shape=(
            jax.ShapeDtypeStruct((everyone, 2, 896), BF16),
            jax.ShapeDtypeStruct((2 * latent_width + value, nope), BF16),
        ),
        in_specs=[in_hbm()] * 8,
        out_specs=(in_vmem(),) * 2,
        scratch_shapes=[
            pltpu.VMEM((seqs, width), BF16),
            pltpu.VMEM((1, width), F32),
            pltpu.VMEM((nope + rope, width), BF16),
            pltpu.VMEM((width, latent_width), BF16),
            pltpu.VMEM((rope, width), BF16),
            pltpu.SemaphoreType.DMA((8,)),
        ],
        compiler_params=params(8),
        name="project",
    )(
        *keep_in_hbm(
            tokens,
            token_gain[None],
            w_query.T,
            w_down_kv,
            w_rope_key.T,
            w_key_up,
            w_value_up,
            w_out,
        )
    )

    before, after, opposite = along(own)
    near = jnp.stack([own, before, after])
    far = swap(near)
    far_opposite = swap(opposite)
    collected = (near, opposite, far, far_opposite)

    got = exchange(sent, SPREAD)
    powers = np.arange(0, rope, 2, dtype=np.float64) / rope
    frequencies = np.tile(1.0 / 10000.0**powers, 2)[None].astype(np.float32)
    sent = pl.pallas_call(
        functools.partial(attend_kernel, factor=factor, nope=nope),
        out_shape=jax.ShapeDtypeStruct((kv_size, groups * local + local, value), BF16),
        in_specs=[in_vmem()] * 5 + [in_hbm()] * 5,
        out_specs=in_vmem(),
        scratch_shapes=[
            pltpu.VMEM((1, seqs), jnp.int32),
            pltpu.VMEM((1, rope), F32),
            pltpu.VMEM((1, latent_width), F32),
            pltpu.VMEM((local, positions, latent_width), BF16),
            pltpu.VMEM((local, rope, positions), BF16),
            pltpu.VMEM((groups, local, 256), F32),
            pltpu.VMEM((groups, local, latent_width), F32),
            pltpu.VMEM((groups, local, rope), F32),
            pltpu.VMEM((local * groups, positions + 128), F32),
            pltpu.VMEM((local * groups, positions), BF16),
            pltpu.VMEM((local, groups, latent_width), F32),
            pltpu.SemaphoreType.DMA((2 * local + 3,)),
        ],
        compiler_params=params(24),
        name="attend",
    )(
        got,
        *collected,
        *keep_in_hbm(
            lengths[None],
            frequencies,
            latent_gain[None],
            cache_latent,
            cache_rope.transpose(0, 2, 1),
        ),
    )
    got = exchange(sent, KV)

    sent = pl.pallas_call(
        functools.partial(
            combine_kernel,
            kv_size=kv_size,
            groups=groups,
            local=local,
            first=2 * latent_width,
        ),
        out_shape=jax.ShapeDtypeStruct((everyone, local, w_out.shape[1]), BF16),
        in_specs=[in_vmem()] * 5,
        out_specs=in_vmem(),
        compiler_params=params(8),
        name="combine",
    )(got, *collected)
    got = exchange(sent, SPREAD)
    return pl.pallas_call(
        functools.partial(finish_kernel, kv_size=kv_size, groups=groups, local=local),
        out_shape=jax.ShapeDtypeStruct((seqs, w_out.shape[1]), BF16),
        in_specs=[in_vmem(), in_vmem()],
        out_specs=in_vmem(),
        compiler_params=params(8),
        name="finish",
    )(got, out_gain[None])


def solution(mesh):
    finer = Mesh(mesh.devices.reshape(4, 4, mesh.shape["tp"] // 2, 2), ALL)

    return jax.shard_map(
        on_device,
        mesh=finer,
        in_specs=(
            P(None, KV),
            P(KV),
            P(KV, TP),
            P(KV, None),
            P(KV, None),
            P(),
            P(TP, None, None),
            P(TP, None, None),
            P(TP, KV),
            P(KV),
            P(TP, KV, None),
            P(TP, KV, None),
            P(),
        ),
        out_specs=P(None, KV),
        check_vma=False,
    )
```

```python
import functools

import jax
import jax.numpy as jnp
import numpy as np
from jax import lax
from jax.experimental import pallas as pl
from jax.experimental.pallas import tpu as pltpu
from jax.sharding import Mesh
from jax.sharding import PartitionSpec as P


KV = ("kv_0", "kv_1")
TP = ("y", "core")
ALL = KV + TP
SPREAD = ("core",) + KV + ("y",)
EPSILON = 1e-06
NEGATIVE = -1e30
F32 = jnp.float32
BF16 = jnp.bfloat16

NT = (((1,), (1,)), ((), ()))
NN = (((1,), (0,)), ((), ()))


def dot(a, b, dims):
    return lax.dot_general(a, b, dims, preferred_element_type=F32)


def params(mib):
    return pltpu.CompilerParams(vmem_limit_bytes=mib * 1024 * 1024)


def in_vmem():
    return pl.BlockSpec(memory_space=pltpu.VMEM)


def in_hbm():
    return pl.BlockSpec(memory_space=pltpu.HBM)


def keep_in_hbm(*arrays):
    return [pltpu.with_memory_space_constraint(x, pltpu.HBM) for x in arrays]


def lanes(shape):
    return lax.broadcasted_iota(jnp.int32, shape, 1)


def rows(shape):
    return lax.broadcasted_iota(jnp.int32, shape, 0)


def block_of(kv, tp, kv_size):
    cores = lax.axis_size("core")
    return (tp % cores * kv_size + kv) * lax.axis_size("y") + tp // cores


def project_kernel(
    tokens, gain, wq, wd, wr, wk, wv, wo, out, own, tokens_, gain_, wq_, wd_, wr_, sems
):
    tp = lax.axis_index(TP)
    groups = lax.axis_size(TP)
    kv_size = lax.axis_size(KV)
    deep = wk.shape[1]
    pairs = (
        (tokens, tokens_),
        (gain, gain_),
        (wq, wq_),
        (wd, wd_),
        (wr, wr_),
        (wk.at[0], own.at[pl.ds(0, deep)]),
        (wv.at[0], own.at[pl.ds(deep, deep)]),
        (wo, own.at[pl.ds(2 * deep, wo.shape[0])]),
    )
    copies = [pltpu.make_async_copy(x, y, sems.at[n]) for n, (x, y) in enumerate(pairs)]
    for copy in copies:
        copy.start()
    for copy in copies[:5]:
        copy.wait()
    scaled = (tokens_[...].astype(F32) * gain_[...]).astype(BF16)
    query = dot(scaled, wq_[...], NT)
    latent = dot(scaled, wd_[...], NN)
    rope = dot(scaled, wr_[...], NT)
    seqs = scaled.shape[0]
    local = seqs // groups
    chunk = latent.shape[1] // groups
    part = latent[:, :chunk]
    for g in range(1, groups):
        part = jnp.where(tp == g, latent[:, g * chunk : (g + 1) * chunk], part)
    width = rope.shape[1]
    rope = jnp.where(lanes(rope.shape) // (width // groups) == tp, rope, 0.0)
    first = query[:, :128].astype(BF16)
    fresh = jnp.concatenate([part, rope], axis=1)
    nothing = jnp.zeros((1, 128), F32)
    for t in range(groups):
        turn = query[t * local : (t + 1) * local, 128:]
        turn = jnp.concatenate([turn[: local // 2], turn[local // 2 :]], axis=1).astype(BF16)
        tiles = [first[t * local + n : t * local + n + 2] for n in range(0, local, 2)]
        tiles += [turn[n : n + 2] for n in range(0, local // 2, 2)]
        for j in range(local):
            r = t * local + j
            new = jnp.concatenate([fresh[r : r + 1], nothing], axis=0).astype(BF16)
            for c in range(kv_size // local):
                b = block_of(c * local + j, t, kv_size)
                for n, tile in enumerate(tiles + [new]):
                    out[b, :, n * 128 : (n + 1) * 128] = tile
    for copy in copies[5:]:
        copy.wait()


def rotate(values, cosine, sine):
    half = values.shape[1] // 2
    swapped = jnp.concatenate([values[:, half:], values[:, :half]], axis=1)
    return values * cosine + swapped * sine


def attend_kernel(
    got, near, last, far, far_last, lengths_, frequencies_, gain_, latents, ropes,
    out, lengths, frequencies, gain, cache, cache_rope,
    sums, lifted, turned, scored, weights, means, sems,
    *, factor, nope,
):
    kv = lax.axis_index(KV)
    tp = lax.axis_index(TP)
    kv_size = lax.axis_size(KV)
    groups = lax.axis_size(TP)
    local, positions, latent_width = cache.shape
    width = cache_rope.shape[1]
    small = []
    for n, (a, b) in enumerate(
        ((lengths_, lengths), (frequencies_, frequencies), (gain_, gain))
    ):
        small.append(pltpu.make_async_copy(a, b, sems.at[2 * local + n]))
        small[n].start()
    copies = []
    for s in range(local):
        a = pltpu.make_async_copy(latents.at[s], cache.at[s], sems.at[s])
        b = pltpu.make_async_copy(ropes.at[s], cache_rope.at[s], sems.at[local + s])
        a.start()
        b.start()
        copies.append((a, b))
    for h in range(groups):
        total = got[block_of(0, h, kv_size)].astype(F32)
        for k in range(1, kv_size):
            total = total + got[block_of(k, h, kv_size)].astype(F32)
        pieces = [total[:, n * 128 : (n + 1) * 128] for n in range(7)]
        turn = jnp.concatenate(pieces[4:6], axis=0)
        sums[h, :, :nope] = jnp.concatenate(pieces[:4], axis=0)
        sums[h, :, nope : nope + width] = jnp.concatenate(
            [turn[:, :width], turn[:, width:]], axis=0
        )
        sums[h, 0:1, nope + width :] = pieces[6][0:1, :width]
        sums[h, 1:2, nope + width :] = pieces[6][0:1, width:]
    for copy in small:
        copy.wait()
    shape = (local, lengths.shape[1])
    length = jnp.sum(
        jnp.where(lanes(shape) == rows(shape) + tp * local, lengths[...], 0), axis=1, keepdims=True
    )
    lane = lanes((local, width))
    angles = length.astype(F32) * frequencies[...]
    cosine = jnp.cos(angles)
    sine = jnp.sin(angles)
    sine = jnp.where(lane < width // 2, -sine, sine)
    half = groups // 2
    y = tp // 2
    core = lax.rem(tp, 2)
    for i in range(groups):
        step = (0, half - 1, 2, 1)[i % half]
        head = 2 * lax.rem(y + step, half) + (core if i < half else 1 - core)
        q = sums[head]
        w = weights_of((near, last, far, far_last), i)
        lifted[i] = dot(q[:, :nope].astype(BF16), w[:latent_width, :], NT)
        turned[i] = rotate(q[:, nope : nope + width].astype(BF16).astype(F32), cosine, sine)
    raw = jnp.concatenate([sums[h][0:1, nope + width :] for h in range(groups)], axis=1)
    rope_raw = sums[0][1:2, nope + width :]
    for h in range(1, groups):
        rope_raw = rope_raw + sums[h][1:2, nope + width :]
    square = jnp.sum(raw * raw, axis=1, keepdims=True) / latent_width
    new_latent = (raw * lax.rsqrt(square + EPSILON) * gain[...]).astype(BF16).astype(F32)
    new_seq = lax.rem(kv, local)
    mine = rows((local, width)) == new_seq
    new_rope = rotate(
        rope_raw,
        jnp.sum(jnp.where(mine, cosine, 0.0), axis=0, keepdims=True),
        jnp.sum(jnp.where(mine, sine, 0.0), axis=0, keepdims=True),
    )
    new_rope = new_rope.astype(BF16).astype(F32)
    pairs = local * groups
    for s in range(local):
        q = lifted[:, s, :].astype(BF16)
        qr = turned[:, s, :].astype(BF16)
        fresh = jnp.sum(q.astype(F32) * new_latent, axis=1, keepdims=True) + jnp.sum(
            qr.astype(F32) * new_rope, axis=1, keepdims=True
        )
        for copy in copies[s]:
            copy.wait()
        r = s * groups
        scored[r : r + groups, :positions] = dot(q, cache[s], NT) + dot(qr, cache_rope[s], NN)
        scored[r : r + groups, positions:] = jnp.broadcast_to(fresh, (groups, 128))
    scores = scored[:, :positions] * factor
    row = rows((pairs, 1))
    sequence = row // groups
    limit = jnp.zeros((pairs, 1), jnp.int32)
    for s in range(local):
        limit = jnp.where(sequence == s, length[s : s + 1, :], limit)
    is_new = jnp.logical_and(sequence == new_seq, kv < local)
    new = jnp.where(is_new, scored[:, positions : positions + 1] * factor, NEGATIVE)
    visible = kv * positions + lanes((pairs, positions)) < limit
    top = jnp.max(jnp.where(visible, scores, NEGATIVE), axis=1, keepdims=True)
    top = jnp.maximum(top, new)
    weight = jnp.where(visible, jnp.exp(scores - top), 0.0)
    new_weight = jnp.where(is_new, jnp.exp(new - top), 0.0)
    total = jnp.sum(weight, axis=1, keepdims=True) + new_weight
    weights[...] = weight.astype(BF16)
    some = total > 0.0
    safe = jnp.where(some, total, 1.0)
    inverse = 1.0 / safe
    logs = jnp.where(some, top + jnp.log(safe), NEGATIVE)
    rounded = new_weight.astype(BF16).astype(F32)
    for s in range(local):
        r = slice(s * groups, (s + 1) * groups)
        mixed = dot(weights[r, :], cache[s], NN) + rounded[r] * new_latent
        means[s] = mixed * inverse[r]
    for i in range(groups):
        w = weights_of((near, last, far, far_last), i)
        x = means[:, i, :].astype(BF16)
        up = dot(x, w[latent_width : 2 * latent_width, :], NN).astype(BF16)
        for k in range(kv_size):
            out[k, i * local : (i + 1) * local, :] = up
    lane = lanes((local, 128))
    table = jnp.zeros((groups, 128), F32)
    for s in range(local):
        table = jnp.where(lanes((groups, 128)) == s, logs[s * groups : (s + 1) * groups], table)
    table = jnp.concatenate([table, jnp.zeros((128 - groups, 128), F32)], axis=0)
    table = jnp.transpose(table)[:local]
    high = table.astype(BF16).astype(F32)
    rest = table - high
    middle = rest.astype(BF16).astype(F32)
    low = (rest - middle).astype(BF16).astype(F32)
    packed = jnp.where(
        lane < groups,
        high,
        jnp.where(
            lane < 2 * groups,
            pltpu.roll(middle, groups, 1),
            jnp.where(lane < 3 * groups, pltpu.roll(low, 2 * groups, 1), 0.0),
        ),
    ).astype(BF16)
    for k in range(kv_size):
        out[k, groups * local :, :] = packed


def weights_of(collected, i):
    near, last, far, far_last = collected
    places = near.shape[0] + 1
    stacked, single = (near, last) if i < places else (far, far_last)
    return single if i % places == places - 1 else stacked.at[i % places]


def combine_kernel(got, near, last, far, far_last, out, *, kv_size, groups, local, first):
    logs = []
    for k in range(kv_size):
        x = got[k, groups * local :, :].astype(F32)
        logs.append(x + pltpu.roll(x, 128 - groups, 1) + pltpu.roll(x, 128 - 2 * groups, 1))
    top = functools.reduce(jnp.maximum, logs)
    shares = [jnp.exp(x - top) for x in logs]
    total = functools.reduce(jnp.add, shares)
    inverse = 1.0 / total
    shares = [x * inverse for x in shares]
    mixed = jnp.zeros((local, out.shape[2]), F32)
    for i in range(groups):
        head = jnp.zeros((local, 128), F32)
        for k in range(kv_size):
            part = got[k, i * local : (i + 1) * local, :].astype(F32)
            head = head + part * shares[k][:, i : i + 1]
        w = weights_of((near, last, far, far_last), i)
        mixed = mixed + dot(head.astype(BF16), w[first:, :], NN)
    mixed = mixed.astype(BF16)
    for d in range(out.shape[0]):
        out[d] = mixed


def finish_kernel(got, gain, out, *, kv_size, groups, local):
    kv = lax.axis_index(KV)
    width = got.shape[2]
    for t in range(groups):
        squares = jnp.zeros((local, width), F32)
        for k in range(kv_size):
            x = got[block_of(k, t, kv_size)].astype(F32)
            squares = squares + x * x
        mean = jnp.sum(squares, axis=1, keepdims=True) / (width * kv_size)
        own = got[block_of(kv, t, kv_size)].astype(F32)
        out[t * local : (t + 1) * local, :] = (
            own * lax.rsqrt(mean + EPSILON) * gain[...]
        ).astype(BF16)


def exchange(value, axes):
    return lax.all_to_all(value, axes, split_axis=0, concat_axis=0, tiled=True)


def swap(value):
    return lax.ppermute(value, TP, [(i, i ^ 1) for i in range(lax.axis_size(TP))])


def along(own):
    size = lax.axis_size(TP)
    collected = []
    for step in (1, 3, 2):
        pairs = [(i, (i + 2 * step) % size) for i in range(size)]
        collected.append(lax.ppermute(own, TP, pairs))
    return collected


def on_device(
    tokens,
    token_gain,
    w_query,
    w_down_kv,
    w_rope_key,
    latent_gain,
    w_key_up,
    w_value_up,
    w_out,
    out_gain,
    cache_latent,
    cache_rope,
    lengths,
):
    kv_size = lax.axis_size(KV)
    groups = lax.axis_size(TP)
    everyone = kv_size * groups
    seqs, width = tokens.shape
    local, positions, latent_width = cache_latent.shape
    rope = cache_rope.shape[2]
    nope = w_key_up.shape[2]
    value = w_value_up.shape[2]
    factor = (nope + rope) ** (-0.5)

    sent, own = pl.pallas_call(
        project_kernel,
        out_shape=(
            jax.ShapeDtypeStruct((everyone, 2, 896), BF16),
            jax.ShapeDtypeStruct((2 * latent_width + value, nope), BF16),
        ),
        in_specs=[in_hbm()] * 8,
        out_specs=(in_vmem(),) * 2,
        scratch_shapes=[
            pltpu.VMEM((seqs, width), BF16),
            pltpu.VMEM((1, width), F32),
            pltpu.VMEM((nope + rope, width), BF16),
            pltpu.VMEM((width, latent_width), BF16),
            pltpu.VMEM((rope, width), BF16),
            pltpu.SemaphoreType.DMA((8,)),
        ],
        compiler_params=params(8),
        name="project",
    )(
        *keep_in_hbm(
            tokens,
            token_gain[None],
            w_query.T,
            w_down_kv,
            w_rope_key.T,
            w_key_up,
            w_value_up,
            w_out,
        )
    )

    before, after, opposite = along(own)
    near = jnp.stack([own, before, opposite])
    far = swap(near)
    far_last = swap(after)
    collected = (near, after, far, far_last)

    got = exchange(sent, SPREAD)
    powers = np.arange(0, rope, 2, dtype=np.float64) / rope
    frequencies = np.tile(1.0 / 10000.0**powers, 2)[None].astype(np.float32)
    sent = pl.pallas_call(
        functools.partial(attend_kernel, factor=factor, nope=nope),
        out_shape=jax.ShapeDtypeStruct((kv_size, groups * local + local, value), BF16),
        in_specs=[in_vmem()] * 5 + [in_hbm()] * 5,
        out_specs=in_vmem(),
        scratch_shapes=[
            pltpu.VMEM((1, seqs), jnp.int32),
            pltpu.VMEM((1, rope), F32),
            pltpu.VMEM((1, latent_width), F32),
            pltpu.VMEM((local, positions, latent_width), BF16),
            pltpu.VMEM((local, rope, positions), BF16),
            pltpu.VMEM((groups, local, 256), F32),
            pltpu.VMEM((groups, local, latent_width), F32),
            pltpu.VMEM((groups, local, rope), F32),
            pltpu.VMEM((local * groups, positions + 128), F32),
            pltpu.VMEM((local * groups, positions), BF16),
            pltpu.VMEM((local, groups, latent_width), F32),
            pltpu.SemaphoreType.DMA((2 * local + 3,)),
        ],
        compiler_params=params(24),
        name="attend",
    )(
        got,
        *collected,
        *keep_in_hbm(
            lengths[None],
            frequencies,
            latent_gain[None],
            cache_latent,
            cache_rope.transpose(0, 2, 1),
        ),
    )
    got = exchange(sent, KV)

    sent = pl.pallas_call(
        functools.partial(
            combine_kernel,
            kv_size=kv_size,
            groups=groups,
            local=local,
            first=2 * latent_width,
        ),
        out_shape=jax.ShapeDtypeStruct((everyone, local, w_out.shape[1]), BF16),
        in_specs=[in_vmem()] * 5,
        out_specs=in_vmem(),
        compiler_params=params(8),
        name="combine",
    )(got, *collected)
    got = exchange(sent, SPREAD)
    return pl.pallas_call(
        functools.partial(finish_kernel, kv_size=kv_size, groups=groups, local=local),
        out_shape=jax.ShapeDtypeStruct((seqs, w_out.shape[1]), BF16),
        in_specs=[in_vmem(), in_vmem()],
        out_specs=in_vmem(),
        compiler_params=params(8),
        name="finish",
    )(got, out_gain[None])


def solution(mesh):
    finer = Mesh(mesh.devices.reshape(4, 4, mesh.shape["tp"] // 2, 2), ALL)

    return jax.shard_map(
        on_device,
        mesh=finer,
        in_specs=(
            P(None, KV),
            P(KV),
            P(KV, TP),
            P(KV, None),
            P(KV, None),
            P(),
            P(TP, None, None),
            P(TP, None, None),
            P(TP, KV),
            P(KV),
            P(TP, KV, None),
            P(TP, KV, None),
            P(),
        ),
        out_specs=P(None, KV),
        check_vma=False,
    )
```

```python
import functools

import jax
import jax.numpy as jnp
import numpy as np
from jax import lax
from jax.experimental import pallas as pl
from jax.experimental.pallas import tpu as pltpu
from jax.sharding import Mesh
from jax.sharding import PartitionSpec as P


KV = ("kv_0", "kv_1")
TP = ("y", "core")
ALL = KV + TP
SPREAD = ("core", "kv_0", "y", "kv_1")
EPSILON = 1e-06
NEGATIVE = -1e30
F32 = jnp.float32
BF16 = jnp.bfloat16

NT = (((1,), (1,)), ((), ()))
NN = (((1,), (0,)), ((), ()))


def dot(a, b, dims):
    return lax.dot_general(a, b, dims, preferred_element_type=F32)


def params(mib):
    return pltpu.CompilerParams(vmem_limit_bytes=mib * 1024 * 1024)


def in_vmem():
    return pl.BlockSpec(memory_space=pltpu.VMEM)


def in_hbm():
    return pl.BlockSpec(memory_space=pltpu.HBM)


def keep_in_hbm(*arrays):
    return [pltpu.with_memory_space_constraint(x, pltpu.HBM) for x in arrays]


def lanes(shape):
    return lax.broadcasted_iota(jnp.int32, shape, 1)


def rows(shape):
    return lax.broadcasted_iota(jnp.int32, shape, 0)


def block_of(kv, tp):
    cores = lax.axis_size("core")
    inner = lax.axis_size("kv_1")
    outer = tp % cores * lax.axis_size("kv_0") + kv // inner
    return (outer * lax.axis_size("y") + tp // cores) * inner + kv % inner


def project_kernel(
    tokens, gain, wq, wd, wr, wk, wv, wo, out, own, tokens_, gain_, wq_, wd_, wr_, sems
):
    tp = lax.axis_index(TP)
    groups = lax.axis_size(TP)
    kv_size = lax.axis_size(KV)
    deep = wk.shape[1]
    pairs = (
        (tokens, tokens_),
        (gain, gain_),
        (wq, wq_),
        (wd, wd_),
        (wr, wr_),
        (wk.at[0], own.at[pl.ds(0, deep)]),
        (wv.at[0], own.at[pl.ds(deep, deep)]),
        (wo, own.at[pl.ds(2 * deep, wo.shape[0])]),
    )
    copies = [pltpu.make_async_copy(x, y, sems.at[n]) for n, (x, y) in enumerate(pairs)]
    for copy in copies:
        copy.start()
    for copy in copies[:5]:
        copy.wait()
    scaled = (tokens_[...].astype(F32) * gain_[...]).astype(BF16)
    query = dot(scaled, wq_[...], NT)
    latent = dot(scaled, wd_[...], NN)
    rope = dot(scaled, wr_[...], NT)
    seqs = scaled.shape[0]
    local = seqs // groups
    chunk = latent.shape[1] // groups
    part = latent[:, :chunk]
    for g in range(1, groups):
        part = jnp.where(tp == g, latent[:, g * chunk : (g + 1) * chunk], part)
    width = rope.shape[1]
    rope = jnp.where(lanes(rope.shape) // (width // groups) == tp, rope, 0.0)
    first = query[:, :128].astype(BF16)
    fresh = jnp.concatenate([part, rope], axis=1)
    nothing = jnp.zeros((1, 128), F32)
    for t in range(groups):
        turn = query[t * local : (t + 1) * local, 128:]
        turn = jnp.concatenate([turn[: local // 2], turn[local // 2 :]], axis=1).astype(BF16)
        tiles = [first[t * local + n : t * local + n + 2] for n in range(0, local, 2)]
        tiles += [turn[n : n + 2] for n in range(0, local // 2, 2)]
        for j in range(local):
            r = t * local + j
            new = jnp.concatenate([fresh[r : r + 1], nothing], axis=0).astype(BF16)
            for c in range(kv_size // local):
                b = block_of(c * local + j, t)
                for n, tile in enumerate(tiles + [new]):
                    out[b, :, n * 128 : (n + 1) * 128] = tile
    for copy in copies[5:]:
        copy.wait()


def rotate(values, cosine, sine):
    half = values.shape[1] // 2
    swapped = jnp.concatenate([values[:, half:], values[:, :half]], axis=1)
    return values * cosine + swapped * sine


def attend_kernel(
    got, near, opposite, far, far_opposite, lengths_, frequencies_, gain_, latents, ropes,
    out, lengths, frequencies, gain, cache, cache_rope,
    sums, lifted, turned, scored, weights, means, sems,
    *, factor, nope,
):
    kv = lax.axis_index(KV)
    tp = lax.axis_index(TP)
    kv_size = lax.axis_size(KV)
    groups = lax.axis_size(TP)
    local, positions, latent_width = cache.shape
    width = cache_rope.shape[1]
    small = []
    for n, (a, b) in enumerate(
        ((lengths_, lengths), (frequencies_, frequencies), (gain_, gain))
    ):
        small.append(pltpu.make_async_copy(a, b, sems.at[2 * local + n]))
        small[n].start()
    copies = []
    for s in range(local):
        a = pltpu.make_async_copy(latents.at[s], cache.at[s], sems.at[s])
        b = pltpu.make_async_copy(ropes.at[s], cache_rope.at[s], sems.at[local + s])
        a.start()
        b.start()
        copies.append((a, b))
    for h in range(groups):
        total = got[block_of(0, h)].astype(F32)
        for k in range(1, kv_size):
            total = total + got[block_of(k, h)].astype(F32)
        pieces = [total[:, n * 128 : (n + 1) * 128] for n in range(7)]
        turn = jnp.concatenate(pieces[4:6], axis=0)
        sums[h, :, :nope] = jnp.concatenate(pieces[:4], axis=0)
        sums[h, :, nope : nope + width] = jnp.concatenate(
            [turn[:, :width], turn[:, width:]], axis=0
        )
        sums[h, 0:1, nope + width :] = pieces[6][0:1, :width]
        sums[h, 1:2, nope + width :] = pieces[6][0:1, width:]
    for copy in small:
        copy.wait()
    shape = (local, lengths.shape[1])
    length = jnp.sum(
        jnp.where(lanes(shape) == rows(shape) + tp * local, lengths[...], 0), axis=1, keepdims=True
    )
    lane = lanes((local, width))
    angles = length.astype(F32) * frequencies[...]
    cosine = jnp.cos(angles)
    sine = jnp.sin(angles)
    sine = jnp.where(lane < width // 2, -sine, sine)
    half = groups // 2
    y = tp // 2
    core = lax.rem(tp, 2)
    for i in range(groups):
        step = (0, half - 1, 1, 2)[i % half]
        head = 2 * lax.rem(y + step, half) + (core if i < half else 1 - core)
        q = sums[head]
        w = weights_of((near, opposite, far, far_opposite), i)
        lifted[i] = dot(q[:, :nope].astype(BF16), w[:latent_width, :], NT)
        turned[i] = rotate(q[:, nope : nope + width].astype(BF16).astype(F32), cosine, sine)
    raw = jnp.concatenate([sums[h][0:1, nope + width :] for h in range(groups)], axis=1)
    rope_raw = sums[0][1:2, nope + width :]
    for h in range(1, groups):
        rope_raw = rope_raw + sums[h][1:2, nope + width :]
    square = jnp.sum(raw * raw, axis=1, keepdims=True) / latent_width
    new_latent = (raw * lax.rsqrt(square + EPSILON) * gain[...]).astype(BF16).astype(F32)
    new_seq = lax.rem(kv, local)
    mine = rows((local, width)) == new_seq
    new_rope = rotate(
        rope_raw,
        jnp.sum(jnp.where(mine, cosine, 0.0), axis=0, keepdims=True),
        jnp.sum(jnp.where(mine, sine, 0.0), axis=0, keepdims=True),
    )
    new_rope = new_rope.astype(BF16).astype(F32)
    pairs = local * groups
    for s in range(local):
        q = lifted[:, s, :].astype(BF16)
        qr = turned[:, s, :].astype(BF16)
        fresh = jnp.sum(q.astype(F32) * new_latent, axis=1, keepdims=True) + jnp.sum(
            qr.astype(F32) * new_rope, axis=1, keepdims=True
        )
        for copy in copies[s]:
            copy.wait()
        r = s * groups
        scored[r : r + groups, :positions] = dot(q, cache[s], NT) + dot(qr, cache_rope[s], NN)
        scored[r : r + groups, positions:] = jnp.broadcast_to(fresh, (groups, 128))
    scores = scored[:, :positions] * factor
    row = rows((pairs, 1))
    sequence = row // groups
    limit = jnp.zeros((pairs, 1), jnp.int32)
    for s in range(local):
        limit = jnp.where(sequence == s, length[s : s + 1, :], limit)
    is_new = jnp.logical_and(sequence == new_seq, kv < local)
    new = jnp.where(is_new, scored[:, positions : positions + 1] * factor, NEGATIVE)
    visible = kv * positions + lanes((pairs, positions)) < limit
    top = jnp.max(jnp.where(visible, scores, NEGATIVE), axis=1, keepdims=True)
    top = jnp.maximum(top, new)
    weight = jnp.where(visible, jnp.exp(scores - top), 0.0)
    new_weight = jnp.where(is_new, jnp.exp(new - top), 0.0)
    total = jnp.sum(weight, axis=1, keepdims=True) + new_weight
    weights[...] = weight.astype(BF16)
    some = total > 0.0
    safe = jnp.where(some, total, 1.0)
    inverse = 1.0 / safe
    logs = jnp.where(some, top + jnp.log(safe), NEGATIVE)
    rounded = new_weight.astype(BF16).astype(F32)
    for s in range(local):
        r = slice(s * groups, (s + 1) * groups)
        mixed = dot(weights[r, :], cache[s], NN) + rounded[r] * new_latent
        means[s] = mixed * inverse[r]
    for i in range(groups):
        w = weights_of((near, opposite, far, far_opposite), i)
        x = means[:, i, :].astype(BF16)
        up = dot(x, w[latent_width : 2 * latent_width, :], NN).astype(BF16)
        for k in range(kv_size):
            out[k, i * local : (i + 1) * local, :] = up
    lane = lanes((local, 128))
    table = jnp.zeros((groups, 128), F32)
    for s in range(local):
        table = jnp.where(lanes((groups, 128)) == s, logs[s * groups : (s + 1) * groups], table)
    table = jnp.concatenate([table, jnp.zeros((128 - groups, 128), F32)], axis=0)
    table = jnp.transpose(table)[:local]
    high = table.astype(BF16).astype(F32)
    rest = table - high
    middle = rest.astype(BF16).astype(F32)
    low = (rest - middle).astype(BF16).astype(F32)
    packed = jnp.where(
        lane < groups,
        high,
        jnp.where(
            lane < 2 * groups,
            pltpu.roll(middle, groups, 1),
            jnp.where(lane < 3 * groups, pltpu.roll(low, 2 * groups, 1), 0.0),
        ),
    ).astype(BF16)
    for k in range(kv_size):
        out[k, groups * local :, :] = packed


def weights_of(collected, i):
    near, opposite, far, far_opposite = collected
    places = near.shape[0] + 1
    stacked, single = (near, opposite) if i < places else (far, far_opposite)
    return single if i % places == places - 1 else stacked.at[i % places]


def combine_kernel(got, near, opposite, far, far_opposite, out, *, kv_size, groups, local, first):
    logs = []
    for k in range(kv_size):
        x = got[k, groups * local :, :].astype(F32)
        logs.append(x + pltpu.roll(x, 128 - groups, 1) + pltpu.roll(x, 128 - 2 * groups, 1))
    top = functools.reduce(jnp.maximum, logs)
    shares = [jnp.exp(x - top) for x in logs]
    total = functools.reduce(jnp.add, shares)
    inverse = 1.0 / total
    shares = [x * inverse for x in shares]
    mixed = jnp.zeros((local, out.shape[2]), F32)
    for i in range(groups):
        head = jnp.zeros((local, 128), F32)
        for k in range(kv_size):
            part = got[k, i * local : (i + 1) * local, :].astype(F32)
            head = head + part * shares[k][:, i : i + 1]
        w = weights_of((near, opposite, far, far_opposite), i)
        mixed = mixed + dot(head.astype(BF16), w[first:, :], NN)
    mixed = mixed.astype(BF16)
    for d in range(out.shape[0]):
        out[d] = mixed


def finish_kernel(got, gain, out, *, kv_size, groups, local):
    kv = lax.axis_index(KV)
    width = got.shape[2]
    for t in range(groups):
        squares = jnp.zeros((local, width), F32)
        for k in range(kv_size):
            x = got[block_of(k, t)].astype(F32)
            squares = squares + x * x
        mean = jnp.sum(squares, axis=1, keepdims=True) / (width * kv_size)
        own = got[block_of(kv, t)].astype(F32)
        out[t * local : (t + 1) * local, :] = (
            own * lax.rsqrt(mean + EPSILON) * gain[...]
        ).astype(BF16)


def exchange(value, axes):
    return lax.all_to_all(value, axes, split_axis=0, concat_axis=0, tiled=True)


def swap(value):
    return lax.ppermute(value, TP, [(i, i ^ 1) for i in range(lax.axis_size(TP))])


def along(own):
    size = lax.axis_size(TP)
    collected = []
    for step in (1, 3, 2):
        pairs = [(i, (i + 2 * step) % size) for i in range(size)]
        collected.append(lax.ppermute(own, TP, pairs))
    return collected


def on_device(
    tokens,
    token_gain,
    w_query,
    w_down_kv,
    w_rope_key,
    latent_gain,
    w_key_up,
    w_value_up,
    w_out,
    out_gain,
    cache_latent,
    cache_rope,
    lengths,
):
    kv_size = lax.axis_size(KV)
    groups = lax.axis_size(TP)
    everyone = kv_size * groups
    seqs, width = tokens.shape
    local, positions, latent_width = cache_latent.shape
    rope = cache_rope.shape[2]
    nope = w_key_up.shape[2]
    value = w_value_up.shape[2]
    factor = (nope + rope) ** (-0.5)

    sent, own = pl.pallas_call(
        project_kernel,
        out_shape=(
            jax.ShapeDtypeStruct((everyone, 2, 896), BF16),
            jax.ShapeDtypeStruct((2 * latent_width + value, nope), BF16),
        ),
        in_specs=[in_hbm()] * 8,
        out_specs=(in_vmem(),) * 2,
        scratch_shapes=[
            pltpu.VMEM((seqs, width), BF16),
            pltpu.VMEM((1, width), F32),
            pltpu.VMEM((nope + rope, width), BF16),
            pltpu.VMEM((width, latent_width), BF16),
            pltpu.VMEM((rope, width), BF16),
            pltpu.SemaphoreType.DMA((8,)),
        ],
        compiler_params=params(8),
        name="project",
    )(
        *keep_in_hbm(
            tokens,
            token_gain[None],
            w_query.T,
            w_down_kv,
            w_rope_key.T,
            w_key_up,
            w_value_up,
            w_out,
        )
    )

    before, after, opposite = along(own)
    near = jnp.stack([own, before, after])
    far = swap(near)
    far_opposite = swap(opposite)
    collected = (near, opposite, far, far_opposite)

    got = exchange(sent, SPREAD)
    powers = np.arange(0, rope, 2, dtype=np.float64) / rope
    frequencies = np.tile(1.0 / 10000.0**powers, 2)[None].astype(np.float32)
    sent = pl.pallas_call(
        functools.partial(attend_kernel, factor=factor, nope=nope),
        out_shape=jax.ShapeDtypeStruct((kv_size, groups * local + local, value), BF16),
        in_specs=[in_vmem()] * 5 + [in_hbm()] * 5,
        out_specs=in_vmem(),
        scratch_shapes=[
            pltpu.VMEM((1, seqs), jnp.int32),
            pltpu.VMEM((1, rope), F32),
            pltpu.VMEM((1, latent_width), F32),
            pltpu.VMEM((local, positions, latent_width), BF16),
            pltpu.VMEM((local, rope, positions), BF16),
            pltpu.VMEM((groups, local, 256), F32),
            pltpu.VMEM((groups, local, latent_width), F32),
            pltpu.VMEM((groups, local, rope), F32),
            pltpu.VMEM((local * groups, positions + 128), F32),
            pltpu.VMEM((local * groups, positions), BF16),
            pltpu.VMEM((local, groups, latent_width), F32),
            pltpu.SemaphoreType.DMA((2 * local + 3,)),
        ],
        compiler_params=params(24),
        name="attend",
    )(
        got,
        *collected,
        *keep_in_hbm(
            lengths[None],
            frequencies,
            latent_gain[None],
            cache_latent,
            cache_rope.transpose(0, 2, 1),
        ),
    )
    got = exchange(sent, KV)

    sent = pl.pallas_call(
        functools.partial(
            combine_kernel,
            kv_size=kv_size,
            groups=groups,
            local=local,
            first=2 * latent_width,
        ),
        out_shape=jax.ShapeDtypeStruct((everyone, local, w_out.shape[1]), BF16),
        in_specs=[in_vmem()] * 5,
        out_specs=in_vmem(),
        compiler_params=params(8),
        name="combine",
    )(got, *collected)
    got = exchange(sent, SPREAD)
    return pl.pallas_call(
        functools.partial(finish_kernel, kv_size=kv_size, groups=groups, local=local),
        out_shape=jax.ShapeDtypeStruct((seqs, w_out.shape[1]), BF16),
        in_specs=[in_vmem(), in_vmem()],
        out_specs=in_vmem(),
        compiler_params=params(8),
        name="finish",
    )(got, out_gain[None])


def solution(mesh):
    finer = Mesh(mesh.devices.reshape(4, 4, mesh.shape["tp"] // 2, 2), ALL)

    return jax.shard_map(
        on_device,
        mesh=finer,
        in_specs=(
            P(None, KV),
            P(KV),
            P(KV, TP),
            P(KV, None),
            P(KV, None),
            P(),
            P(TP, None, None),
            P(TP, None, None),
            P(TP, KV),
            P(KV),
            P(TP, KV, None),
            P(TP, KV, None),
            P(),
        ),
        out_specs=P(None, KV),
        check_vma=False,
    )
```
